32 devices in a mesh: sp: 8 (over z, y), tp: 4 (over x, core).
Axes of the slice: x: 2, y: 2, z: 4, core: 2. Of those that a mesh axis runs over, the one named last changes fastest.
Arguments:
- tokens: bfloat16 [2048, 4096], P('sp'), may hold values from -6 to 6
- norm_gain: float32 [4096], replicated, may hold values from 0.1 to 1.9
- w_query: bfloat16 [4096, 512], P('sp', 'tp'), may hold values from -0.09375 to 0.09375
- w_key: bfloat16 [4096, 512], P('sp', 'tp'), may hold values from -0.09375 to 0.09375
- w_value: bfloat16 [4096, 1024], P('sp', 'tp'), may hold values from -0.09375 to 0.09375
- w_gates: bfloat16 [4096, 2, 2, 4], P(None, None, None, 'tp'), may hold values from -0.09375 to 0.09375
- input_bias: float32 [2, 4], P(None, 'tp'), may hold values from -2 to 90
- forget_bias: float32 [2, 4], P(None, 'tp'), as said below
- decay_shift: float32 [2, 2048, 4], P(None, 'sp', 'tp'), may hold values from -2.5 to 0
- head_gain: float32 [1024], P('tp'), may hold values from 0.1 to 1.9
- w_conv_b: bfloat16 [4096, 1024], P('sp', 'tp'), may hold values from -0.09375 to 0.09375
- w_conv_c: bfloat16 [4096, 1024], P('sp', 'tp'), may hold values from -0.09375 to 0.09375
- w_conv_in: bfloat16 [4096, 1024], P('sp', 'tp'), may hold values from -0.09375 to 0.09375
- conv_taps: bfloat16 [3, 1024], P(None, 'tp'), may hold values from -3.5 to 3.5
- w_out: bfloat16 [2048, 4096], P('sp', 'tp'), may hold values from -0.125 to 0.125
Outputs:
- mixed_out: bfloat16 [2048, 4096], P('sp', 'tp')
The draws below stay inside these ranges and needn't reach their ends.
Inputs may be any that keep to these rules, and one draw needn't show every extreme that they name: `forget_bias`: at most the natural logarithm of 2048 plus 2.
All inputs are finite; a program needn't handle non-finite values.
Results may differ from the reference program's by a relative error of at most 0.02.
Values may be sent and summed in bfloat16 or wider, within the bound.
A program may use at most 128 MiB of HBM per device.

```python
import jax
import jax.numpy as jnp
from jax import lax

D = 4096
HEADS = 4
DQK = 128
DV = 256
BLOCK = 128
TOK_DEV = 256
BW = 1024
SEQ = 2048


def lasting_heads(key):
    shuffled = jax.random.permutation(jax.random.fold_in(key, 7), 2 * HEADS)
    keep_mask = shuffled < HEADS
    return keep_mask.reshape(2, HEADS)


def forget_values(key):
    lasting_mask = lasting_heads(key)
    quick_bias = jax.random.uniform(jax.random.fold_in(key, 11), (2, HEADS), jnp.float32, 3.5, 4.5)
    lasting = jnp.log(jnp.float32(SEQ)) + 1.5 + jax.random.uniform(jax.random.fold_in(key, 12), (2, HEADS), jnp.float32, -0.5, 0.5)
    return jnp.where(lasting_mask, lasting, quick_bias)


def draw_forget_bias(key, part):
    return forget_values(key)


def draw_decay_shift(key, part):
    decay_speed = jax.nn.softplus(-forget_values(key))
    blocks = SEQ // TOK_DEV
    multiplier = jnp.exp(jax.random.uniform(jax.random.fold_in(key, 13), (2, blocks, HEADS), jnp.float32, 0.0, jnp.log(4.0)))
    multiplier = jnp.repeat(multiplier, TOK_DEV, axis=1)
    locations = jax.random.randint(jax.random.fold_in(key, 14), (3, 2, 1, HEADS), 0, SEQ)
    loss_values = -jnp.log1p(-jax.random.uniform(jax.random.fold_in(key, 15), (3, 2, 1, HEADS), jnp.float32, 0.2, 0.5))
    token_positions = jnp.arange(SEQ, dtype=jnp.int32)[None, None, :, None]
    spike_groups = jnp.sum(jnp.where(token_positions == locations, loss_values, 0.0), axis=0)
    return -(multiplier - 1.0) * decay_speed[:, None, :] - spike_groups


def draw_input_bias(key, part):
    base_values = jax.random.uniform(key, (2, HEADS), jnp.float32, -2.0, 1.0)
    return base_values


def levels(stream_key, extent, pieces, low, top_value):
    loudness, own = 1.0, jax.random.fold_in(stream_key, 6)
    for position, shards_of in pieces:
        heights = jnp.exp(jax.random.uniform(jax.random.fold_in(own, position), (shards_of,), jnp.float32, low / len(pieces), top_value / len(pieces)))
        loudness = loudness * jnp.repeat(heights, extent[position] // shards_of).reshape([-1 if axis == position else 1 for axis in range(len(extent))])
    return loudness


def scatter_about(stream_key, shape, spread, most, split=(), held_as=jnp.bfloat16):
    loudness = levels(stream_key, shape, split, -0.22, 0.18) if split else 1.0
    values = jax.random.normal(stream_key, shape, jnp.float32) * spread * loudness
    return jnp.minimum(jnp.maximum(values, -most), most).astype(held_as)


def setup_inputs(seed: int = 0) -> dict:
    keys = jax.random.split(jax.random.key(seed), 16)
    return {
        "tokens": scatter_about(keys[0], (SEQ, D), 1.0, 6.0, ((0, 8),)),
        "norm_gain": jnp.clip(1.0 + 0.18 * jax.random.normal(keys[1], (D,), jnp.float32), 0.1, 1.9),
        "w_query": scatter_about(keys[2], (D, HEADS * DQK), D ** -0.5, 0.09375, ((0, 8), (1, 4))),
        "w_key": scatter_about(keys[3], (D, HEADS * DQK), D ** -0.5, 0.09375, ((0, 8), (1, 4))),
        "w_value": scatter_about(keys[4], (D, BW), D ** -0.5, 0.09375, ((0, 8), (1, 4))),
        "w_gates": scatter_about(keys[5], (D, 2, 2, HEADS), D ** -0.5, 0.09375, ((3, 4),)),
        "input_bias": draw_input_bias(jax.random.fold_in(keys[15], 71), 0),
        "forget_bias": draw_forget_bias(jax.random.fold_in(keys[15], 71), 0),
        "decay_shift": draw_decay_shift(jax.random.fold_in(keys[15], 71), 0),
        "head_gain": jnp.clip(1.0 + 0.18 * jax.random.normal(keys[9], (BW,), jnp.float32), 0.1, 1.9),
        "w_conv_b": scatter_about(keys[10], (D, BW), D ** -0.5, 0.09375, ((0, 8), (1, 4))),
        "w_conv_c": scatter_about(keys[11], (D, BW), D ** -0.5, 0.09375, ((0, 8), (1, 4))),
        "w_conv_in": scatter_about(keys[12], (D, BW), D ** -0.5, 0.09375, ((0, 8), (1, 4))),
        "conv_taps": scatter_about(keys[13], (3, BW), 3 ** -0.5, 3.5, ((1, 4),)),
        "w_out": scatter_about(keys[14], (2 * BW, D), (2 * BW) ** -0.5, 0.125, ((0, 8), (1, 4))),
    }


EPS = 1e-06
HIGH = lax.Precision.HIGHEST

def row_norm(tokens, norm_gain):
    values = tokens.astype(jnp.float32)
    inverse_rms = lax.rsqrt(lax.optimization_barrier(jnp.mean(values * values, axis=-1, keepdims=True)) + EPS)
    return (values * inverse_rms * norm_gain).astype(jnp.bfloat16)

def project(normed, weight):
    return jnp.dot(normed, weight, preferred_element_type=jnp.float32).astype(jnp.bfloat16)

def to_heads(source, head_count):
    length = source.shape[0]
    return source.astype(jnp.float32).reshape(length, head_count, -1).transpose(1, 0, 2)

def direction_pass(queries, keys_all, values_all, in_gate, log_forget):
    head_count, length = in_gate.shape
    block_count = length // BLOCK

    def blocked(source):
        shaped = source.reshape((head_count, block_count, BLOCK) + source.shape[2:])
        return jnp.moveaxis(shaped, 1, 0)
    lower_mask = jnp.tril(jnp.ones((BLOCK, BLOCK), dtype=bool))

    def advance(carried_state, inputs):
        memory, normer, stable = carried_state
        query_block, key_blk, value_blk, gate_blk, forget_blk = inputs
        cumulative = jnp.cumsum(forget_blk, axis=-1)
        log_weight = jnp.where(lower_mask, cumulative[:, :, None] - cumulative[:, None, :] + gate_blk[:, None, :], -jnp.inf)
        carried = cumulative + stable[:, None]
        running_max = jnp.maximum(carried, lax.optimization_barrier(jnp.max(log_weight, axis=-1)))
        scores = jnp.einsum('htd,hsd->hts', query_block, key_blk, precision=HIGH) * jnp.exp(log_weight - running_max[:, :, None])
        carry_weight = jnp.exp(carried - running_max)
        numerator = jnp.einsum('hts,hsv->htv', scores, value_blk, precision=HIGH) + carry_weight[:, :, None] * jnp.einsum('hvd,htd->htv', memory, query_block, precision=HIGH)
        denominator = lax.optimization_barrier(jnp.sum(scores, axis=-1)) + carry_weight * jnp.einsum('hd,htd->ht', normer, query_block, precision=HIGH)
        output = numerator / jnp.maximum(jnp.abs(denominator), jnp.exp(-running_max))[:, :, None]
        block_total = cumulative[:, -1]
        log_update = block_total[:, None] - cumulative + gate_blk
        new_stable = jnp.maximum(block_total + stable, lax.optimization_barrier(jnp.max(log_update, axis=-1)))
        update = jnp.exp(log_update - new_stable[:, None])
        carry_decay = jnp.exp(block_total + stable - new_stable)
        memory = carry_decay[:, None, None] * memory + jnp.einsum('hsv,hsd->hvd', value_blk * update[:, :, None], key_blk, precision=HIGH)
        normer = carry_decay[:, None] * normer + jnp.einsum('hs,hsd->hd', update, key_blk, precision=HIGH)
        return ((memory, normer, new_stable), output)
    starting_value = (jnp.zeros((head_count, DV, DQK), jnp.float32), jnp.zeros((head_count, DQK), jnp.float32), jnp.full((head_count,), -1e+30, jnp.float32))
    ignored, outputs = lax.scan(advance, starting_value, (blocked(queries), blocked(keys_all), blocked(values_all), blocked(in_gate), blocked(log_forget)))
    return jnp.moveaxis(outputs, 0, 1).reshape(head_count, length, DV)

def flipped(source):
    return jnp.flip(source, axis=1)

def reference(tokens, norm_gain, w_query, w_key, w_value, w_gates, input_bias, forget_bias, decay_shift, head_gain, w_conv_b, w_conv_c, w_conv_in, conv_taps, w_out):
    normed = row_norm(tokens, norm_gain)
    length = normed.shape[0]
    queries = to_heads(project(normed, w_query), HEADS) * DQK ** (-0.5)
    keys_all = to_heads(project(normed, w_key), HEADS)
    values_all = to_heads(project(normed, w_value), HEADS)
    gate_pre = jnp.dot(normed, w_gates.reshape(D, 4 * HEADS), preferred_element_type=jnp.float32).reshape(length, 2, 2, HEADS)
    summed = jnp.zeros((HEADS, length, DV), jnp.float32)
    for direction in range(2):
        in_gate = (gate_pre[:, direction, 0, :] + input_bias[direction]).T
        log_forget = (jax.nn.log_sigmoid(gate_pre[:, direction, 1, :] + forget_bias[direction]) + decay_shift[direction]).T
        if direction == 1:
            result = flipped(direction_pass(flipped(queries), flipped(keys_all), flipped(values_all), flipped(in_gate), flipped(log_forget)))
        else:
            result = direction_pass(queries, keys_all, values_all, in_gate, log_forget)
        summed = summed + result
    inverse_rms = lax.rsqrt(lax.optimization_barrier(jnp.mean(summed * summed, axis=-1, keepdims=True)) + EPS)
    lstm_out = ((summed * inverse_rms).transpose(1, 0, 2) * head_gain.reshape(HEADS, DV)).astype(jnp.bfloat16)
    gate_outer = project(normed, w_conv_b)
    gate_inner = project(normed, w_conv_c)
    conv_input = project(normed, w_conv_in)
    mixed_in = (gate_inner.astype(jnp.float32) * conv_input.astype(jnp.float32)).astype(jnp.bfloat16)
    padded = jnp.pad(mixed_in, ((1, 1), (0, 0))).astype(jnp.float32)
    taps_wide = conv_taps.astype(jnp.float32)
    filtered = taps_wide[0] * padded[:-2] + taps_wide[1] * padded[1:-1] + taps_wide[2] * padded[2:]
    conv_out = (gate_outer.astype(jnp.float32) * filtered).astype(jnp.bfloat16).reshape(length, HEADS, DV)
    joined = jnp.stack([lstm_out, conv_out], axis=2).reshape(length, 2 * HEADS * DV)
    return jnp.dot(joined, w_out, preferred_element_type=jnp.float32).astype(jnp.bfloat16)
```

```python
import functools

import jax
import jax.numpy as jnp
from jax import lax
from jax.experimental import pallas as pl
from jax.experimental.pallas import tpu as pltpu
from jax.sharding import PartitionSpec as P

EPS = 1e-06
HIGH = lax.Precision.HIGHEST
LOWEST = -1e30
PIECES = 4
F32 = jnp.float32
BF16 = jnp.bfloat16


def dot(a, b, dims, precision=None):
    return lax.dot_general(a, b, (dims, ((), ())), precision=precision, preferred_element_type=F32)


NN = ((1,), (0,))
NT = ((1,), (1,))
TN = ((0,), (0,))


def ring_place(index, n):
    odd = lax.rem(index, 2)
    half = lax.div(index, 2)
    return (1 - odd) * half + odd * (n - 1 - half)


def ring_index(place, n):
    late = lax.div(place, n // 2)
    return (1 - late) * (2 * place) + late * (2 * (n - 1 - place) + 1)


def pieces(depth):
    return max(1, min(PIECES, depth // 16))


def gather_kernel(
    n,
    t,
    dk,
    dv,
    tokens,
    norm_gain,
    w_query,
    w_key,
    w_value,
    w_conv_b,
    w_conv_c,
    w_conv_in,
    w_out,
    w_gates,
    input_bias,
    forget_bias,
    decay_shift,
    head_gain,
    taps,
    out,
    normed,
    w_all,
    wo_all,
    proj,
    state_out,
    pack_out,
    state_in,
    pack_in,
    carry_c,
    carry_n,
    joined,
    w_ss,
    w_rs,
    wo_ss,
    wo_rs,
    st_ss,
    st_rs,
    pk_ss,
    pk_rs,
    j_ss,
    j_rs,
    own_sem,
    gate_bias,
    decay,
):
    me = lax.axis_index("sp")
    head = lax.axis_index("tp")
    place = ring_place(me, n)
    right = ring_index(lax.rem(place + 1, n), n)
    left = ring_index(lax.rem(place + n - 1, n), n)
    rows = tokens.shape[0]

    parts = (w_query, w_key, w_value, w_conv_b, w_conv_c, w_conv_in)
    copies = []
    offset = 0
    for part in parts:
        depth, cols = part.shape
        spot = w_all.at[pl.ds(pl.multiple_of(me * depth, depth), depth), pl.ds(offset, cols)]
        copies.append(pltpu.make_async_copy(part, spot, own_sem.at[len(copies)]))
        offset += cols
    depth_o = w_out.shape[0]
    spot = wo_all.at[pl.ds(pl.multiple_of(me * depth_o, depth_o), depth_o), :]
    copies.append(pltpu.make_async_copy(w_out, spot, own_sem.at[len(copies)]))
    for copy in copies:
        copy.start()

    barrier = pltpu.get_barrier_semaphore()

    def greet_sp(o, c):
        pl.semaphore_signal(barrier, inc=1, device_id={"sp": lax.rem(me + o, n)})
        return c

    def greet_tp(o, c):
        pl.semaphore_signal(barrier, inc=1, device_id={"tp": lax.rem(head + o, t)})
        return c

    lax.fori_loop(1, n, greet_sp, 0)
    lax.fori_loop(1, t, greet_tp, 0)
    pl.semaphore_wait(barrier, n + t - 2)

    def hop(depth, whole, ss, rs, way, step, piece):
        width = whole.shape[1]
        half, tall = width // 2, depth // pieces(depth)
        holder = ring_index(lax.rem(place + (n + step if way else n - step), n), n)
        columns = pl.ds(way * half, half)
        there = whole.at[pl.ds(pl.multiple_of(holder * depth + piece * tall, tall), tall), columns]
        turn = step * pieces(depth) + piece
        return pltpu.make_async_remote_copy(
            src_ref=there,
            dst_ref=there,
            send_sem=ss.at[way, turn],
            recv_sem=rs.at[way, turn],
            device_id={"sp": left if way else right},
        )

    def ring_start(*ring):
        for piece in range(pieces(ring[0])):
            for way in range(2):
                hop(*ring, way, 0, piece).start()

    def ring_step(step, *ring):
        for piece in range(pieces(ring[0])):
            for way in range(2):
                hop(*ring, way, step - 1, piece).wait_recv()
                hop(*ring, way, step, piece).start()

    def ring_last(*ring):
        for piece in range(pieces(ring[0])):
            for way in range(2):
                hop(*ring, way, n - 2, piece).wait_recv()

    def ring_drain(*ring):
        def drain(step, c):
            for piece in range(pieces(ring[0])):
                for way in range(2):
                    hop(*ring, way, step, piece).wait_send()
            return c

        lax.fori_loop(0, n - 1, drain, 0)

    w_ring = (w_query.shape[0], w_all, w_ss, w_rs)
    wo_ring = (depth_o, wo_all, wo_ss, wo_rs)
    for copy in copies:
        copy.wait()
    ring_start(*w_ring)

    gate_bias[...] = jnp.zeros_like(gate_bias)
    gate_bias[0:2, :] = input_bias[...]
    gate_bias[2:4, :] = forget_bias[...]
    decay[...] = jnp.zeros_like(decay)
    decay[2:4, :] = decay_shift[...]

    chunk = 32

    def norm_rows(i, c):
        span = pl.ds(pl.multiple_of(i * chunk, chunk), chunk)
        values = tokens[span, :].astype(F32)
        inverse = lax.rsqrt(jnp.mean(values * values, axis=-1, keepdims=True) + EPS)
        normed[span, :] = (values * inverse * norm_gain[...]).astype(BF16)
        return c

    lax.fori_loop(0, rows // chunk, norm_rows, 0)

    gates = dot(w_gates[...], normed[...], NT) + gate_bias[...]
    forget = jnp.minimum(gates, 0.0) - jnp.log1p(jnp.exp(-jnp.abs(gates))) + decay[...]
    row_id = lax.broadcasted_iota(jnp.int32, (rows, rows), 0)
    col_id = lax.broadcasted_iota(jnp.int32, (rows, rows), 1)
    upto = (row_id <= col_id).astype(F32)
    after = (row_id >= col_id).astype(F32)
    sums = (dot(forget, upto, NN, HIGH), dot(forget, after, NN, HIGH))
    gates_t = gates.T
    sums_t = (sums[0].T, sums[1].T)

    lax.fori_loop(1, n - 1, lambda s, c: (ring_step(s, *w_ring), c)[1], 0)
    ring_start(*wo_ring)
    ring_last(*w_ring)
    done = [0]

    def advance():
        if done[0] + 1 < n - 1:
            done[0] += 1
            ring_step(done[0], *wo_ring)

    width = 256

    def project(i, c):
        span = pl.ds(pl.multiple_of(i * width, width), width)
        proj[:, span] = dot(normed[...], w_all[:, span], NN).astype(BF16)
        return c

    lax.fori_loop(0, proj.shape[1] // width, project, 0)

    query = proj[:, :dk]
    keys = proj[:, dk : 2 * dk]
    values = proj[:, 2 * dk : 2 * dk + dv]
    base = 2 * dk + dv
    bw = (proj.shape[1] - base) // 3
    mixed = (proj[:, base + bw : base + 2 * bw].astype(F32) * proj[:, base + 2 * bw :].astype(F32)).astype(BF16).astype(F32)

    keys_f = keys.astype(F32)
    totals = []
    for d in range(2):
        cum_c = sums_t[d][:, 2 + d : 3 + d]
        in_c = gates_t[:, d : d + 1]
        last = rows - 1 if d == 0 else 0
        total = cum_c[last : last + 1, :]
        update = total - cum_c + in_c
        stable = jnp.max(update, axis=0, keepdims=True)
        weighted = keys_f * jnp.exp(update - stable)
        state_out[d] = dot(weighted.astype(BF16), values, TN).astype(BF16)
        edge = mixed[rows - 1 :, :] if d == 0 else mixed[:1, :]
        wide = pack_out.shape[-1]
        pack_out[d, 0:1, :] = edge
        pack_out[d, 1:2, :dk] = jnp.sum(weighted, axis=0, keepdims=True)
        pack_out[d, 1:2, dk:] = jnp.zeros((1, wide - dk), F32)
        pack_out[d, 2:3, :] = jnp.broadcast_to(total, (1, wide))
        pack_out[d, 3:4, :] = jnp.broadcast_to(stable, (1, wide))
        pack_out[d, 4:, :] = jnp.zeros((4, wide), F32)

    def give(o):
        other = lax.rem(me + o, n)
        d = lax.div(me + o, n)
        ids = {"sp": other}
        return (
            pltpu.make_async_remote_copy(state_out.at[d], state_in.at[me], st_ss.at[o], st_rs.at[me], device_id=ids),
            pltpu.make_async_remote_copy(pack_out.at[d], pack_in.at[me], pk_ss.at[o], pk_rs.at[me], device_id=ids),
        )

    def take(o):
        source = lax.rem(me + o, n)
        ids = {"sp": source}
        return (
            pltpu.make_async_remote_copy(state_out.at[0], state_in.at[source], st_ss.at[o], st_rs.at[source], device_id=ids),
            pltpu.make_async_remote_copy(pack_out.at[0], pack_in.at[source], pk_ss.at[o], pk_rs.at[source], device_id=ids),
        )

    def give_all(o, c):
        for copy in give(o):
            copy.start()
        return c

    def take_all(o, c):
        for copy in take(o):
            copy.wait_recv()
        return c

    def give_end(o, c):
        for copy in give(o):
            copy.wait_send()
        return c

    lax.fori_loop(1, n, give_all, 0)
    advance()

    scale = dk ** (-0.5)
    scores = dot(query, keys, NT) * scale
    local = []
    for d in range(2):
        cum_c = sums_t[d][:, 2 + d : 3 + d]
        cum_r = sums[d][2 + d : 3 + d, :]
        in_r = gates[d : d + 1, :]
        allowed = row_id >= col_id if d == 0 else row_id <= col_id
        log_weight = jnp.where(allowed, cum_c - cum_r + in_r, -jnp.inf)
        peak = jnp.max(log_weight, axis=-1, keepdims=True)
        part = scores * jnp.exp(log_weight - peak)
        num = dot(part, values.astype(F32), NN, HIGH)
        local.append((cum_c, peak, num, jnp.sum(part, axis=-1, keepdims=True)))
        advance()

    lax.fori_loop(1, n, take_all, 0)

    before = pack_in[lax.rem(me + n - 1, n), 0:1, :] * jnp.minimum(me, 1).astype(F32)
    behind = pack_in[lax.rem(me + 1, n), 0:1, :] * jnp.minimum(n - 1 - me, 1).astype(F32)
    pos = lax.broadcasted_iota(jnp.int32, mixed.shape, 0)
    prior = jnp.where(pos == 0, before, pltpu.roll(mixed, 1, 0))
    later = jnp.where(pos == rows - 1, behind, pltpu.roll(mixed, rows - 1, 0))
    taps_f = taps[...].astype(F32)
    filtered = taps_f[0:1] * prior + taps_f[1:2] * mixed + taps_f[2:3] * later
    joined[head, :, dv:] = (proj[:, base : base + bw].astype(F32) * filtered).astype(BF16)

    def share(part, o, source):
        columns = pl.ds(part * dv, dv)
        slot = joined.at[source, :, columns]
        return pltpu.make_async_remote_copy(
            slot,
            slot,
            j_ss.at[part, o],
            j_rs.at[part, source],
            device_id={"tp": lax.rem(head + o, t)},
        )

    for o in range(1, t):
        share(1, o, head).start()
    advance()

    summed = None
    query_f = query.astype(F32) * scale
    for d in range(2):
        carry_c[...] = jnp.zeros_like(carry_c)
        carry_n[...] = jnp.zeros_like(carry_n)

        def join(i, peak_in):
            source = i if d == 0 else n - 1 - i
            total = pack_in[source, 2:3, :]
            stable = pack_in[source, 3:4, :]
            new = jnp.maximum(peak_in + total, stable)
            old_w = jnp.exp(peak_in + total - new)
            new_w = jnp.exp(stable - new)
            carry_c[...] = old_w * carry_c[...] + new_w * state_in[source].astype(F32)
            carry_n[...] = old_w * carry_n[...] + new_w * pack_in[source, 1:2, :]
            return new

        peak_in = lax.fori_loop(0, me if d == 0 else n - 1 - me, join, jnp.full((1, dv), LOWEST, F32))
        cum_c, peak, num, den = local[d]
        carried = cum_c + peak_in[:, :1]
        top = jnp.maximum(carried, peak)
        carry_w = jnp.exp(carried - top)
        own_w = jnp.exp(peak - top)
        num = own_w * num + carry_w * dot(query_f, carry_c[...], NN, HIGH)
        den = own_w * den + carry_w * jnp.sum(query_f * carry_n[:, :dk], axis=-1, keepdims=True)
        result = num / jnp.maximum(jnp.abs(den), jnp.exp(-top))
        summed = result if d == 0 else summed + result
        if d == 0:
            advance()
    inverse = lax.rsqrt(jnp.mean(summed * summed, axis=-1, keepdims=True) + EPS)
    joined[head, :, :dv] = (summed * inverse * head_gain[...]).astype(BF16)
    for o in range(1, t):
        share(0, o, head).start()

    lax.fori_loop(done[0] + 1, n - 1, lambda s, c: (ring_step(s, *wo_ring), c)[1], 0)
    ring_last(*wo_ring)
    for part in range(2):
        for o in range(1, t):
            share(part, o, lax.rem(head + o, t)).wait_recv()

    span_j = 2 * dv

    def emit(i, c):
        span = pl.ds(pl.multiple_of(i * width, width), width)
        total = dot(joined[0], wo_all[0:span_j, span], NN)
        for j in range(1, t):
            total += dot(joined[j], wo_all[j * span_j : (j + 1) * span_j, span], NN)
        out[:, span] = total.astype(BF16)
        return c

    lax.fori_loop(0, out.shape[1] // width, emit, 0)
    ring_drain(*w_ring)
    ring_drain(*wo_ring)
    lax.fori_loop(1, n, give_end, 0)
    for part in range(2):
        for o in range(1, t):
            share(part, o, head).wait_send()


def gather_body(
    n,
    t,
    tokens,
    norm_gain,
    w_query,
    w_key,
    w_value,
    w_gates,
    input_bias,
    forget_bias,
    decay_shift,
    head_gain,
    w_conv_b,
    w_conv_c,
    w_conv_in,
    conv_taps,
    w_out,
):
    rows, model = tokens.shape
    dk, dv = w_query.shape[1], w_value.shape[1]
    gates = jnp.transpose(w_gates[..., 0], (2, 1, 0)).reshape(4, model)
    gates = jnp.pad(gates, ((0, 4), (0, 0)))
    depth = w_query.shape[0]
    wide, cols = 2 * dk + dv + 3 * w_conv_b.shape[1], w_out.shape[1]
    hbm = pl.BlockSpec(memory_space=pl.ANY)
    vmem = pl.BlockSpec(memory_space=pltpu.VMEM)
    dma = pltpu.SemaphoreType.DMA
    return pl.pallas_call(
        functools.partial(gather_kernel, n, t, dk, dv),
        out_shape=jax.ShapeDtypeStruct((rows, cols), BF16),
        in_specs=[vmem] * 2 + [hbm] * 7 + [vmem] * 6,
        out_specs=vmem,
        scratch_shapes=[
            pltpu.VMEM((rows, model), BF16),
            pltpu.VMEM((n * depth, wide), BF16),
            pltpu.VMEM((n * w_out.shape[0], cols), BF16),
            pltpu.VMEM((rows, wide), BF16),
            pltpu.VMEM((2, dk, dv), BF16),
            pltpu.VMEM((2, 8, dv), F32),
            pltpu.VMEM((n, dk, dv), BF16),
            pltpu.VMEM((n, 8, dv), F32),
            pltpu.VMEM((dk, dv), F32),
            pltpu.VMEM((1, dv), F32),
            pltpu.VMEM((t, rows, 2 * dv), BF16),
            dma((2, (n - 1) * pieces(depth))),
            dma((2, (n - 1) * pieces(depth))),
            dma((2, (n - 1) * pieces(w_out.shape[0]))),
            dma((2, (n - 1) * pieces(w_out.shape[0]))),
            dma((n,)),
            dma((n,)),
            dma((n,)),
            dma((n,)),
            dma((2, t)),
            dma((2, t)),
            dma((7,)),
            pltpu.VMEM((8, 1), F32),
            pltpu.VMEM((8, rows), F32),
        ],
        compiler_params=pltpu.CompilerParams(
            collective_id=0, has_side_effects=True, vmem_limit_bytes=60 * 1024 * 1024
        ),
    )(
        tokens,
        norm_gain.reshape(1, model),
        w_query,
        w_key,
        w_value,
        w_conv_b,
        w_conv_c,
        w_conv_in,
        w_out,
        gates,
        input_bias,
        forget_bias,
        decay_shift[..., 0],
        head_gain.reshape(1, dv),
        conv_taps,
    )


PAIR = 2
WO_PIECES = 2


def fits(n, t, tokens, norm_gain, w_query, w_key, w_value, *rest):
    w_conv, w_out = rest[5], rest[9]
    depth, dk = w_query.shape
    dv = w_value.shape[1]
    rows = tokens.shape[0]
    even = n % PAIR == 0 and n > PAIR and t == 4
    wide = 2 * dk == dv and w_conv.shape[1] == dv and dv % 128 == 0 and dk % 128 == 0
    deep = (PAIR * depth) % (t * 128) == 0 and rows % 32 == 0 and w_out.shape[0] % (16 * WO_PIECES) == 0
    return even and wide and deep and rows <= depth


def kernel(
    n,
    t,
    dk,
    dv,
    tokens,
    norm_gain,
    w_query,
    w_key,
    w_value,
    w_conv_b,
    w_conv_c,
    w_conv_in,
    w_out,
    w_gates,
    input_bias,
    forget_bias,
    decay_shift,
    head_gain,
    taps,
    out,
    tok,
    nbuf,
    tall,
    wbuf,
    wo_all,
    acc,
    sbuf,
    rbuf,
    proj,
    wg,
    decay,
    state_out,
    pack_out,
    state_in,
    pack_in,
    edge_out,
    edge_in,
    carry_c,
    carry_n,
    local_num,
    joined,
    own_sem,
    tk_ss,
    tk_rs,
    tf_ss,
    tf_rs,
    w_ss,
    w_rs,
    rs_ss,
    rs_rs,
    st_ss,
    st_rs,
    pk_ss,
    pk_rs,
    ed_ss,
    ed_rs,
    j_ss,
    j_rs,
    oz_ss,
    oz_rs,
    oy_ss,
    oy_rs,
):
    me = lax.axis_index("sp")
    head = lax.axis_index("tp")
    lines = n // PAIR
    z = lax.div(me, PAIR)
    y = lax.rem(me, PAIR)
    mate = me + 1 - 2 * y
    core = lax.rem(head, 2)
    core_mate = head + 1 - 2 * core
    x_mate = lax.rem(head + 2, t)
    far_mate = lax.rem(core_mate + 2, t)
    rows, model = tokens.shape
    depth = w_query.shape[0]
    part_k = nbuf.shape[-1]
    chunks = wbuf.shape[0]

    def at_line(line):
        return PAIR * line + y

    load_tok = pltpu.make_async_copy(tokens, tok, own_sem.at[0])
    load_tok.start()
    mine = pl.ds(pl.multiple_of(y * depth, depth), depth)
    loads = []
    plan = ((w_query, 0, 0), (w_key, 0, dk), (w_value, 1, 0), (w_conv_c, 2, 0), (w_conv_in, 3, 0), (w_conv_b, 4, 0))
    for part, chunk, offset in plan:
        spot = wbuf.at[chunk, mine, pl.ds(offset, part.shape[1])]
        loads.append(pltpu.make_async_copy(part, spot, own_sem.at[1 + len(loads)]))
    depth_o = w_out.shape[0]
    spot = wo_all.at[pl.ds(pl.multiple_of(me * depth_o, depth_o), depth_o), :]
    loads.append(pltpu.make_async_copy(w_out, spot, own_sem.at[1 + len(loads)]))
    for load in loads:
        load.start()

    edge_in[...] = jnp.zeros_like(edge_in)

    barrier = pltpu.get_barrier_semaphore()

    def greet_sp(o, c):
        pl.semaphore_signal(barrier, inc=1, device_id={"sp": lax.rem(me + o, n)})
        return c

    def greet_tp(o, c):
        pl.semaphore_signal(barrier, inc=1, device_id={"tp": lax.rem(head + o, t)})
        return c

    lax.fori_loop(1, n, greet_sp, 0)
    lax.fori_loop(1, t, greet_tp, 0)

    load_tok.wait()
    rows_at_once = 32

    def norm_rows(i, c):
        span = pl.ds(pl.multiple_of(i * rows_at_once, rows_at_once), rows_at_once)
        values = tok[span, :].astype(F32)
        inverse = lax.rsqrt(jnp.mean(values * values, axis=-1, keepdims=True) + EPS)
        normed = (values * inverse * norm_gain[...]).astype(BF16)
        for b in range(lines * t):
            nbuf[b // t, b % t, span, :] = normed[:, b * part_k : (b + 1) * part_k]
        return c

    lax.fori_loop(0, rows // rows_at_once, norm_rows, 0)
    pl.semaphore_wait(barrier, n + t - 2)

    ups = lines - 1 - z

    def pick(k, near):
        up = jnp.clip(ups - k, 0, 1)
        down_k = k - ups
        if near:
            return up, up * (z + 1 + k) + (1 - up) * (z - 1 - down_k)
        return up, up * (lines - 1 - k) + (1 - up) * down_k

    def token_send(line):
        return pltpu.make_async_remote_copy(
            nbuf.at[line, head], tall.at[z, head], tk_ss.at[line], tk_rs.at[z], device_id={"sp": at_line(line)}
        )

    def token_take(line):
        return pltpu.make_async_remote_copy(
            nbuf.at[line, head], tall.at[line, head], tk_ss.at[line], tk_rs.at[line], device_id={"sp": at_line(line)}
        )

    def token_pass(line, way):
        quarter = (head, head, x_mate)[way]
        there = tall.at[line, quarter]
        return pltpu.make_async_remote_copy(
            there, there, tf_ss.at[way, line], tf_rs.at[way, line], device_id={"tp": (core_mate, x_mate, core_mate)[way]}
        )

    def token_get(line, way):
        quarter = (core_mate, x_mate, far_mate)[way]
        there = tall.at[line, quarter]
        return pltpu.make_async_remote_copy(
            there, there, tf_ss.at[way, line], tf_rs.at[way, line], device_id={"tp": (core_mate, x_mate, core_mate)[way]}
        )

    def send_tokens(k, c):
        _, line = pick(k, False)
        token_send(line).start()
        return c

    lax.fori_loop(0, lines - 1, send_tokens, 0)

    def w_send(chunk):
        there = wbuf.at[chunk, mine, :]
        return pltpu.make_async_remote_copy(there, there, w_ss.at[chunk], w_rs.at[chunk], device_id={"sp": mate})

    def w_take(chunk):
        there = wbuf.at[chunk, pl.ds(pl.multiple_of((1 - y) * depth, depth), depth), :]
        return pltpu.make_async_remote_copy(there, there, w_ss.at[chunk], w_rs.at[chunk], device_id={"sp": mate})

    for load in loads:
        load.wait()
    for chunk in range(chunks):
        w_send(chunk).start()

    tall_o = depth_o // WO_PIECES

    def wo_rows(index, piece):
        return wo_all.at[pl.ds(pl.multiple_of(index * depth_o + piece * tall_o, tall_o), tall_o), :]

    def wo_line(line, piece, way, sem):
        there = wo_rows(at_line(line), piece)
        return pltpu.make_async_remote_copy(
            there, there, oz_ss.at[sem, piece], oz_rs.at[line, piece], device_id={"sp": at_line(z + way)}
        )

    def wo_mate(line, piece):
        there = wo_rows(at_line(line), piece)
        return pltpu.make_async_remote_copy(
            there, there, oy_ss.at[line, piece], oy_rs.at[line, piece], device_id={"sp": mate}
        )

    def wo_mate_take(line, piece):
        there = wo_rows(PAIR * line + 1 - y, piece)
        return pltpu.make_async_remote_copy(
            there, there, oy_ss.at[line, piece], oy_rs.at[line, piece], device_id={"sp": mate}
        )

    def wo_own(way, wanted):
        @pl.when(wanted)
        def _():
            for piece in range(WO_PIECES):
                wo_line(z, piece, way, lines + (way + 1) // 2).start()

    half_way = lines // 2
    has_up, has_down = z < lines - 1, z > 0
    at_end = jnp.logical_or(z == 0, z == lines - 1)
    upper = z >= half_way

    def wo_outward():
        wo_own(1, jnp.logical_and(upper, has_up))
        wo_own(-1, jnp.logical_and(jnp.logical_not(upper), has_down))

    def wo_inward(ends):
        here = at_end if ends else jnp.logical_not(at_end)
        wo_own(-1, jnp.logical_and(jnp.logical_and(upper, has_down), here))
        wo_own(1, jnp.logical_and(jnp.logical_and(jnp.logical_not(upper), has_up), here))

    def wo_relay(line):
        @pl.when(z != line)
        def _():
            for piece in range(WO_PIECES):
                wo_line(line, piece, 0, line).wait_recv()

                @pl.when(jnp.logical_and(z > line, has_up))
                def _():
                    wo_line(line, piece, 1, line).start()

                @pl.when(jnp.logical_and(z < line, has_down))
                def _():
                    wo_line(line, piece, -1, line).start()

                wo_mate(line, piece).start()

    for piece in range(WO_PIECES):
        wo_mate(z, piece).start()
    wo_outward()

    wg[...] = jnp.zeros_like(wg)
    wg[0:2, :] = w_gates[0]
    wg[2:4, :] = w_gates[1]
    decay[...] = jnp.zeros_like(decay)
    decay[1:2, :] = decay_shift[0]
    decay[3:4, :] = decay_shift[1]
    gates = None
    for b in range(lines * t):
        piece = dot(wg[:, b * part_k : (b + 1) * part_k], nbuf[b // t, b % t], NT)
        gates = piece if b == 0 else gates + piece
    gate_id = lax.broadcasted_iota(jnp.int32, gates.shape, 0)
    offsets = (input_bias[0, 0], forget_bias[0, 0], input_bias[0, 1], forget_bias[0, 1])
    for i, offset in enumerate(offsets):
        gates = jnp.where(gate_id == i, gates + offset, gates)
    forget = jnp.minimum(gates, 0.0) - jnp.log1p(jnp.exp(-jnp.abs(gates))) + decay[...]
    row_id = lax.broadcasted_iota(jnp.int32, (rows, rows), 0)
    col_id = lax.broadcasted_iota(jnp.int32, (rows, rows), 1)
    upto = (row_id <= col_id).astype(F32)
    after = (row_id >= col_id).astype(F32)
    sums = (dot(forget, upto, NN, HIGH), dot(forget, after, NN, HIGH))
    gates_t = gates.T
    sums_t = (sums[0].T, sums[1].T)

    def relay_direct(k, c):
        _, line = pick(k, True)
        token_take(line).wait_recv()
        token_pass(line, 1).start()
        token_pass(line, 0).start()
        return c

    def relay_across(k, c):
        _, line = pick(k, True)
        token_get(line, 1).wait_recv()
        token_pass(line, 2).start()
        return c

    def tokens_ready(k, c):
        _, line = pick(k, True)
        token_get(line, 0).wait_recv()
        token_get(line, 2).wait_recv()
        return c

    lax.fori_loop(0, lines - 1, relay_direct, 0)
    lax.fori_loop(0, lines - 1, relay_across, 0)
    lax.fori_loop(0, lines - 1, tokens_ready, 0)

    def product(source, line, chunk):
        total = dot(source[line, 0], wbuf[chunk, 0:part_k, :], NN)
        for q in range(1, t):
            total += dot(source[line, q], wbuf[chunk, q * part_k : (q + 1) * part_k, :], NN)
        return total

    def hop(chunk, k, near):
        up, line = pick(k, near)
        last = (1 - up) * (1 - jnp.minimum(jnp.abs(z - line) - 1, 1))
        slot = line + last * (lines - line)
        copy = pltpu.make_async_remote_copy(
            sbuf.at[chunk, k], rbuf.at[chunk, slot], rs_ss.at[chunk, k], rs_rs.at[chunk, slot],
            device_id={"sp": at_line(z + 2 * up - 1)},
        )
        return up, line, copy

    def arrived(chunk, slot):
        return pltpu.make_async_remote_copy(
            sbuf.at[chunk, 0], rbuf.at[chunk, slot], rs_ss.at[chunk, 0], rs_rs.at[chunk, slot], device_id={"sp": me}
        )

    def reduce_chunk(chunk):
        near = chunk == 0

        def one(k, c):
            up, line, copy = hop(chunk, k, near)
            acc[...] = product(tall, line, chunk)
            before = up * jnp.minimum(z, 1) + (1 - up) * jnp.minimum(ups, 1)

            @pl.when(before == 1)
            def _():
                arrived(chunk, line).wait_recv()
                sbuf[chunk, k] = (acc[...] + rbuf[chunk, line].astype(F32)).astype(BF16)

            @pl.when(before == 0)
            def _():
                sbuf[chunk, k] = acc[...].astype(BF16)

            copy.start()
            return c

        w_take(chunk).wait_recv()
        lax.fori_loop(0, lines - 1, one, 0)

    def own_chunk(chunk):
        acc[...] = product(nbuf, z, chunk)

        @pl.when(has_down)
        def _():
            arrived(chunk, z).wait_recv()
            acc[...] += rbuf[chunk, z].astype(F32)

        @pl.when(has_up)
        def _():
            arrived(chunk, lines).wait_recv()
            acc[...] += rbuf[chunk, lines].astype(F32)

        proj[chunk] = acc[...].astype(BF16)

    reduce_chunk(0)
    reduce_chunk(1)
    wo_inward(False)
    own_chunk(0)
    reduce_chunk(2)
    own_chunk(1)

    keys_f = proj[0, :, dk:].astype(F32)
    wide = pack_out.shape[-1]
    for d in range(2):
        cum_c = sums_t[d][:, 2 * d + 1 : 2 * d + 2]
        in_c = gates_t[:, 2 * d : 2 * d + 1]
        last = rows - 1 if d == 0 else 0
        total = cum_c[last : last + 1, :]
        update = total - cum_c + in_c
        stable = jnp.max(update, axis=0, keepdims=True)
        weighted = keys_f * jnp.exp(update - stable)
        state_out[d] = dot(weighted.astype(BF16), proj[1], TN).astype(BF16)
        pack_out[d, 0:1, :dk] = jnp.sum(weighted, axis=0, keepdims=True)
        pack_out[d, 0:1, dk:] = jnp.zeros((1, wide - dk), F32)
        pack_out[d, 1:2, :] = jnp.broadcast_to(total, (1, wide))
        pack_out[d, 2:3, :] = jnp.broadcast_to(stable, (1, wide))
        pack_out[d, 3:, :] = jnp.zeros((5, wide), F32)

    def give(o):
        other = lax.rem(me + o, n)
        d = lax.div(me + o, n)
        ids = {"sp": other}
        return (
            pltpu.make_async_remote_copy(state_out.at[d], state_in.at[me], st_ss.at[o], st_rs.at[me], device_id=ids),
            pltpu.make_async_remote_copy(pack_out.at[d], pack_in.at[me], pk_ss.at[o], pk_rs.at[me], device_id=ids),
        )

    def take(o):
        source = lax.rem(me + o, n)
        ids = {"sp": source}
        return (
            pltpu.make_async_remote_copy(state_out.at[0], state_in.at[source], st_ss.at[o], st_rs.at[source], device_id=ids),
            pltpu.make_async_remote_copy(pack_out.at[0], pack_in.at[source], pk_ss.at[o], pk_rs.at[source], device_id=ids),
        )

    def give_all(o, c):
        for copy in give(o):
            copy.start()
        return c

    def take_all(o, c):
        for copy in take(o):
            copy.wait_recv()
        return c

    def give_end(o, c):
        for copy in give(o):
            copy.wait_send()
        return c

    lax.fori_loop(1, n, give_all, 0)

    reduce_chunk(3)
    own_chunk(2)

    scale = dk ** (-0.5)
    scores = dot(proj[0, :, :dk], proj[0, :, dk:], NT) * scale
    local = []
    for d in range(2):
        cum_c = sums_t[d][:, 2 * d + 1 : 2 * d + 2]
        cum_r = sums[d][2 * d + 1 : 2 * d + 2, :]
        in_r = gates[2 * d : 2 * d + 1, :]
        allowed = row_id >= col_id if d == 0 else row_id <= col_id
        log_weight = jnp.where(allowed, cum_c - cum_r + in_r, -jnp.inf)
        peak = jnp.max(log_weight, axis=-1, keepdims=True)
        part = scores * jnp.exp(log_weight - peak)
        local_num[d] = dot(part.astype(BF16), proj[1], NN)
        local.append((cum_c, peak, jnp.sum(part, axis=-1, keepdims=True)))

    reduce_chunk(4)
    wo_inward(True)
    own_chunk(3)

    mixed = (proj[2].astype(F32) * proj[3].astype(F32)).astype(BF16).astype(F32)
    edge_out[0, 0:1, :] = mixed[rows - 1 :, :]
    edge_out[1, 0:1, :] = mixed[:1, :]
    edge_out[0, 1:, :] = jnp.zeros((7, dv), F32)
    edge_out[1, 1:, :] = jnp.zeros((7, dv), F32)

    def edge(way):
        other = me + 1 if way == 0 else me - 1
        return pltpu.make_async_remote_copy(
            edge_out.at[way], edge_in.at[way], ed_ss.at[way], ed_rs.at[way], device_id={"sp": other}
        )

    later_exists, prior_exists = me < n - 1, me > 0

    @pl.when(later_exists)
    def _():
        edge(0).start()

    @pl.when(prior_exists)
    def _():
        edge(1).start()

    for line in range(1, lines - 1):
        wo_relay(line)

    def share(part, o, source):
        columns = pl.ds(part * dv, dv)
        slot = joined.at[source, :, columns]
        return pltpu.make_async_remote_copy(
            slot,
            slot,
            j_ss.at[part, o],
            j_rs.at[part, source],
            device_id={"tp": lax.rem(head + o, t)},
        )

    lax.fori_loop(1, n, take_all, 0)
    summed = None
    query_f = proj[0, :, :dk].astype(F32) * scale
    for d in range(2):
        carry_c[...] = jnp.zeros_like(carry_c)
        carry_n[...] = jnp.zeros_like(carry_n)

        def join(i, peak_in):
            source = i if d == 0 else n - 1 - i
            total = pack_in[source, 1:2, :]
            stable = pack_in[source, 2:3, :]
            new = jnp.maximum(peak_in + total, stable)
            old_w = jnp.exp(peak_in + total - new)
            new_w = jnp.exp(stable - new)
            carry_c[...] = old_w * carry_c[...] + new_w * state_in[source].astype(F32)
            carry_n[...] = old_w * carry_n[...] + new_w * pack_in[source, 0:1, :]
            return new

        peak_in = lax.fori_loop(0, me if d == 0 else n - 1 - me, join, jnp.full((1, dv), LOWEST, F32))
        cum_c, peak, den = local[d]
        carried = cum_c + peak_in[:, :1]
        top = jnp.maximum(carried, peak)
        carry_w = jnp.exp(carried - top)
        own_w = jnp.exp(peak - top)
        num = own_w * local_num[d] + carry_w * dot(query_f.astype(BF16), carry_c[...].astype(BF16), NN)
        den = own_w * den + carry_w * jnp.sum(query_f * carry_n[:, :dk], axis=-1, keepdims=True)
        result = num / jnp.maximum(jnp.abs(den), jnp.exp(-top))
        summed = result if d == 0 else summed + result
    inverse = lax.rsqrt(jnp.mean(summed * summed, axis=-1, keepdims=True) + EPS)
    joined[head, :, :dv] = (summed * inverse * head_gain[...]).astype(BF16)
    for o in range(1, t):
        share(0, o, head).start()

    own_chunk(4)

    @pl.when(prior_exists)
    def _():
        edge(0).wait_recv()

    @pl.when(later_exists)
    def _():
        edge(1).wait_recv()

    mixed = (proj[2].astype(F32) * proj[3].astype(F32)).astype(BF16).astype(F32)
    pos = lax.broadcasted_iota(jnp.int32, mixed.shape, 0)
    prior = jnp.where(pos == 0, edge_in[0, 0:1, :], pltpu.roll(mixed, 1, 0))
    later = jnp.where(pos == rows - 1, edge_in[1, 0:1, :], pltpu.roll(mixed, rows - 1, 0))
    taps_f = taps[...].astype(F32)
    filtered = taps_f[0:1] * prior + taps_f[1:2] * mixed + taps_f[2:3] * later
    joined[head, :, dv:] = (proj[4].astype(F32) * filtered).astype(BF16)
    for o in range(1, t):
        share(1, o, head).start()

    wo_relay(0)
    wo_relay(lines - 1)

    for line in range(lines):
        for piece in range(WO_PIECES):
            wo_mate_take(line, piece).wait_recv()
    for part in range(2):
        for o in range(1, t):
            share(part, o, lax.rem(head + o, t)).wait_recv()

    span_j = 2 * dv
    width = 256

    def emit(i, c):
        span = pl.ds(pl.multiple_of(i * width, width), width)
        total = dot(joined[0], wo_all[0:span_j, span], NN)
        for j in range(1, t):
            total += dot(joined[j], wo_all[j * span_j : (j + 1) * span_j, span], NN)
        out[:, span] = total.astype(BF16)
        return c

    lax.fori_loop(0, out.shape[1] // width, emit, 0)

    def token_end(k, c):
        _, line = pick(k, False)
        token_send(line).wait_send()
        for way in range(3):
            token_pass(line, way).wait_send()
        for chunk in range(chunks):
            hop(chunk, k, chunk == 0)[2].wait_send()
        return c

    lax.fori_loop(0, lines - 1, token_end, 0)
    for chunk in range(chunks):
        w_send(chunk).wait_send()
    lax.fori_loop(1, n, give_end, 0)

    @pl.when(later_exists)
    def _():
        edge(0).wait_send()

    @pl.when(prior_exists)
    def _():
        edge(1).wait_send()

    for part in range(2):
        for o in range(1, t):
            share(part, o, head).wait_send()
    for piece in range(WO_PIECES):

        @pl.when(has_up)
        def _():
            wo_line(z, piece, 1, lines + 1).wait_send()

        @pl.when(has_down)
        def _():
            wo_line(z, piece, -1, lines).wait_send()

        for line in range(lines):

            @pl.when(jnp.logical_and(z > line, has_up))
            def _():
                wo_line(line, piece, 1, line).wait_send()

            @pl.when(jnp.logical_and(z < line, has_down))
            def _():
                wo_line(line, piece, -1, line).wait_send()

            wo_mate(line, piece).wait_send()


def body(
    n,
    t,
    tokens,
    norm_gain,
    w_query,
    w_key,
    w_value,
    w_gates,
    input_bias,
    forget_bias,
    decay_shift,
    head_gain,
    w_conv_b,
    w_conv_c,
    w_conv_in,
    conv_taps,
    w_out,
):
    rows, model = tokens.shape
    depth, dk = w_query.shape
    dv = w_value.shape[1]
    lines = n // PAIR
    chunks = 5
    part_k = PAIR * depth // t
    cols = w_out.shape[1]
    gates = jnp.transpose(w_gates[..., 0], (1, 2, 0))
    hbm = pl.BlockSpec(memory_space=pl.ANY)
    vmem = pl.BlockSpec(memory_space=pltpu.VMEM)
    smem = pl.BlockSpec(memory_space=pltpu.SMEM)
    dma = pltpu.SemaphoreType.DMA
    return pl.pallas_call(
        functools.partial(kernel, n, t, dk, dv),
        out_shape=jax.ShapeDtypeStruct((rows, cols), BF16),
        in_specs=[hbm, vmem] + [hbm] * 7 + [vmem] + [smem] * 2 + [vmem] * 3,
        out_specs=vmem,
        scratch_shapes=[
            pltpu.VMEM((rows, model), BF16),
            pltpu.VMEM((lines, t, rows, part_k), BF16),
            pltpu.VMEM((lines, t, rows, part_k), BF16),
            pltpu.VMEM((chunks, PAIR * depth, dv), BF16),
            pltpu.VMEM((n * w_out.shape[0], cols), BF16),
            pltpu.VMEM((rows, dv), F32),
            pltpu.VMEM((chunks, lines - 1, rows, dv), BF16),
            pltpu.VMEM((chunks, lines + 1, rows, dv), BF16),
            pltpu.VMEM((chunks, rows, dv), BF16),
            pltpu.VMEM((8, model), BF16),
            pltpu.VMEM((8, rows), F32),
            pltpu.VMEM((2, dk, dv), BF16),
            pltpu.VMEM((2, 8, dv), F32),
            pltpu.VMEM((n, dk, dv), BF16),
            pltpu.VMEM((n, 8, dv), F32),
            pltpu.VMEM((2, 8, dv), F32),
            pltpu.VMEM((2, 8, dv), F32),
            pltpu.VMEM((dk, dv), F32),
            pltpu.VMEM((1, dv), F32),
            pltpu.VMEM((2, rows, dv), F32),
            pltpu.VMEM((t, rows, 2 * dv), BF16),
            dma((8,)),
            dma((lines,)),
            dma((lines,)),
            dma((3, lines)),
            dma((3, lines)),
            dma((chunks,)),
            dma((chunks,)),
            dma((chunks, lines - 1)),
            dma((chunks, lines + 1)),
            dma((n,)),
            dma((n,)),
            dma((n,)),
            dma((n,)),
            dma((2,)),
            dma((2,)),
            dma((2, t)),
            dma((2, t)),
            dma((lines + 2, WO_PIECES)),
            dma((lines, WO_PIECES)),
            dma((lines, WO_PIECES)),
            dma((lines, WO_PIECES)),
        ],
        compiler_params=pltpu.CompilerParams(
            collective_id=0, has_side_effects=True, vmem_limit_bytes=60 * 1024 * 1024
        ),
    )(
        tokens,
        norm_gain.reshape(1, model),
        w_query,
        w_key,
        w_value,
        w_conv_b,
        w_conv_c,
        w_conv_in,
        w_out,
        gates,
        input_bias.T,
        forget_bias.T,
        jnp.swapaxes(decay_shift, 1, 2),
        head_gain.reshape(1, dv),
        conv_taps,
    )


def solution(mesh):
    placed = (
        P("sp", None),
        P(),
        P("sp", "tp"),
        P("sp", "tp"),
        P("sp", "tp"),
        P(None, None, None, "tp"),
        P(None, "tp"),
        P(None, "tp"),
        P(None, "sp", "tp"),
        P("tp"),
        P("sp", "tp"),
        P("sp", "tp"),
        P("sp", "tp"),
        P(None, "tp"),
        P("sp", "tp"),
    )
    n, t = mesh.shape["sp"], mesh.shape["tp"]

    def step(*args):
        form = body if fits(n, t, *args) else gather_body
        return form(n, t, *args)

    return jax.shard_map(step, mesh=mesh, in_specs=placed, out_specs=P("sp", "tp"), check_vma=False)
```

```python
import functools

import jax
import jax.numpy as jnp
from jax import lax
from jax.experimental import pallas as pl
from jax.experimental.pallas import tpu as pltpu
from jax.sharding import PartitionSpec as P

EPS = 1e-06
HIGH = lax.Precision.HIGHEST
LOWEST = -1e30
PIECES = 4
F32 = jnp.float32
BF16 = jnp.bfloat16


def dot(a, b, dims, precision=None):
    return lax.dot_general(a, b, (dims, ((), ())), precision=precision, preferred_element_type=F32)


NN = ((1,), (0,))
NT = ((1,), (1,))
TN = ((0,), (0,))


def ring_place(index, n):
    odd = lax.rem(index, 2)
    half = lax.div(index, 2)
    return (1 - odd) * half + odd * (n - 1 - half)


def ring_index(place, n):
    late = lax.div(place, n // 2)
    return (1 - late) * (2 * place) + late * (2 * (n - 1 - place) + 1)


def pieces(depth):
    return max(1, min(PIECES, depth // 16))


def gather_kernel(
    n,
    t,
    dk,
    dv,
    tokens,
    norm_gain,
    w_query,
    w_key,
    w_value,
    w_conv_b,
    w_conv_c,
    w_conv_in,
    w_out,
    w_gates,
    input_bias,
    forget_bias,
    decay_shift,
    head_gain,
    taps,
    out,
    normed,
    w_all,
    wo_all,
    proj,
    state_out,
    pack_out,
    state_in,
    pack_in,
    carry_c,
    carry_n,
    joined,
    w_ss,
    w_rs,
    wo_ss,
    wo_rs,
    st_ss,
    st_rs,
    pk_ss,
    pk_rs,
    j_ss,
    j_rs,
    own_sem,
    gate_bias,
    decay,
):
    me = lax.axis_index("sp")
    head = lax.axis_index("tp")
    place = ring_place(me, n)
    right = ring_index(lax.rem(place + 1, n), n)
    left = ring_index(lax.rem(place + n - 1, n), n)
    rows = tokens.shape[0]

    parts = (w_query, w_key, w_value, w_conv_b, w_conv_c, w_conv_in)
    copies = []
    offset = 0
    for part in parts:
        depth, cols = part.shape
        spot = w_all.at[pl.ds(pl.multiple_of(me * depth, depth), depth), pl.ds(offset, cols)]
        copies.append(pltpu.make_async_copy(part, spot, own_sem.at[len(copies)]))
        offset += cols
    depth_o = w_out.shape[0]
    spot = wo_all.at[pl.ds(pl.multiple_of(me * depth_o, depth_o), depth_o), :]
    copies.append(pltpu.make_async_copy(w_out, spot, own_sem.at[len(copies)]))
    for copy in copies:
        copy.start()

    barrier = pltpu.get_barrier_semaphore()

    def greet_sp(o, c):
        pl.semaphore_signal(barrier, inc=1, device_id={"sp": lax.rem(me + o, n)})
        return c

    def greet_tp(o, c):
        pl.semaphore_signal(barrier, inc=1, device_id={"tp": lax.rem(head + o, t)})
        return c

    lax.fori_loop(1, n, greet_sp, 0)
    lax.fori_loop(1, t, greet_tp, 0)
    pl.semaphore_wait(barrier, n + t - 2)

    def hop(depth, whole, ss, rs, way, step, piece):
        width = whole.shape[1]
        half, tall = width // 2, depth // pieces(depth)
        holder = ring_index(lax.rem(place + (n + step if way else n - step), n), n)
        columns = pl.ds(way * half, half)
        there = whole.at[pl.ds(pl.multiple_of(holder * depth + piece * tall, tall), tall), columns]
        turn = step * pieces(depth) + piece
        return pltpu.make_async_remote_copy(
            src_ref=there,
            dst_ref=there,
            send_sem=ss.at[way, turn],
            recv_sem=rs.at[way, turn],
            device_id={"sp": left if way else right},
        )

    def ring_start(*ring):
        for piece in range(pieces(ring[0])):
            for way in range(2):
                hop(*ring, way, 0, piece).start()

    def ring_step(step, *ring):
        for piece in range(pieces(ring[0])):
            for way in range(2):
                hop(*ring, way, step - 1, piece).wait_recv()
                hop(*ring, way, step, piece).start()

    def ring_last(*ring):
        for piece in range(pieces(ring[0])):
            for way in range(2):
                hop(*ring, way, n - 2, piece).wait_recv()

    def ring_drain(*ring):
        def drain(step, c):
            for piece in range(pieces(ring[0])):
                for way in range(2):
                    hop(*ring, way, step, piece).wait_send()
            return c

        lax.fori_loop(0, n - 1, drain, 0)

    w_ring = (w_query.shape[0], w_all, w_ss, w_rs)
    wo_ring = (depth_o, wo_all, wo_ss, wo_rs)
    for copy in copies:
        copy.wait()
    ring_start(*w_ring)

    gate_bias[...] = jnp.zeros_like(gate_bias)
    gate_bias[0:2, :] = input_bias[...]
    gate_bias[2:4, :] = forget_bias[...]
    decay[...] = jnp.zeros_like(decay)
    decay[2:4, :] = decay_shift[...]

    chunk = 32

    def norm_rows(i, c):
        span = pl.ds(pl.multiple_of(i * chunk, chunk), chunk)
        values = tokens[span, :].astype(F32)
        inverse = lax.rsqrt(jnp.mean(values * values, axis=-1, keepdims=True) + EPS)
        normed[span, :] = (values * inverse * norm_gain[...]).astype(BF16)
        return c

    lax.fori_loop(0, rows // chunk, norm_rows, 0)

    gates = dot(w_gates[...], normed[...], NT) + gate_bias[...]
    forget = jnp.minimum(gates, 0.0) - jnp.log1p(jnp.exp(-jnp.abs(gates))) + decay[...]
    row_id = lax.broadcasted_iota(jnp.int32, (rows, rows), 0)
    col_id = lax.broadcasted_iota(jnp.int32, (rows, rows), 1)
    upto = (row_id <= col_id).astype(F32)
    after = (row_id >= col_id).astype(F32)
    sums = (dot(forget, upto, NN, HIGH), dot(forget, after, NN, HIGH))
    gates_t = gates.T
    sums_t = (sums[0].T, sums[1].T)

    lax.fori_loop(1, n - 1, lambda s, c: (ring_step(s, *w_ring), c)[1], 0)
    ring_start(*wo_ring)
    ring_last(*w_ring)
    done = [0]

    def advance():
        if done[0] + 1 < n - 1:
            done[0] += 1
            ring_step(done[0], *wo_ring)

    width = 256

    def project(i, c):
        span = pl.ds(pl.multiple_of(i * width, width), width)
        proj[:, span] = dot(normed[...], w_all[:, span], NN).astype(BF16)
        return c

    lax.fori_loop(0, proj.shape[1] // width, project, 0)

    query = proj[:, :dk]
    keys = proj[:, dk : 2 * dk]
    values = proj[:, 2 * dk : 2 * dk + dv]
    base = 2 * dk + dv
    bw = (proj.shape[1] - base) // 3
    mixed = (proj[:, base + bw : base + 2 * bw].astype(F32) * proj[:, base + 2 * bw :].astype(F32)).astype(BF16).astype(F32)

    keys_f = keys.astype(F32)
    totals = []
    for d in range(2):
        cum_c = sums_t[d][:, 2 + d : 3 + d]
        in_c = gates_t[:, d : d + 1]
        last = rows - 1 if d == 0 else 0
        total = cum_c[last : last + 1, :]
        update = total - cum_c + in_c
        stable = jnp.max(update, axis=0, keepdims=True)
        weighted = keys_f * jnp.exp(update - stable)
        state_out[d] = dot(weighted.astype(BF16), values, TN).astype(BF16)
        edge = mixed[rows - 1 :, :] if d == 0 else mixed[:1, :]
        wide = pack_out.shape[-1]
        pack_out[d, 0:1, :] = edge
        pack_out[d, 1:2, :dk] = jnp.sum(weighted, axis=0, keepdims=True)
        pack_out[d, 1:2, dk:] = jnp.zeros((1, wide - dk), F32)
        pack_out[d, 2:3, :] = jnp.broadcast_to(total, (1, wide))
        pack_out[d, 3:4, :] = jnp.broadcast_to(stable, (1, wide))
        pack_out[d, 4:, :] = jnp.zeros((4, wide), F32)

    def give(o):
        other = lax.rem(me + o, n)
        d = lax.div(me + o, n)
        ids = {"sp": other}
        return (
            pltpu.make_async_remote_copy(state_out.at[d], state_in.at[me], st_ss.at[o], st_rs.at[me], device_id=ids),
            pltpu.make_async_remote_copy(pack_out.at[d], pack_in.at[me], pk_ss.at[o], pk_rs.at[me], device_id=ids),
        )

    def take(o):
        source = lax.rem(me + o, n)
        ids = {"sp": source}
        return (
            pltpu.make_async_remote_copy(state_out.at[0], state_in.at[source], st_ss.at[o], st_rs.at[source], device_id=ids),
            pltpu.make_async_remote_copy(pack_out.at[0], pack_in.at[source], pk_ss.at[o], pk_rs.at[source], device_id=ids),
        )

    def give_all(o, c):
        for copy in give(o):
            copy.start()
        return c

    def take_all(o, c):
        for copy in take(o):
            copy.wait_recv()
        return c

    def give_end(o, c):
        for copy in give(o):
            copy.wait_send()
        return c

    lax.fori_loop(1, n, give_all, 0)
    advance()

    scale = dk ** (-0.5)
    scores = dot(query, keys, NT) * scale
    local = []
    for d in range(2):
        cum_c = sums_t[d][:, 2 + d : 3 + d]
        cum_r = sums[d][2 + d : 3 + d, :]
        in_r = gates[d : d + 1, :]
        allowed = row_id >= col_id if d == 0 else row_id <= col_id
        log_weight = jnp.where(allowed, cum_c - cum_r + in_r, -jnp.inf)
        peak = jnp.max(log_weight, axis=-1, keepdims=True)
        part = scores * jnp.exp(log_weight - peak)
        num = dot(part, values.astype(F32), NN, HIGH)
        local.append((cum_c, peak, num, jnp.sum(part, axis=-1, keepdims=True)))
        advance()

    lax.fori_loop(1, n, take_all, 0)

    before = pack_in[lax.rem(me + n - 1, n), 0:1, :] * jnp.minimum(me, 1).astype(F32)
    behind = pack_in[lax.rem(me + 1, n), 0:1, :] * jnp.minimum(n - 1 - me, 1).astype(F32)
    pos = lax.broadcasted_iota(jnp.int32, mixed.shape, 0)
    prior = jnp.where(pos == 0, before, pltpu.roll(mixed, 1, 0))
    later = jnp.where(pos == rows - 1, behind, pltpu.roll(mixed, rows - 1, 0))
    taps_f = taps[...].astype(F32)
    filtered = taps_f[0:1] * prior + taps_f[1:2] * mixed + taps_f[2:3] * later
    joined[head, :, dv:] = (proj[:, base : base + bw].astype(F32) * filtered).astype(BF16)

    def share(part, o, source):
        columns = pl.ds(part * dv, dv)
        slot = joined.at[source, :, columns]
        return pltpu.make_async_remote_copy(
            slot,
            slot,
            j_ss.at[part, o],
            j_rs.at[part, source],
            device_id={"tp": lax.rem(head + o, t)},
        )

    for o in range(1, t):
        share(1, o, head).start()
    advance()

    summed = None
    query_f = query.astype(F32) * scale
    for d in range(2):
        carry_c[...] = jnp.zeros_like(carry_c)
        carry_n[...] = jnp.zeros_like(carry_n)

        def join(i, peak_in):
            source = i if d == 0 else n - 1 - i
            total = pack_in[source, 2:3, :]
            stable = pack_in[source, 3:4, :]
            new = jnp.maximum(peak_in + total, stable)
            old_w = jnp.exp(peak_in + total - new)
            new_w = jnp.exp(stable - new)
            carry_c[...] = old_w * carry_c[...] + new_w * state_in[source].astype(F32)
            carry_n[...] = old_w * carry_n[...] + new_w * pack_in[source, 1:2, :]
            return new

        peak_in = lax.fori_loop(0, me if d == 0 else n - 1 - me, join, jnp.full((1, dv), LOWEST, F32))
        cum_c, peak, num, den = local[d]
        carried = cum_c + peak_in[:, :1]
        top = jnp.maximum(carried, peak)
        carry_w = jnp.exp(carried - top)
        own_w = jnp.exp(peak - top)
        num = own_w * num + carry_w * dot(query_f, carry_c[...], NN, HIGH)
        den = own_w * den + carry_w * jnp.sum(query_f * carry_n[:, :dk], axis=-1, keepdims=True)
        result = num / jnp.maximum(jnp.abs(den), jnp.exp(-top))
        summed = result if d == 0 else summed + result
        if d == 0:
            advance()
    inverse = lax.rsqrt(jnp.mean(summed * summed, axis=-1, keepdims=True) + EPS)
    joined[head, :, :dv] = (summed * inverse * head_gain[...]).astype(BF16)
    for o in range(1, t):
        share(0, o, head).start()

    lax.fori_loop(done[0] + 1, n - 1, lambda s, c: (ring_step(s, *wo_ring), c)[1], 0)
    ring_last(*wo_ring)
    for part in range(2):
        for o in range(1, t):
            share(part, o, lax.rem(head + o, t)).wait_recv()

    span_j = 2 * dv

    def emit(i, c):
        span = pl.ds(pl.multiple_of(i * width, width), width)
        total = dot(joined[0], wo_all[0:span_j, span], NN)
        for j in range(1, t):
            total += dot(joined[j], wo_all[j * span_j : (j + 1) * span_j, span], NN)
        out[:, span] = total.astype(BF16)
        return c

    lax.fori_loop(0, out.shape[1] // width, emit, 0)
    ring_drain(*w_ring)
    ring_drain(*wo_ring)
    lax.fori_loop(1, n, give_end, 0)
    for part in range(2):
        for o in range(1, t):
            share(part, o, head).wait_send()


def gather_body(
    n,
    t,
    tokens,
    norm_gain,
    w_query,
    w_key,
    w_value,
    w_gates,
    input_bias,
    forget_bias,
    decay_shift,
    head_gain,
    w_conv_b,
    w_conv_c,
    w_conv_in,
    conv_taps,
    w_out,
):
    rows, model = tokens.shape
    dk, dv = w_query.shape[1], w_value.shape[1]
    gates = jnp.transpose(w_gates[..., 0], (2, 1, 0)).reshape(4, model)
    gates = jnp.pad(gates, ((0, 4), (0, 0)))
    depth = w_query.shape[0]
    wide, cols = 2 * dk + dv + 3 * w_conv_b.shape[1], w_out.shape[1]
    hbm = pl.BlockSpec(memory_space=pl.ANY)
    vmem = pl.BlockSpec(memory_space=pltpu.VMEM)
    dma = pltpu.SemaphoreType.DMA
    return pl.pallas_call(
        functools.partial(gather_kernel, n, t, dk, dv),
        out_shape=jax.ShapeDtypeStruct((rows, cols), BF16),
        in_specs=[vmem] * 2 + [hbm] * 7 + [vmem] * 6,
        out_specs=vmem,
        scratch_shapes=[
            pltpu.VMEM((rows, model), BF16),
            pltpu.VMEM((n * depth, wide), BF16),
            pltpu.VMEM((n * w_out.shape[0], cols), BF16),
            pltpu.VMEM((rows, wide), BF16),
            pltpu.VMEM((2, dk, dv), BF16),
            pltpu.VMEM((2, 8, dv), F32),
            pltpu.VMEM((n, dk, dv), BF16),
            pltpu.VMEM((n, 8, dv), F32),
            pltpu.VMEM((dk, dv), F32),
            pltpu.VMEM((1, dv), F32),
            pltpu.VMEM((t, rows, 2 * dv), BF16),
            dma((2, (n - 1) * pieces(depth))),
            dma((2, (n - 1) * pieces(depth))),
            dma((2, (n - 1) * pieces(w_out.shape[0]))),
            dma((2, (n - 1) * pieces(w_out.shape[0]))),
            dma((n,)),
            dma((n,)),
            dma((n,)),
            dma((n,)),
            dma((2, t)),
            dma((2, t)),
            dma((7,)),
            pltpu.VMEM((8, 1), F32),
            pltpu.VMEM((8, rows), F32),
        ],
        compiler_params=pltpu.CompilerParams(
            collective_id=0, has_side_effects=True, vmem_limit_bytes=60 * 1024 * 1024
        ),
    )(
        tokens,
        norm_gain.reshape(1, model),
        w_query,
        w_key,
        w_value,
        w_conv_b,
        w_conv_c,
        w_conv_in,
        w_out,
        gates,
        input_bias,
        forget_bias,
        decay_shift[..., 0],
        head_gain.reshape(1, dv),
        conv_taps,
    )


PAIR = 2
WO_PIECES = 2


def fits(n, t, tokens, norm_gain, w_query, w_key, w_value, *rest):
    w_conv, w_out = rest[5], rest[9]
    depth, dk = w_query.shape
    dv = w_value.shape[1]
    rows = tokens.shape[0]
    even = n % PAIR == 0 and n > PAIR and t == 4
    wide = 2 * dk == dv and w_conv.shape[1] == dv and dv % 128 == 0 and dk % 128 == 0
    deep = (PAIR * depth) % (t * 128) == 0 and rows % 32 == 0 and w_out.shape[0] % (16 * WO_PIECES) == 0
    return even and wide and deep and rows <= depth


def kernel(
    n,
    t,
    dk,
    dv,
    tokens,
    norm_gain,
    w_query,
    w_key,
    w_value,
    w_conv_b,
    w_conv_c,
    w_conv_in,
    w_out,
    w_gates,
    input_bias,
    forget_bias,
    decay_shift,
    head_gain,
    taps,
    out,
    tok,
    nbuf,
    tall,
    wbuf,
    wo_all,
    acc,
    sbuf,
    rbuf,
    proj,
    wg,
    decay,
    state_out,
    pack_out,
    mate_state,
    mate_pack,
    pair_state,
    pair_pack,
    state_in,
    pack_in,
    edge_out,
    edge_in,
    carry_c,
    carry_n,
    local_num,
    joined,
    own_sem,
    tk_ss,
    tk_rs,
    tf_ss,
    tf_rs,
    w_ss,
    w_rs,
    rs_ss,
    rs_rs,
    st_ss,
    st_rs,
    pk_ss,
    pk_rs,
    ed_ss,
    ed_rs,
    j_ss,
    j_rs,
    oz_ss,
    oz_rs,
    oy_ss,
    oy_rs,
):
    me = lax.axis_index("sp")
    head = lax.axis_index("tp")
    lines = n // PAIR
    z = lax.div(me, PAIR)
    y = lax.rem(me, PAIR)
    mate = me + 1 - 2 * y
    core = lax.rem(head, 2)
    core_mate = head + 1 - 2 * core
    x_mate = lax.rem(head + 2, t)
    far_mate = lax.rem(core_mate + 2, t)
    rows, model = tokens.shape
    depth = w_query.shape[0]
    part_k = nbuf.shape[-1]
    chunks = wbuf.shape[0]

    def at_line(line):
        return PAIR * line + y

    load_tok = pltpu.make_async_copy(tokens, tok, own_sem.at[0])
    load_tok.start()
    mine = pl.ds(pl.multiple_of(y * depth, depth), depth)
    loads = []
    plan = ((w_query, 0, 0), (w_key, 0, dk), (w_value, 1, 0), (w_conv_c, 2, 0), (w_conv_in, 3, 0), (w_conv_b, 4, 0))
    for part, chunk, offset in plan:
        spot = wbuf.at[chunk, mine, pl.ds(offset, part.shape[1])]
        loads.append(pltpu.make_async_copy(part, spot, own_sem.at[1 + len(loads)]))
    depth_o = w_out.shape[0]
    spot = wo_all.at[pl.ds(pl.multiple_of(me * depth_o, depth_o), depth_o), :]
    loads.append(pltpu.make_async_copy(w_out, spot, own_sem.at[1 + len(loads)]))
    for load in loads:
        load.start()

    edge_in[...] = jnp.zeros_like(edge_in)

    barrier = pltpu.get_barrier_semaphore()

    def greet_sp(o, c):
        pl.semaphore_signal(barrier, inc=1, device_id={"sp": lax.rem(me + o, n)})
        return c

    def greet_tp(o, c):
        pl.semaphore_signal(barrier, inc=1, device_id={"tp": lax.rem(head + o, t)})
        return c

    lax.fori_loop(1, n, greet_sp, 0)
    lax.fori_loop(1, t, greet_tp, 0)

    load_tok.wait()
    rows_at_once = 32

    def norm_rows(i, c):
        span = pl.ds(pl.multiple_of(i * rows_at_once, rows_at_once), rows_at_once)
        values = tok[span, :].astype(F32)
        inverse = lax.rsqrt(jnp.mean(values * values, axis=-1, keepdims=True) + EPS)
        normed = (values * inverse * norm_gain[...]).astype(BF16)
        for b in range(lines * t):
            nbuf[b // t, b % t, span, :] = normed[:, b * part_k : (b + 1) * part_k]
        return c

    lax.fori_loop(0, rows // rows_at_once, norm_rows, 0)
    pl.semaphore_wait(barrier, n + t - 2)

    ups = lines - 1 - z

    half_way = lines // 2
    end_here = 1 - jnp.minimum(z, 1) * jnp.minimum(ups, 1)
    inner_up = jnp.minimum(lax.div(ups, half_way), 1)
    inner_count = inner_up * ups + (1 - inner_up) * z

    def pick(k, near):
        up = jnp.clip(ups - k, 0, 1)
        down_k = k - ups
        if near:
            return up, up * (z + 1 + k) + (1 - up) * (z - 1 - down_k)
        return up, up * (lines - 1 - k) + (1 - up) * down_k

    def token_send(line):
        return pltpu.make_async_remote_copy(
            nbuf.at[line, head], tall.at[z, head], tk_ss.at[line], tk_rs.at[z], device_id={"sp": at_line(line)}
        )

    def token_take(line):
        return pltpu.make_async_remote_copy(
            nbuf.at[line, head], tall.at[line, head], tk_ss.at[line], tk_rs.at[line], device_id={"sp": at_line(line)}
        )

    def token_pass(line, way):
        quarter = (head, head, x_mate)[way]
        there = tall.at[line, quarter]
        return pltpu.make_async_remote_copy(
            there, there, tf_ss.at[way, line], tf_rs.at[way, line], device_id={"tp": (core_mate, x_mate, core_mate)[way]}
        )

    def token_get(line, way):
        quarter = (core_mate, x_mate, far_mate)[way]
        there = tall.at[line, quarter]
        return pltpu.make_async_remote_copy(
            there, there, tf_ss.at[way, line], tf_rs.at[way, line], device_id={"tp": (core_mate, x_mate, core_mate)[way]}
        )

    def send_tokens(k, c):
        _, line = pick(k, False)
        token_send(line).start()
        return c

    lax.fori_loop(0, lines - 1, send_tokens, 0)

    def w_send(chunk):
        there = wbuf.at[chunk, mine, :]
        return pltpu.make_async_remote_copy(there, there, w_ss.at[chunk], w_rs.at[chunk], device_id={"sp": mate})

    def w_take(chunk):
        there = wbuf.at[chunk, pl.ds(pl.multiple_of((1 - y) * depth, depth), depth), :]
        return pltpu.make_async_remote_copy(there, there, w_ss.at[chunk], w_rs.at[chunk], device_id={"sp": mate})

    for load in loads:
        load.wait()
    for chunk in range(chunks):
        w_send(chunk).start()

    tall_o = depth_o // WO_PIECES

    def wo_rows(index, piece):
        return wo_all.at[pl.ds(pl.multiple_of(index * depth_o + piece * tall_o, tall_o), tall_o), :]

    def wo_line(line, piece, way, sem):
        there = wo_rows(at_line(line), piece)
        return pltpu.make_async_remote_copy(
            there, there, oz_ss.at[sem, piece], oz_rs.at[line, piece], device_id={"sp": at_line(z + way)}
        )

    def wo_mate(line, piece):
        there = wo_rows(at_line(line), piece)
        return pltpu.make_async_remote_copy(
            there, there, oy_ss.at[line, piece], oy_rs.at[line, piece], device_id={"sp": mate}
        )

    def wo_mate_take(line, piece):
        there = wo_rows(PAIR * line + 1 - y, piece)
        return pltpu.make_async_remote_copy(
            there, there, oy_ss.at[line, piece], oy_rs.at[line, piece], device_id={"sp": mate}
        )

    def wo_own(way, wanted):
        @pl.when(wanted)
        def _():
            for piece in range(WO_PIECES):
                wo_line(z, piece, way, lines + (way + 1) // 2).start()

    has_up, has_down = z < lines - 1, z > 0
    at_end = jnp.logical_or(z == 0, z == lines - 1)
    upper = z >= half_way

    def wo_outward():
        wo_own(1, jnp.logical_and(upper, has_up))
        wo_own(-1, jnp.logical_and(jnp.logical_not(upper), has_down))

    def wo_inward(ends):
        here = at_end if ends else jnp.logical_not(at_end)
        wo_own(-1, jnp.logical_and(jnp.logical_and(upper, has_down), here))
        wo_own(1, jnp.logical_and(jnp.logical_and(jnp.logical_not(upper), has_up), here))

    def wo_relay(line, wanted, along, across, pieces_now=range(WO_PIECES)):
        @pl.when(jnp.logical_and(wanted, jnp.logical_and(line >= 0, line < lines)))
        def _():
            for piece in pieces_now:
                if along:
                    wo_line(line, piece, 0, line).wait_recv()

                    @pl.when(jnp.logical_and(line < z, has_up))
                    def _():
                        wo_line(line, piece, 1, line).start()

                    @pl.when(jnp.logical_and(line > z, has_down))
                    def _():
                        wo_line(line, piece, -1, line).start()

                if across:
                    wo_mate(line, piece).start()

    inner_way = 2 * inner_up - 1

    def wo_first(pieces_now):
        wo_relay(z - inner_way * (1 - 2 * end_here), True, True, True, pieces_now)

    def wo_second(along, across):
        wo_relay(z + inner_way, jnp.logical_not(at_end), along, across)

    def wo_rest(away, pieces_now):
        wo_relay(z - away, True, True, True, pieces_now)
        wo_relay(z + away, True, True, True, pieces_now)

    for piece in range(WO_PIECES):
        wo_mate(z, piece).start()
    wo_inward(True)

    wg[...] = jnp.zeros_like(wg)
    wg[0:2, :] = w_gates[0]
    wg[2:4, :] = w_gates[1]
    decay[...] = jnp.zeros_like(decay)
    decay[1:2, :] = decay_shift[0]
    decay[3:4, :] = decay_shift[1]
    gates = None
    for b in range(lines * t):
        piece = dot(wg[:, b * part_k : (b + 1) * part_k], nbuf[b // t, b % t], NT)
        gates = piece if b == 0 else gates + piece
    gate_id = lax.broadcasted_iota(jnp.int32, gates.shape, 0)
    offsets = (input_bias[0, 0], forget_bias[0, 0], input_bias[0, 1], forget_bias[0, 1])
    for i, offset in enumerate(offsets):
        gates = jnp.where(gate_id == i, gates + offset, gates)
    forget = jnp.minimum(gates, 0.0) - jnp.log1p(jnp.exp(-jnp.abs(gates))) + decay[...]
    row_id = lax.broadcasted_iota(jnp.int32, (rows, rows), 0)
    col_id = lax.broadcasted_iota(jnp.int32, (rows, rows), 1)
    upto = (row_id <= col_id).astype(F32)
    after = (row_id >= col_id).astype(F32)
    sums = (dot(forget, upto, NN, HIGH), dot(forget, after, NN, HIGH))
    gates_t = gates.T
    sums_t = (sums[0].T, sums[1].T)

    def relay_direct(k, c):
        _, line = pick(k, True)
        token_take(line).wait_recv()
        token_pass(line, 1).start()
        token_pass(line, 0).start()
        return c

    def relay_across(k, c):
        _, line = pick(k, True)
        token_get(line, 1).wait_recv()
        token_pass(line, 2).start()
        return c

    def tokens_ready(k, c):
        _, line = pick(k, True)
        token_get(line, 0).wait_recv()
        token_get(line, 2).wait_recv()
        return c

    lax.fori_loop(0, lines - 1, relay_direct, 0)
    wo_outward()
    wo_inward(False)
    lax.fori_loop(0, lines - 1, relay_across, 0)
    lax.fori_loop(0, lines - 1, tokens_ready, 0)
    def product(source, line, chunk):
        total = dot(source[line, 0], wbuf[chunk, 0:part_k, :], NN)
        for q in range(1, t):
            total += dot(source[line, q], wbuf[chunk, q * part_k : (q + 1) * part_k, :], NN)
        return total

    def hop(chunk, k, up, line):
        last = (1 - up) * (1 - jnp.minimum(jnp.abs(z - line) - 1, 1))
        slot = line + last * (lines - line)
        return pltpu.make_async_remote_copy(
            sbuf.at[chunk, k],
            rbuf.at[chunk, slot],
            rs_ss.at[chunk, k],
            rs_rs.at[chunk, slot],
            device_id={"sp": at_line(z + 2 * up - 1)},
        )

    def arrived(chunk, slot):
        return pltpu.make_async_remote_copy(
            sbuf.at[chunk, 0], rbuf.at[chunk, slot], rs_ss.at[chunk, 0], rs_rs.at[chunk, slot], device_id={"sp": me}
        )

    def add_along(chunk, slot, up, line):
        acc[...] = product(tall, line, chunk)
        before = up * jnp.minimum(z, 1) + (1 - up) * jnp.minimum(ups, 1)

        @pl.when(before == 1)
        def _():
            arrived(chunk, line).wait_recv()
            sbuf[chunk, slot] = (acc[...] + rbuf[chunk, line].astype(F32)).astype(BF16)

        @pl.when(before == 0)
        def _():
            sbuf[chunk, slot] = acc[...].astype(BF16)

        hop(chunk, slot, up, line).start()

    def inward(end_chunk, mid_chunk):
        end_runs, mid_runs = int(end_chunk < chunks), int(0 <= mid_chunk < chunks)
        runs = end_here * end_runs + (1 - end_here) * mid_runs
        chunk = end_here * end_chunk + (1 - end_here) * mid_chunk

        @pl.when(runs == 1)
        def _():
            w_take(chunk).wait_recv()

        def one(k, c):
            line = inner_up * (lines - 1 - k) + (1 - inner_up) * k
            add_along(chunk, k, inner_up, line)
            return c

        lax.fori_loop(0, runs * inner_count, one, 0)

    def outward(chunk):
        def one(k, c):
            line = (1 - inner_up) * (lines - 1 - k) + inner_up * k
            add_along(chunk, inner_count + k, 1 - inner_up, line)
            return c

        lax.fori_loop(0, lines - 1 - inner_count, one, 0)

    def own_chunk(chunk):
        acc[...] = product(nbuf, z, chunk)

        @pl.when(has_down)
        def _():
            arrived(chunk, z).wait_recv()
            acc[...] += rbuf[chunk, z].astype(F32)

        @pl.when(has_up)
        def _():
            arrived(chunk, lines).wait_recv()
            acc[...] += rbuf[chunk, lines].astype(F32)

        proj[chunk] = acc[...].astype(BF16)

    inward(0, -1)
    inward(1, -1)
    inward(2, 0)
    wo_first((0,))
    wo_second(True, False)
    inward(3, 1)
    wo_first(range(1, WO_PIECES))
    outward(0)
    own_chunk(0)
    inward(4, 2)
    outward(1)
    own_chunk(1)

    keys_f = proj[0, :, dk:].astype(F32)
    wide = pack_out.shape[-1]
    for d in range(2):
        cum_c = sums_t[d][:, 2 * d + 1 : 2 * d + 2]
        in_c = gates_t[:, 2 * d : 2 * d + 1]
        last = rows - 1 if d == 0 else 0
        total = cum_c[last : last + 1, :]
        update = total - cum_c + in_c
        stable = jnp.max(update, axis=0, keepdims=True)
        weighted = keys_f * jnp.exp(update - stable)
        state_out[d] = dot(weighted.astype(BF16), proj[1], TN).astype(BF16)
        pack_out[d, 0:1, :dk] = jnp.sum(weighted, axis=0, keepdims=True)
        pack_out[d, 0:1, dk:] = jnp.zeros((1, wide - dk), F32)
        pack_out[d, 1:2, :] = jnp.broadcast_to(total, (1, wide))
        pack_out[d, 2:3, :] = jnp.broadcast_to(stable, (1, wide))
        pack_out[d, 3:, :] = jnp.zeros((5, wide), F32)

    def swap_states():
        return (
            pltpu.make_async_remote_copy(state_out, mate_state, st_ss.at[lines], st_rs.at[lines], device_id={"sp": mate}),
            pltpu.make_async_remote_copy(pack_out, mate_pack, pk_ss.at[lines], pk_rs.at[lines], device_id={"sp": mate}),
        )

    for copy in swap_states():
        copy.start()
    wo_second(False, True)
    wo_rest(2, (0,))

    def give(o):
        other = lax.rem(z + o, lines)
        d = lax.div(z + o, lines)
        ids = {"sp": at_line(other)}
        return (
            pltpu.make_async_remote_copy(pair_state.at[d], state_in.at[z], st_ss.at[o], st_rs.at[z], device_id=ids),
            pltpu.make_async_remote_copy(pair_pack.at[d], pack_in.at[z], pk_ss.at[o], pk_rs.at[z], device_id=ids),
        )

    def take(o):
        source = lax.rem(z + o, lines)
        ids = {"sp": at_line(source)}
        return (
            pltpu.make_async_remote_copy(pair_state.at[0], state_in.at[source], st_ss.at[o], st_rs.at[source], device_id=ids),
            pltpu.make_async_remote_copy(pair_pack.at[0], pack_in.at[source], pk_ss.at[o], pk_rs.at[source], device_id=ids),
        )

    def give_all(o, c):
        for copy in give(o):
            copy.start()
        return c

    def take_all(o, c):
        for copy in take(o):
            copy.wait_recv()
        return c

    def give_end(o, c):
        for copy in give(o):
            copy.wait_send()
        return c

    def blend(first, second):
        total = first[1:2, :] + second[1:2, :]
        moved = first[2:3, :] + second[1:2, :]
        stable = jnp.maximum(moved, second[2:3, :])
        return total, stable, jnp.exp(moved - stable), jnp.exp(second[2:3, :] - stable)

    def pair_up():
        for copy in swap_states():
            copy.wait_recv()
        own_first = (1 - y).astype(F32)
        for d in range(2):
            lead = own_first if d == 0 else 1.0 - own_first
            mine_p, other_p = pack_out[d], mate_pack[d]
            first = lead * mine_p + (1.0 - lead) * other_p
            second = lead * other_p + (1.0 - lead) * mine_p
            total, stable, first_w, second_w = blend(first, second)
            mine_w = lead * first_w + (1.0 - lead) * second_w
            other_w = lead * second_w + (1.0 - lead) * first_w
            joint = mine_w * state_out[d].astype(F32) + other_w * mate_state[d].astype(F32)
            pair_state[d] = joint.astype(BF16)
            pair_pack[d, 0:1, :] = mine_w * mine_p[0:1, :] + other_w * other_p[0:1, :]
            pair_pack[d, 1:2, :] = total
            pair_pack[d, 2:3, :] = stable
            pair_pack[d, 3:, :] = jnp.zeros((5, wide), F32)

    inward(5, 3)
    pair_up()
    lax.fori_loop(1, lines, give_all, 0)
    outward(2)
    wo_rest(2, range(1, WO_PIECES))
    own_chunk(2)

    scale = dk ** (-0.5)
    scores = dot(proj[0, :, :dk], proj[0, :, dk:], NT) * scale
    local = []
    for d in range(2):
        cum_c = sums_t[d][:, 2 * d + 1 : 2 * d + 2]
        cum_r = sums[d][2 * d + 1 : 2 * d + 2, :]
        in_r = gates[2 * d : 2 * d + 1, :]
        allowed = row_id >= col_id if d == 0 else row_id <= col_id
        log_weight = jnp.where(allowed, cum_c - cum_r + in_r, -jnp.inf)
        peak = jnp.max(log_weight, axis=-1, keepdims=True)
        part = scores * jnp.exp(log_weight - peak)
        local_num[d] = dot(part.astype(BF16), proj[1], NN)
        local.append((cum_c, peak, jnp.sum(part, axis=-1, keepdims=True)))

    inward(6, 4)
    outward(3)
    own_chunk(3)

    mixed = (proj[2].astype(F32) * proj[3].astype(F32)).astype(BF16).astype(F32)
    edge_out[0, 0:1, :] = mixed[rows - 1 :, :]
    edge_out[1, 0:1, :] = mixed[:1, :]
    edge_out[0, 1:, :] = jnp.zeros((7, dv), F32)
    edge_out[1, 1:, :] = jnp.zeros((7, dv), F32)

    def edge(way):
        other = me + 1 if way == 0 else me - 1
        return pltpu.make_async_remote_copy(
            edge_out.at[way], edge_in.at[way], ed_ss.at[way], ed_rs.at[way], device_id={"sp": other}
        )

    later_exists, prior_exists = me < n - 1, me > 0

    @pl.when(later_exists)
    def _():
        edge(0).start()

    @pl.when(prior_exists)
    def _():
        edge(1).start()

    for away in range(3, lines):
        wo_rest(away, range(WO_PIECES))
    outward(4)

    def share(part, o, source):
        columns = pl.ds(part * dv, dv)
        slot = joined.at[source, :, columns]
        return pltpu.make_async_remote_copy(
            slot,
            slot,
            j_ss.at[part, o],
            j_rs.at[part, source],
            device_id={"tp": lax.rem(head + o, t)},
        )

    lax.fori_loop(1, lines, take_all, 0)
    summed = None
    query_f = proj[0, :, :dk].astype(F32) * scale
    for d in range(2):
        carry_c[...] = jnp.zeros_like(carry_c)
        carry_n[...] = jnp.zeros_like(carry_n)

        def merge(state, pack, peak_in):
            total = pack[1:2, :]
            stable = pack[2:3, :]
            new = jnp.maximum(peak_in + total, stable)
            old_w = jnp.exp(peak_in + total - new)
            new_w = jnp.exp(stable - new)
            carry_c[...] = old_w * carry_c[...] + new_w * state.astype(F32)
            carry_n[...] = old_w * carry_n[...] + new_w * pack[0:1, :]
            return new

        def join(i, peak_in):
            source = i if d == 0 else lines - 1 - i
            return merge(state_in[source], pack_in[source], peak_in)

        def join_mate(i, peak_in):
            return merge(mate_state[d], mate_pack[d], peak_in)

        peak_in = lax.fori_loop(0, z if d == 0 else ups, join, jnp.full((1, dv), LOWEST, F32))
        peak_in = lax.fori_loop(0, y if d == 0 else 1 - y, join_mate, peak_in)
        cum_c, peak, den = local[d]
        carried = cum_c + peak_in[:, :1]
        top = jnp.maximum(carried, peak)
        carry_w = jnp.exp(carried - top)
        own_w = jnp.exp(peak - top)
        num = own_w * local_num[d] + carry_w * dot(query_f.astype(BF16), carry_c[...].astype(BF16), NN)
        den = own_w * den + carry_w * jnp.sum(query_f * carry_n[:, :dk], axis=-1, keepdims=True)
        result = num / jnp.maximum(jnp.abs(den), jnp.exp(-top))
        summed = result if d == 0 else summed + result
    inverse = lax.rsqrt(jnp.mean(summed * summed, axis=-1, keepdims=True) + EPS)
    joined[head, :, :dv] = (summed * inverse * head_gain[...]).astype(BF16)
    for o in range(1, t):
        share(0, o, head).start()

    own_chunk(4)

    @pl.when(prior_exists)
    def _():
        edge(0).wait_recv()

    @pl.when(later_exists)
    def _():
        edge(1).wait_recv()

    mixed = (proj[2].astype(F32) * proj[3].astype(F32)).astype(BF16).astype(F32)
    pos = lax.broadcasted_iota(jnp.int32, mixed.shape, 0)
    prior = jnp.where(pos == 0, edge_in[0, 0:1, :], pltpu.roll(mixed, 1, 0))
    later = jnp.where(pos == rows - 1, edge_in[1, 0:1, :], pltpu.roll(mixed, rows - 1, 0))
    taps_f = taps[...].astype(F32)
    filtered = taps_f[0:1] * prior + taps_f[1:2] * mixed + taps_f[2:3] * later
    joined[head, :, dv:] = (proj[4].astype(F32) * filtered).astype(BF16)
    for o in range(1, t):
        share(1, o, head).start()

    for line in range(lines):
        for piece in range(WO_PIECES):
            wo_mate_take(line, piece).wait_recv()
    for part in range(2):
        for o in range(1, t):
            share(part, o, lax.rem(head + o, t)).wait_recv()

    span_j = 2 * dv
    width = 256

    def emit(i, c):
        span = pl.ds(pl.multiple_of(i * width, width), width)
        total = dot(joined[0], wo_all[0:span_j, span], NN)
        for j in range(1, t):
            total += dot(joined[j], wo_all[j * span_j : (j + 1) * span_j, span], NN)
        out[:, span] = total.astype(BF16)
        return c

    lax.fori_loop(0, out.shape[1] // width, emit, 0)

    def token_end(k, c):
        _, line = pick(k, False)
        token_send(line).wait_send()
        for way in range(3):
            token_pass(line, way).wait_send()
        inner = jnp.clip(inner_count - k, 0, 1)
        up = inner * inner_up + (1 - inner) * (1 - inner_up)
        step = inner * k + (1 - inner) * (k - inner_count)
        line = up * (lines - 1 - step) + (1 - up) * step
        for chunk in range(chunks):
            hop(chunk, k, up, line).wait_send()
        return c

    lax.fori_loop(0, lines - 1, token_end, 0)
    for chunk in range(chunks):
        w_send(chunk).wait_send()
    for copy in swap_states():
        copy.wait_send()
    lax.fori_loop(1, lines, give_end, 0)

    @pl.when(later_exists)
    def _():
        edge(0).wait_send()

    @pl.when(prior_exists)
    def _():
        edge(1).wait_send()

    for part in range(2):
        for o in range(1, t):
            share(part, o, head).wait_send()
    for piece in range(WO_PIECES):

        @pl.when(has_up)
        def _():
            wo_line(z, piece, 1, lines + 1).wait_send()

        @pl.when(has_down)
        def _():
            wo_line(z, piece, -1, lines).wait_send()

        for line in range(lines):

            @pl.when(jnp.logical_and(z > line, has_up))
            def _():
                wo_line(line, piece, 1, line).wait_send()

            @pl.when(jnp.logical_and(z < line, has_down))
            def _():
                wo_line(line, piece, -1, line).wait_send()

            wo_mate(line, piece).wait_send()


def body(
    n,
    t,
    tokens,
    norm_gain,
    w_query,
    w_key,
    w_value,
    w_gates,
    input_bias,
    forget_bias,
    decay_shift,
    head_gain,
    w_conv_b,
    w_conv_c,
    w_conv_in,
    conv_taps,
    w_out,
):
    rows, model = tokens.shape
    depth, dk = w_query.shape
    dv = w_value.shape[1]
    lines = n // PAIR
    chunks = 5
    part_k = PAIR * depth // t
    cols = w_out.shape[1]
    gates = jnp.transpose(w_gates[..., 0], (1, 2, 0))
    hbm = pl.BlockSpec(memory_space=pl.ANY)
    vmem = pl.BlockSpec(memory_space=pltpu.VMEM)
    smem = pl.BlockSpec(memory_space=pltpu.SMEM)
    dma = pltpu.SemaphoreType.DMA
    return pl.pallas_call(
        functools.partial(kernel, n, t, dk, dv),
        out_shape=jax.ShapeDtypeStruct((rows, cols), BF16),
        in_specs=[hbm, vmem] + [hbm] * 7 + [vmem] + [smem] * 2 + [vmem] * 3,
        out_specs=vmem,
        scratch_shapes=[
            pltpu.VMEM((rows, model), BF16),
            pltpu.VMEM((lines, t, rows, part_k), BF16),
            pltpu.VMEM((lines, t, rows, part_k), BF16),
            pltpu.VMEM((chunks, PAIR * depth, dv), BF16),
            pltpu.VMEM((n * w_out.shape[0], cols), BF16),
            pltpu.VMEM((rows, dv), F32),
            pltpu.VMEM((chunks, lines - 1, rows, dv), BF16),
            pltpu.VMEM((chunks, lines + 1, rows, dv), BF16),
            pltpu.VMEM((chunks, rows, dv), BF16),
            pltpu.VMEM((8, model), BF16),
            pltpu.VMEM((8, rows), F32),
            pltpu.VMEM((2, dk, dv), BF16),
            pltpu.VMEM((2, 8, dv), F32),
            pltpu.VMEM((2, dk, dv), BF16),
            pltpu.VMEM((2, 8, dv), F32),
            pltpu.VMEM((2, dk, dv), BF16),
            pltpu.VMEM((2, 8, dv), F32),
            pltpu.VMEM((lines, dk, dv), BF16),
            pltpu.VMEM((lines, 8, dv), F32),
            pltpu.VMEM((2, 8, dv), F32),
            pltpu.VMEM((2, 8, dv), F32),
            pltpu.VMEM((dk, dv), F32),
            pltpu.VMEM((1, dv), F32),
            pltpu.VMEM((2, rows, dv), F32),
            pltpu.VMEM((t, rows, 2 * dv), BF16),
            dma((8,)),
            dma((lines,)),
            dma((lines,)),
            dma((3, lines)),
            dma((3, lines)),
            dma((chunks,)),
            dma((chunks,)),
            dma((chunks, lines - 1)),
            dma((chunks, lines + 1)),
            dma((lines + 1,)),
            dma((lines + 1,)),
            dma((lines + 1,)),
            dma((lines + 1,)),
            dma((2,)),
            dma((2,)),
            dma((2, t)),
            dma((2, t)),
            dma((lines + 2, WO_PIECES)),
            dma((lines, WO_PIECES)),
            dma((lines, WO_PIECES)),
            dma((lines, WO_PIECES)),
        ],
        compiler_params=pltpu.CompilerParams(
            collective_id=0, has_side_effects=True, vmem_limit_bytes=60 * 1024 * 1024
        ),
    )(
        tokens,
        norm_gain.reshape(1, model),
        w_query,
        w_key,
        w_value,
        w_conv_b,
        w_conv_c,
        w_conv_in,
        w_out,
        gates,
        input_bias.T,
        forget_bias.T,
        jnp.swapaxes(decay_shift, 1, 2),
        head_gain.reshape(1, dv),
        conv_taps,
    )


def solution(mesh):
    placed = (
        P("sp", None),
        P(),
        P("sp", "tp"),
        P("sp", "tp"),
        P("sp", "tp"),
        P(None, None, None, "tp"),
        P(None, "tp"),
        P(None, "tp"),
        P(None, "sp", "tp"),
        P("tp"),
        P("sp", "tp"),
        P("sp", "tp"),
        P("sp", "tp"),
        P(None, "tp"),
        P("sp", "tp"),
    )
    n, t = mesh.shape["sp"], mesh.shape["tp"]

    def step(*args):
        form = body if fits(n, t, *args) else gather_body
        return form(n, t, *args)

    return jax.shard_map(step, mesh=mesh, in_specs=placed, out_specs=P("sp", "tp"), check_vma=False)
```

```python
import functools

import jax
import jax.numpy as jnp
from jax import lax
from jax.experimental import pallas as pl
from jax.experimental.pallas import tpu as pltpu
from jax.sharding import PartitionSpec as P

EPS = 1e-06
HIGH = lax.Precision.HIGHEST
LOWEST = -1e30
PIECES = 4
F32 = jnp.float32
BF16 = jnp.bfloat16


def dot(a, b, dims, precision=None):
    return lax.dot_general(a, b, (dims, ((), ())), precision=precision, preferred_element_type=F32)


NN = ((1,), (0,))
NT = ((1,), (1,))
TN = ((0,), (0,))


def ring_place(index, n):
    odd = lax.rem(index, 2)
    half = lax.div(index, 2)
    return (1 - odd) * half + odd * (n - 1 - half)


def ring_index(place, n):
    late = lax.div(place, n // 2)
    return (1 - late) * (2 * place) + late * (2 * (n - 1 - place) + 1)


def pieces(depth):
    return max(1, min(PIECES, depth // 16))


def gather_kernel(
    n,
    t,
    dk,
    dv,
    tokens,
    norm_gain,
    w_query,
    w_key,
    w_value,
    w_conv_b,
    w_conv_c,
    w_conv_in,
    w_out,
    w_gates,
    input_bias,
    forget_bias,
    decay_shift,
    head_gain,
    taps,
    out,
    normed,
    w_all,
    wo_all,
    proj,
    state_out,
    pack_out,
    state_in,
    pack_in,
    carry_c,
    carry_n,
    joined,
    w_ss,
    w_rs,
    wo_ss,
    wo_rs,
    st_ss,
    st_rs,
    pk_ss,
    pk_rs,
    j_ss,
    j_rs,
    own_sem,
    gate_bias,
    decay,
):
    me = lax.axis_index("sp")
    head = lax.axis_index("tp")
    place = ring_place(me, n)
    right = ring_index(lax.rem(place + 1, n), n)
    left = ring_index(lax.rem(place + n - 1, n), n)
    rows = tokens.shape[0]

    parts = (w_query, w_key, w_value, w_conv_b, w_conv_c, w_conv_in)
    copies = []
    offset = 0
    for part in parts:
        depth, cols = part.shape
        spot = w_all.at[pl.ds(pl.multiple_of(me * depth, depth), depth), pl.ds(offset, cols)]
        copies.append(pltpu.make_async_copy(part, spot, own_sem.at[len(copies)]))
        offset += cols
    depth_o = w_out.shape[0]
    spot = wo_all.at[pl.ds(pl.multiple_of(me * depth_o, depth_o), depth_o), :]
    copies.append(pltpu.make_async_copy(w_out, spot, own_sem.at[len(copies)]))
    for copy in copies:
        copy.start()

    barrier = pltpu.get_barrier_semaphore()

    def greet_sp(o, c):
        pl.semaphore_signal(barrier, inc=1, device_id={"sp": lax.rem(me + o, n)})
        return c

    def greet_tp(o, c):
        pl.semaphore_signal(barrier, inc=1, device_id={"tp": lax.rem(head + o, t)})
        return c

    lax.fori_loop(1, n, greet_sp, 0)
    lax.fori_loop(1, t, greet_tp, 0)
    pl.semaphore_wait(barrier, n + t - 2)

    def hop(depth, whole, ss, rs, way, step, piece):
        width = whole.shape[1]
        half, tall = width // 2, depth // pieces(depth)
        holder = ring_index(lax.rem(place + (n + step if way else n - step), n), n)
        columns = pl.ds(way * half, half)
        there = whole.at[pl.ds(pl.multiple_of(holder * depth + piece * tall, tall), tall), columns]
        turn = step * pieces(depth) + piece
        return pltpu.make_async_remote_copy(
            src_ref=there,
            dst_ref=there,
            send_sem=ss.at[way, turn],
            recv_sem=rs.at[way, turn],
            device_id={"sp": left if way else right},
        )

    def ring_start(*ring):
        for piece in range(pieces(ring[0])):
            for way in range(2):
                hop(*ring, way, 0, piece).start()

    def ring_step(step, *ring):
        for piece in range(pieces(ring[0])):
            for way in range(2):
                hop(*ring, way, step - 1, piece).wait_recv()
                hop(*ring, way, step, piece).start()

    def ring_last(*ring):
        for piece in range(pieces(ring[0])):
            for way in range(2):
                hop(*ring, way, n - 2, piece).wait_recv()

    def ring_drain(*ring):
        def drain(step, c):
            for piece in range(pieces(ring[0])):
                for way in range(2):
                    hop(*ring, way, step, piece).wait_send()
            return c

        lax.fori_loop(0, n - 1, drain, 0)

    w_ring = (w_query.shape[0], w_all, w_ss, w_rs)
    wo_ring = (depth_o, wo_all, wo_ss, wo_rs)
    for copy in copies:
        copy.wait()
    ring_start(*w_ring)

    gate_bias[...] = jnp.zeros_like(gate_bias)
    gate_bias[0:2, :] = input_bias[...]
    gate_bias[2:4, :] = forget_bias[...]
    decay[...] = jnp.zeros_like(decay)
    decay[2:4, :] = decay_shift[...]

    chunk = 32

    def norm_rows(i, c):
        span = pl.ds(pl.multiple_of(i * chunk, chunk), chunk)
        values = tokens[span, :].astype(F32)
        inverse = lax.rsqrt(jnp.mean(values * values, axis=-1, keepdims=True) + EPS)
        normed[span, :] = (values * inverse * norm_gain[...]).astype(BF16)
        return c

    lax.fori_loop(0, rows // chunk, norm_rows, 0)

    gates = dot(w_gates[...], normed[...], NT) + gate_bias[...]
    forget = jnp.minimum(gates, 0.0) - jnp.log1p(jnp.exp(-jnp.abs(gates))) + decay[...]
    row_id = lax.broadcasted_iota(jnp.int32, (rows, rows), 0)
    col_id = lax.broadcasted_iota(jnp.int32, (rows, rows), 1)
    upto = (row_id <= col_id).astype(F32)
    after = (row_id >= col_id).astype(F32)
    sums = (dot(forget, upto, NN, HIGH), dot(forget, after, NN, HIGH))
    gates_t = gates.T
    sums_t = (sums[0].T, sums[1].T)

    lax.fori_loop(1, n - 1, lambda s, c: (ring_step(s, *w_ring), c)[1], 0)
    ring_start(*wo_ring)
    ring_last(*w_ring)
    done = [0]

    def advance():
        if done[0] + 1 < n - 1:
            done[0] += 1
            ring_step(done[0], *wo_ring)

    width = 256

    def project(i, c):
        span = pl.ds(pl.multiple_of(i * width, width), width)
        proj[:, span] = dot(normed[...], w_all[:, span], NN).astype(BF16)
        return c

    lax.fori_loop(0, proj.shape[1] // width, project, 0)

    query = proj[:, :dk]
    keys = proj[:, dk : 2 * dk]
    values = proj[:, 2 * dk : 2 * dk + dv]
    base = 2 * dk + dv
    bw = (proj.shape[1] - base) // 3
    mixed = (proj[:, base + bw : base + 2 * bw].astype(F32) * proj[:, base + 2 * bw :].astype(F32)).astype(BF16).astype(F32)

    keys_f = keys.astype(F32)
    totals = []
    for d in range(2):
        cum_c = sums_t[d][:, 2 + d : 3 + d]
        in_c = gates_t[:, d : d + 1]
        last = rows - 1 if d == 0 else 0
        total = cum_c[last : last + 1, :]
        update = total - cum_c + in_c
        stable = jnp.max(update, axis=0, keepdims=True)
        weighted = keys_f * jnp.exp(update - stable)
        state_out[d] = dot(weighted.astype(BF16), values, TN).astype(BF16)
        edge = mixed[rows - 1 :, :] if d == 0 else mixed[:1, :]
        wide = pack_out.shape[-1]
        pack_out[d, 0:1, :] = edge
        pack_out[d, 1:2, :dk] = jnp.sum(weighted, axis=0, keepdims=True)
        pack_out[d, 1:2, dk:] = jnp.zeros((1, wide - dk), F32)
        pack_out[d, 2:3, :] = jnp.broadcast_to(total, (1, wide))
        pack_out[d, 3:4, :] = jnp.broadcast_to(stable, (1, wide))
        pack_out[d, 4:, :] = jnp.zeros((4, wide), F32)

    def give(o):
        other = lax.rem(me + o, n)
        d = lax.div(me + o, n)
        ids = {"sp": other}
        return (
            pltpu.make_async_remote_copy(state_out.at[d], state_in.at[me], st_ss.at[o], st_rs.at[me], device_id=ids),
            pltpu.make_async_remote_copy(pack_out.at[d], pack_in.at[me], pk_ss.at[o], pk_rs.at[me], device_id=ids),
        )

    def take(o):
        source = lax.rem(me + o, n)
        ids = {"sp": source}
        return (
            pltpu.make_async_remote_copy(state_out.at[0], state_in.at[source], st_ss.at[o], st_rs.at[source], device_id=ids),
            pltpu.make_async_remote_copy(pack_out.at[0], pack_in.at[source], pk_ss.at[o], pk_rs.at[source], device_id=ids),
        )

    def give_all(o, c):
        for copy in give(o):
            copy.start()
        return c

    def take_all(o, c):
        for copy in take(o):
            copy.wait_recv()
        return c

    def give_end(o, c):
        for copy in give(o):
            copy.wait_send()
        return c

    lax.fori_loop(1, n, give_all, 0)
    advance()

    scale = dk ** (-0.5)
    scores = dot(query, keys, NT) * scale
    local = []
    for d in range(2):
        cum_c = sums_t[d][:, 2 + d : 3 + d]
        cum_r = sums[d][2 + d : 3 + d, :]
        in_r = gates[d : d + 1, :]
        allowed = row_id >= col_id if d == 0 else row_id <= col_id
        log_weight = jnp.where(allowed, cum_c - cum_r + in_r, -jnp.inf)
        peak = jnp.max(log_weight, axis=-1, keepdims=True)
        part = scores * jnp.exp(log_weight - peak)
        num = dot(part, values.astype(F32), NN, HIGH)
        local.append((cum_c, peak, num, jnp.sum(part, axis=-1, keepdims=True)))
        advance()

    lax.fori_loop(1, n, take_all, 0)

    before = pack_in[lax.rem(me + n - 1, n), 0:1, :] * jnp.minimum(me, 1).astype(F32)
    behind = pack_in[lax.rem(me + 1, n), 0:1, :] * jnp.minimum(n - 1 - me, 1).astype(F32)
    pos = lax.broadcasted_iota(jnp.int32, mixed.shape, 0)
    prior = jnp.where(pos == 0, before, pltpu.roll(mixed, 1, 0))
    later = jnp.where(pos == rows - 1, behind, pltpu.roll(mixed, rows - 1, 0))
    taps_f = taps[...].astype(F32)
    filtered = taps_f[0:1] * prior + taps_f[1:2] * mixed + taps_f[2:3] * later
    joined[head, :, dv:] = (proj[:, base : base + bw].astype(F32) * filtered).astype(BF16)

    def share(part, o, source):
        columns = pl.ds(part * dv, dv)
        slot = joined.at[source, :, columns]
        return pltpu.make_async_remote_copy(
            slot,
            slot,
            j_ss.at[part, o],
            j_rs.at[part, source],
            device_id={"tp": lax.rem(head + o, t)},
        )

    for o in range(1, t):
        share(1, o, head).start()
    advance()

    summed = None
    query_f = query.astype(F32) * scale
    for d in range(2):
        carry_c[...] = jnp.zeros_like(carry_c)
        carry_n[...] = jnp.zeros_like(carry_n)

        def join(i, peak_in):
            source = i if d == 0 else n - 1 - i
            total = pack_in[source, 2:3, :]
            stable = pack_in[source, 3:4, :]
            new = jnp.maximum(peak_in + total, stable)
            old_w = jnp.exp(peak_in + total - new)
            new_w = jnp.exp(stable - new)
            carry_c[...] = old_w * carry_c[...] + new_w * state_in[source].astype(F32)
            carry_n[...] = old_w * carry_n[...] + new_w * pack_in[source, 1:2, :]
            return new

        peak_in = lax.fori_loop(0, me if d == 0 else n - 1 - me, join, jnp.full((1, dv), LOWEST, F32))
        cum_c, peak, num, den = local[d]
        carried = cum_c + peak_in[:, :1]
        top = jnp.maximum(carried, peak)
        carry_w = jnp.exp(carried - top)
        own_w = jnp.exp(peak - top)
        num = own_w * num + carry_w * dot(query_f, carry_c[...], NN, HIGH)
        den = own_w * den + carry_w * jnp.sum(query_f * carry_n[:, :dk], axis=-1, keepdims=True)
        result = num / jnp.maximum(jnp.abs(den), jnp.exp(-top))
        summed = result if d == 0 else summed + result
        if d == 0:
            advance()
    inverse = lax.rsqrt(jnp.mean(summed * summed, axis=-1, keepdims=True) + EPS)
    joined[head, :, :dv] = (summed * inverse * head_gain[...]).astype(BF16)
    for o in range(1, t):
        share(0, o, head).start()

    lax.fori_loop(done[0] + 1, n - 1, lambda s, c: (ring_step(s, *wo_ring), c)[1], 0)
    ring_last(*wo_ring)
    for part in range(2):
        for o in range(1, t):
            share(part, o, lax.rem(head + o, t)).wait_recv()

    span_j = 2 * dv

    def emit(i, c):
        span = pl.ds(pl.multiple_of(i * width, width), width)
        total = dot(joined[0], wo_all[0:span_j, span], NN)
        for j in range(1, t):
            total += dot(joined[j], wo_all[j * span_j : (j + 1) * span_j, span], NN)
        out[:, span] = total.astype(BF16)
        return c

    lax.fori_loop(0, out.shape[1] // width, emit, 0)
    ring_drain(*w_ring)
    ring_drain(*wo_ring)
    lax.fori_loop(1, n, give_end, 0)
    for part in range(2):
        for o in range(1, t):
            share(part, o, head).wait_send()


def gather_body(
    n,
    t,
    tokens,
    norm_gain,
    w_query,
    w_key,
    w_value,
    w_gates,
    input_bias,
    forget_bias,
    decay_shift,
    head_gain,
    w_conv_b,
    w_conv_c,
    w_conv_in,
    conv_taps,
    w_out,
):
    rows, model = tokens.shape
    dk, dv = w_query.shape[1], w_value.shape[1]
    gates = jnp.transpose(w_gates[..., 0], (2, 1, 0)).reshape(4, model)
    gates = jnp.pad(gates, ((0, 4), (0, 0)))
    depth = w_query.shape[0]
    wide, cols = 2 * dk + dv + 3 * w_conv_b.shape[1], w_out.shape[1]
    hbm = pl.BlockSpec(memory_space=pl.ANY)
    vmem = pl.BlockSpec(memory_space=pltpu.VMEM)
    dma = pltpu.SemaphoreType.DMA
    return pl.pallas_call(
        functools.partial(gather_kernel, n, t, dk, dv),
        out_shape=jax.ShapeDtypeStruct((rows, cols), BF16),
        in_specs=[vmem] * 2 + [hbm] * 7 + [vmem] * 6,
        out_specs=vmem,
        scratch_shapes=[
            pltpu.VMEM((rows, model), BF16),
            pltpu.VMEM((n * depth, wide), BF16),
            pltpu.VMEM((n * w_out.shape[0], cols), BF16),
            pltpu.VMEM((rows, wide), BF16),
            pltpu.VMEM((2, dk, dv), BF16),
            pltpu.VMEM((2, 8, dv), F32),
            pltpu.VMEM((n, dk, dv), BF16),
            pltpu.VMEM((n, 8, dv), F32),
            pltpu.VMEM((dk, dv), F32),
            pltpu.VMEM((1, dv), F32),
            pltpu.VMEM((t, rows, 2 * dv), BF16),
            dma((2, (n - 1) * pieces(depth))),
            dma((2, (n - 1) * pieces(depth))),
            dma((2, (n - 1) * pieces(w_out.shape[0]))),
            dma((2, (n - 1) * pieces(w_out.shape[0]))),
            dma((n,)),
            dma((n,)),
            dma((n,)),
            dma((n,)),
            dma((2, t)),
            dma((2, t)),
            dma((7,)),
            pltpu.VMEM((8, 1), F32),
            pltpu.VMEM((8, rows), F32),
        ],
        compiler_params=pltpu.CompilerParams(
            collective_id=0, has_side_effects=True, vmem_limit_bytes=60 * 1024 * 1024
        ),
    )(
        tokens,
        norm_gain.reshape(1, model),
        w_query,
        w_key,
        w_value,
        w_conv_b,
        w_conv_c,
        w_conv_in,
        w_out,
        gates,
        input_bias,
        forget_bias,
        decay_shift[..., 0],
        head_gain.reshape(1, dv),
        conv_taps,
    )


PAIR = 2
WO_PIECES = 2


def fits(n, t, tokens, norm_gain, w_query, w_key, w_value, *rest):
    w_conv, w_out = rest[5], rest[9]
    depth, dk = w_query.shape
    dv = w_value.shape[1]
    rows = tokens.shape[0]
    even = n % PAIR == 0 and n > PAIR and t == 4
    wide = 2 * dk == dv and w_conv.shape[1] == dv and dv % 128 == 0 and dk % 128 == 0
    deep = (PAIR * depth) % (t * 128) == 0 and rows % 32 == 0 and w_out.shape[0] % (16 * WO_PIECES) == 0
    return even and wide and deep and rows <= depth


def kernel(
    n,
    t,
    dk,
    dv,
    tokens,
    norm_gain,
    w_query,
    w_key,
    w_value,
    w_conv_b,
    w_conv_c,
    w_conv_in,
    w_out,
    w_gates,
    input_bias,
    forget_bias,
    decay_shift,
    head_gain,
    taps,
    out,
    tok,
    nbuf,
    tall,
    wbuf,
    wo_all,
    acc,
    sbuf,
    rbuf,
    proj,
    wg,
    decay,
    state_out,
    pack_out,
    mate_state,
    mate_pack,
    pair_state,
    pair_pack,
    state_in,
    pack_in,
    edge_out,
    edge_in,
    carry_c,
    carry_n,
    local_num,
    joined,
    own_sem,
    tok_sem,
    tk_ss,
    tk_rs,
    tf_ss,
    tf_rs,
    w_ss,
    w_rs,
    rs_ss,
    rs_rs,
    st_ss,
    st_rs,
    pk_ss,
    pk_rs,
    ed_ss,
    ed_rs,
    j_ss,
    j_rs,
    jp_ss,
    jp_rs,
    oz_ss,
    oz_rs,
    oy_ss,
    oy_rs,
):
    me = lax.axis_index("sp")
    head = lax.axis_index("tp")
    lines = n // PAIR
    z = lax.div(me, PAIR)
    y = lax.rem(me, PAIR)
    mate = me + 1 - 2 * y
    core = lax.rem(head, 2)
    core_mate = head + 1 - 2 * core
    x_mate = lax.rem(head + 2, t)
    far_mate = lax.rem(core_mate + 2, t)
    rows, model = tokens.shape
    depth = w_query.shape[0]
    part_k = nbuf.shape[-1]
    chunks = wbuf.shape[0]

    def at_line(line):
        return PAIR * line + y

    rows_at_once = 32

    def load_rows(i):
        span = pl.ds(pl.multiple_of(i * rows_at_once, rows_at_once), rows_at_once)
        return pltpu.make_async_copy(tokens.at[span, :], tok.at[span, :], tok_sem.at[i])

    def load_start(i, c):
        load_rows(i).start()
        return c

    lax.fori_loop(0, rows // rows_at_once, load_start, 0)
    mine = pl.ds(pl.multiple_of(y * depth, depth), depth)
    loads = []
    plan = ((w_query, 0, 0), (w_key, 0, dk), (w_value, 1, 0), (w_conv_c, 2, 0), (w_conv_in, 3, 0), (w_conv_b, 4, 0))
    for part, chunk, offset in plan:
        spot = wbuf.at[chunk, mine, pl.ds(offset, part.shape[1])]
        loads.append(pltpu.make_async_copy(part, spot, own_sem.at[1 + len(loads)]))
    depth_o = w_out.shape[0]
    spot = wo_all.at[pl.ds(pl.multiple_of(me * depth_o, depth_o), depth_o), :]
    loads.append(pltpu.make_async_copy(w_out, spot, own_sem.at[1 + len(loads)]))
    for load in loads:
        load.start()

    edge_in[...] = jnp.zeros_like(edge_in)

    barrier = pltpu.get_barrier_semaphore()

    def greet_sp(o, c):
        pl.semaphore_signal(barrier, inc=1, device_id={"sp": lax.rem(me + o, n)})
        return c

    def greet_tp(o, c):
        pl.semaphore_signal(barrier, inc=1, device_id={"tp": lax.rem(head + o, t)})
        return c

    lax.fori_loop(1, n, greet_sp, 0)
    lax.fori_loop(1, t, greet_tp, 0)

    def norm_rows(i, c):
        load_rows(i).wait()
        span = pl.ds(pl.multiple_of(i * rows_at_once, rows_at_once), rows_at_once)
        values = tok[span, :].astype(F32)
        inverse = lax.rsqrt(jnp.mean(values * values, axis=-1, keepdims=True) + EPS)
        normed = (values * inverse * norm_gain[...]).astype(BF16)
        for b in range(lines * t):
            nbuf[b // t, b % t, span, :] = normed[:, b * part_k : (b + 1) * part_k]
        return c

    lax.fori_loop(0, rows // rows_at_once, norm_rows, 0)
    pl.semaphore_wait(barrier, n + t - 2)

    ups = lines - 1 - z

    half_way = lines // 2
    end_here = 1 - jnp.minimum(z, 1) * jnp.minimum(ups, 1)
    inner_up = jnp.minimum(lax.div(ups, half_way), 1)
    inner_count = inner_up * ups + (1 - inner_up) * z

    def pick(k, near):
        up = jnp.clip(ups - k, 0, 1)
        down_k = k - ups
        if near:
            return up, up * (z + 1 + k) + (1 - up) * (z - 1 - down_k)
        return up, up * (lines - 1 - k) + (1 - up) * down_k

    def token_send(line):
        return pltpu.make_async_remote_copy(
            nbuf.at[line, head], tall.at[z, head], tk_ss.at[line], tk_rs.at[z], device_id={"sp": at_line(line)}
        )

    def token_take(line):
        return pltpu.make_async_remote_copy(
            nbuf.at[line, head], tall.at[line, head], tk_ss.at[line], tk_rs.at[line], device_id={"sp": at_line(line)}
        )

    def token_pass(line, way):
        quarter = (head, head, x_mate)[way]
        there = tall.at[line, quarter]
        return pltpu.make_async_remote_copy(
            there, there, tf_ss.at[way, line], tf_rs.at[way, line], device_id={"tp": (core_mate, x_mate, core_mate)[way]}
        )

    def token_get(line, way):
        quarter = (core_mate, x_mate, far_mate)[way]
        there = tall.at[line, quarter]
        return pltpu.make_async_remote_copy(
            there, there, tf_ss.at[way, line], tf_rs.at[way, line], device_id={"tp": (core_mate, x_mate, core_mate)[way]}
        )

    def send_tokens(k, c):
        _, line = pick(k, False)
        token_send(line).start()
        return c

    lax.fori_loop(0, lines - 1, send_tokens, 0)

    def w_send(chunk):
        there = wbuf.at[chunk, mine, :]
        return pltpu.make_async_remote_copy(there, there, w_ss.at[chunk], w_rs.at[chunk], device_id={"sp": mate})

    def w_take(chunk):
        there = wbuf.at[chunk, pl.ds(pl.multiple_of((1 - y) * depth, depth), depth), :]
        return pltpu.make_async_remote_copy(there, there, w_ss.at[chunk], w_rs.at[chunk], device_id={"sp": mate})

    for load in loads:
        load.wait()
    for chunk in range(chunks):
        w_send(chunk).start()

    tall_o = depth_o // WO_PIECES

    def wo_rows(index, piece):
        return wo_all.at[pl.ds(pl.multiple_of(index * depth_o + piece * tall_o, tall_o), tall_o), :]

    def wo_line(line, piece, way, sem):
        there = wo_rows(at_line(line), piece)
        return pltpu.make_async_remote_copy(
            there, there, oz_ss.at[sem, piece], oz_rs.at[line, piece], device_id={"sp": at_line(z + way)}
        )

    def wo_mate(line, piece):
        there = wo_rows(at_line(line), piece)
        return pltpu.make_async_remote_copy(
            there, there, oy_ss.at[line, piece], oy_rs.at[line, piece], device_id={"sp": mate}
        )

    def wo_mate_take(line, piece):
        there = wo_rows(PAIR * line + 1 - y, piece)
        return pltpu.make_async_remote_copy(
            there, there, oy_ss.at[line, piece], oy_rs.at[line, piece], device_id={"sp": mate}
        )

    def wo_own(way, wanted):
        @pl.when(wanted)
        def _():
            for piece in range(WO_PIECES):
                wo_line(z, piece, way, lines + (way + 1) // 2).start()

    has_up, has_down = z < lines - 1, z > 0
    at_end = jnp.logical_or(z == 0, z == lines - 1)
    upper = z >= half_way

    def wo_outward():
        wo_own(1, jnp.logical_and(upper, has_up))
        wo_own(-1, jnp.logical_and(jnp.logical_not(upper), has_down))

    def wo_inward(ends):
        here = at_end if ends else jnp.logical_not(at_end)
        wo_own(-1, jnp.logical_and(jnp.logical_and(upper, has_down), here))
        wo_own(1, jnp.logical_and(jnp.logical_and(jnp.logical_not(upper), has_up), here))

    def wo_relay(line, wanted, along, across, pieces_now=range(WO_PIECES)):
        @pl.when(jnp.logical_and(wanted, jnp.logical_and(line >= 0, line < lines)))
        def _():
            for piece in pieces_now:
                if along:
                    wo_line(line, piece, 0, line).wait_recv()

                    @pl.when(jnp.logical_and(line < z, has_up))
                    def _():
                        wo_line(line, piece, 1, line).start()

                    @pl.when(jnp.logical_and(line > z, has_down))
                    def _():
                        wo_line(line, piece, -1, line).start()

                if across:
                    wo_mate(line, piece).start()

    inner_way = 2 * inner_up - 1

    def wo_first(pieces_now, along=True, across=True, wanted=True):
        wo_relay(z - inner_way * (1 - 2 * end_here), wanted, along, across, pieces_now)

    def wo_second(along, across):
        wo_relay(z + inner_way, jnp.logical_not(at_end), along, across)

    def wo_rest(away, pieces_now, along=True, across=True, wanted=True):
        wo_relay(z - away, wanted, along, across, pieces_now)
        wo_relay(z + away, wanted, along, across, pieces_now)

    for piece in range(WO_PIECES):
        wo_mate(z, piece).start()
    wo_inward(True)

    wg[...] = jnp.zeros_like(wg)
    wg[0:2, :] = w_gates[0]
    wg[2:4, :] = w_gates[1]
    decay[...] = jnp.zeros_like(decay)
    decay[1:2, :] = decay_shift[0]
    decay[3:4, :] = decay_shift[1]
    gates = None
    for b in range(lines * t):
        piece = dot(wg[:, b * part_k : (b + 1) * part_k], nbuf[b // t, b % t], NT)
        gates = piece if b == 0 else gates + piece
    gate_id = lax.broadcasted_iota(jnp.int32, gates.shape, 0)
    offsets = (input_bias[0, 0], forget_bias[0, 0], input_bias[0, 1], forget_bias[0, 1])
    for i, offset in enumerate(offsets):
        gates = jnp.where(gate_id == i, gates + offset, gates)
    forget = jnp.minimum(gates, 0.0) - jnp.log1p(jnp.exp(-jnp.abs(gates))) + decay[...]
    row_id = lax.broadcasted_iota(jnp.int32, (rows, rows), 0)
    col_id = lax.broadcasted_iota(jnp.int32, (rows, rows), 1)
    upto = (row_id <= col_id).astype(F32)
    after = (row_id >= col_id).astype(F32)
    sums = (dot(forget, upto, NN, HIGH), dot(forget, after, NN, HIGH))
    gates_t = gates.T
    sums_t = (sums[0].T, sums[1].T)

    def relay_direct(k, c):
        _, line = pick(k, True)
        token_take(line).wait_recv()
        token_pass(line, 1).start()
        token_pass(line, 0).start()
        return c

    def relay_across(k, c):
        _, line = pick(k, True)
        token_get(line, 1).wait_recv()
        token_pass(line, 2).start()
        return c

    def tokens_ready(k, c):
        _, line = pick(k, True)
        token_get(line, 0).wait_recv()
        token_get(line, 2).wait_recv()
        return c

    lax.fori_loop(0, lines - 1, relay_direct, 0)
    wo_outward()
    wo_inward(False)
    lax.fori_loop(0, lines - 1, relay_across, 0)
    lax.fori_loop(0, lines - 1, tokens_ready, 0)
    def parts_of(chunk):
        if isinstance(chunk, int) and chunk == chunks - 1:
            return ((0, rows // 2, chunk), (rows // 2, rows // 2, chunks))
        return ((0, rows, chunk),)

    def hop(chunk, part, k, up, line):
        first, count, sem = part
        last = (1 - up) * (1 - jnp.minimum(jnp.abs(z - line) - 1, 1))
        slot = line + last * (lines - line)
        return pltpu.make_async_remote_copy(
            sbuf.at[chunk, k, pl.ds(first, count)],
            rbuf.at[chunk, slot, pl.ds(first, count)],
            rs_ss.at[sem, k],
            rs_rs.at[sem, slot],
            device_id={"sp": at_line(z + 2 * up - 1)},
        )

    def arrived(chunk, part, slot):
        first, count, sem = part
        return pltpu.make_async_remote_copy(
            sbuf.at[chunk, 0, pl.ds(first, count)],
            rbuf.at[chunk, slot, pl.ds(first, count)],
            rs_ss.at[sem, 0],
            rs_rs.at[sem, slot],
            device_id={"sp": me},
        )

    def product(source, line, chunk, part):
        span = pl.ds(part[0], part[1])
        total = dot(source[line, 0, span, :], wbuf[chunk, 0:part_k, :], NN)
        for q in range(1, t):
            total += dot(source[line, q, span, :], wbuf[chunk, q * part_k : (q + 1) * part_k, :], NN)
        return total

    def add_along(chunk, part, slot, up, line):
        span = pl.ds(part[0], part[1])
        acc[span, :] = product(tall, line, chunk, part)
        before = up * jnp.minimum(z, 1) + (1 - up) * jnp.minimum(ups, 1)

        @pl.when(before == 1)
        def _():
            arrived(chunk, part, line).wait_recv()
            sbuf[chunk, slot, span, :] = (acc[span, :] + rbuf[chunk, line, span, :].astype(F32)).astype(BF16)

        @pl.when(before == 0)
        def _():
            sbuf[chunk, slot, span, :] = acc[span, :].astype(BF16)

        hop(chunk, part, slot, up, line).start()

    def inward_where(runs, chunk):
        @pl.when(runs == 1)
        def _():
            w_take(chunk).wait_recv()

        for part in parts_of(chunk):

            def one(k, c):
                line = inner_up * (lines - 1 - k) + (1 - inner_up) * k
                add_along(chunk, part, k, inner_up, line)
                return c

            lax.fori_loop(0, runs * inner_count, one, 0)

    def inward(end_chunk, mid_chunk):
        end_runs, mid_runs = end_chunk < chunks, mid_chunk >= 0
        if end_runs and mid_runs and max(end_chunk, mid_chunk) < chunks - 1:
            inward_where(1, end_here * end_chunk + (1 - end_here) * mid_chunk)
            return
        if end_runs:
            inward_where(end_here, end_chunk)
        if mid_runs:
            inward_where(1 - end_here, mid_chunk)

    def outward(chunk):
        for part in parts_of(chunk):

            def one(k, c):
                line = (1 - inner_up) * (lines - 1 - k) + inner_up * k
                add_along(chunk, part, inner_count + k, 1 - inner_up, line)
                return c

            lax.fori_loop(0, lines - 1 - inner_count, one, 0)

    def own_part(chunk, part):
        span = pl.ds(part[0], part[1])
        acc[span, :] = product(nbuf, z, chunk, part)

        @pl.when(has_down)
        def _():
            arrived(chunk, part, z).wait_recv()
            acc[span, :] += rbuf[chunk, z, span, :].astype(F32)

        @pl.when(has_up)
        def _():
            arrived(chunk, part, lines).wait_recv()
            acc[span, :] += rbuf[chunk, lines, span, :].astype(F32)

    def own_chunk(chunk):
        own_part(chunk, parts_of(chunk)[0])
        proj[chunk] = acc[...].astype(BF16)

    inward(0, -1)
    inward(1, -1)
    inward(2, 0)
    wo_first((0,))
    wo_second(True, False)
    inward(3, 1)
    wo_first(range(1, WO_PIECES), True, False)
    wo_first(range(1, WO_PIECES), False, True, at_end)
    outward(0)
    own_chunk(0)
    inward(chunks, 2)
    outward(1)
    own_chunk(1)

    keys_f = proj[0, :, dk:].astype(F32)
    wide = pack_out.shape[-1]
    for d in range(2):
        cum_c = sums_t[d][:, 2 * d + 1 : 2 * d + 2]
        in_c = gates_t[:, 2 * d : 2 * d + 1]
        last = rows - 1 if d == 0 else 0
        total = cum_c[last : last + 1, :]
        update = total - cum_c + in_c
        stable = jnp.max(update, axis=0, keepdims=True)
        weighted = keys_f * jnp.exp(update - stable)
        state_out[d] = dot(weighted.astype(BF16), proj[1], TN).astype(BF16)
        pack_out[d, 0:1, :dk] = jnp.sum(weighted, axis=0, keepdims=True)
        pack_out[d, 0:1, dk:] = jnp.zeros((1, wide - dk), F32)
        pack_out[d, 1:2, :] = jnp.broadcast_to(total, (1, wide))
        pack_out[d, 2:3, :] = jnp.broadcast_to(stable, (1, wide))
        pack_out[d, 3:, :] = jnp.zeros((5, wide), F32)

    def swap_states():
        return (
            pltpu.make_async_remote_copy(state_out, mate_state, st_ss.at[2], st_rs.at[2], device_id={"sp": mate}),
            pltpu.make_async_remote_copy(pack_out, mate_pack, pk_ss.at[2], pk_rs.at[2], device_id={"sp": mate}),
        )

    for copy in swap_states():
        copy.start()
    wo_first(range(1, WO_PIECES), False, True, jnp.logical_not(at_end))
    wo_second(False, True)
    wo_rest(2, (0,), True, True)
    wo_rest(2, range(1, WO_PIECES), True, False)
    wo_rest(2, range(1, WO_PIECES), False, True, at_end)

    d_in, d_out = 1 - inner_up, inner_up

    def chain(d, way):
        ids = {"sp": at_line(z + way)}
        return (
            pltpu.make_async_remote_copy(pair_state.at[d], state_in.at[d], st_ss.at[d], st_rs.at[d], device_id=ids),
            pltpu.make_async_remote_copy(pair_pack.at[d], pack_in.at[d], pk_ss.at[d], pk_rs.at[d], device_id=ids),
        )

    def chain_add(d):
        for copy in chain(d, 0):
            copy.wait_recv()
        total, stable, first_w, second_w = blend(pack_in[d], pair_pack[d])
        joint = first_w[:, :1] * state_in[d].astype(F32) + second_w[:, :1] * pair_state[d].astype(F32)
        pair_state[d] = joint.astype(BF16)
        pair_pack[d, 0:1, :] = first_w * pack_in[d, 0:1, :] + second_w * pair_pack[d, 0:1, :]
        pair_pack[d, 1:2, :] = total
        pair_pack[d, 2:3, :] = stable

    def chain_from_end():
        @pl.when(at_end)
        def _():
            for copy in chain(d_in, inner_way):
                copy.start()

    def chain_inward():
        @pl.when(jnp.logical_not(at_end))
        def _():
            chain_add(d_in)
            for copy in chain(d_in, inner_way):
                copy.start()

    def chain_outward():
        @pl.when(jnp.logical_not(at_end))
        def _():
            chain_add(d_out)
            for copy in chain(d_out, -inner_way):
                copy.start()

        @pl.when(at_end)
        def _():
            for copy in chain(d_out, 0):
                copy.wait_recv()

    def blend(first, second):
        total = first[1:2, :] + second[1:2, :]
        moved = first[2:3, :] + second[1:2, :]
        stable = jnp.maximum(moved, second[2:3, :])
        return total, stable, jnp.exp(moved - stable), jnp.exp(second[2:3, :] - stable)

    def pair_up():
        for copy in swap_states():
            copy.wait_recv()
        own_first = (1 - y).astype(F32)
        for d in range(2):
            lead = own_first if d == 0 else 1.0 - own_first
            mine_p, other_p = pack_out[d], mate_pack[d]
            first = lead * mine_p + (1.0 - lead) * other_p
            second = lead * other_p + (1.0 - lead) * mine_p
            total, stable, first_w, second_w = blend(first, second)
            mine_w = lead * first_w + (1.0 - lead) * second_w
            other_w = lead * second_w + (1.0 - lead) * first_w
            joint = mine_w * state_out[d].astype(F32) + other_w * mate_state[d].astype(F32)
            pair_state[d] = joint.astype(BF16)
            pair_pack[d, 0:1, :] = mine_w * mine_p[0:1, :] + other_w * other_p[0:1, :]
            pair_pack[d, 1:2, :] = total
            pair_pack[d, 2:3, :] = stable
            pair_pack[d, 3:, :] = jnp.zeros((5, wide), F32)

    inward(chunks, 3)
    pair_up()
    chain_from_end()
    inward(4, -1)
    outward(2)
    for away in range(3, lines):
        wo_rest(away, (0,))
    own_chunk(2)

    scale = dk ** (-0.5)
    scores = dot(proj[0, :, :dk], proj[0, :, dk:], NT) * scale
    local = []
    for d in range(2):
        cum_c = sums_t[d][:, 2 * d + 1 : 2 * d + 2]
        cum_r = sums[d][2 * d + 1 : 2 * d + 2, :]
        in_r = gates[2 * d : 2 * d + 1, :]
        allowed = row_id >= col_id if d == 0 else row_id <= col_id
        log_weight = jnp.where(allowed, cum_c - cum_r + in_r, -jnp.inf)
        peak = jnp.max(log_weight, axis=-1, keepdims=True)
        part = scores * jnp.exp(log_weight - peak)
        local_num[d] = dot(part.astype(BF16), proj[1], NN)
        local.append((cum_c, peak, jnp.sum(part, axis=-1, keepdims=True)))

    chain_inward()
    inward(chunks, 4)
    outward(3)
    own_chunk(3)

    mixed = (proj[2].astype(F32) * proj[3].astype(F32)).astype(BF16).astype(F32)
    edge_out[0, 0:1, :] = mixed[rows - 1 :, :]
    edge_out[1, 0:1, :] = mixed[:1, :]
    edge_out[0, 1:, :] = jnp.zeros((7, dv), F32)
    edge_out[1, 1:, :] = jnp.zeros((7, dv), F32)

    def edge(way):
        other = me + 1 if way == 0 else me - 1
        return pltpu.make_async_remote_copy(
            edge_out.at[way], edge_in.at[way], ed_ss.at[way], ed_rs.at[way], device_id={"sp": other}
        )

    later_exists, prior_exists = me < n - 1, me > 0

    @pl.when(later_exists)
    def _():
        edge(0).start()

    @pl.when(prior_exists)
    def _():
        edge(1).start()

    wo_rest(2, range(1, WO_PIECES), False, True, jnp.logical_not(at_end))
    for away in range(3, lines):
        wo_rest(away, range(1, WO_PIECES))
    chain_outward()
    outward(4)

    half_rows = rows // 2

    def joined_part(part, source, way):
        columns = pl.ds(part * dv, dv)
        if way == 0:
            return joined.at[source, :, columns]
        return joined.at[source, pl.ds((way - 1) * half_rows, half_rows), columns]

    others = (core_mate, x_mate, far_mate)

    def share(part, way, source):
        slot = joined_part(part, source, way)
        return pltpu.make_async_remote_copy(
            slot, slot, j_ss.at[part, way], j_rs.at[part, way], device_id={"tp": others[way]}
        )

    def share_pass(part, way, source):
        slot = joined_part(part, source, way)
        return pltpu.make_async_remote_copy(
            slot, slot, jp_ss.at[part, way - 1], jp_rs.at[part, way - 1], device_id={"tp": core_mate}
        )

    def share_start(part):
        for way in (1, 2, 0):
            share(part, way, head).start()

    def share_relay(part):
        for way in (1, 2):
            share(part, way, others[way]).wait_recv()
            share_pass(part, way, others[way]).start()

    def share_wait(part):
        share(part, 0, core_mate).wait_recv()
        for way in (1, 2):
            share_pass(part, way, others[3 - way]).wait_recv()

    def share_end(part):
        for way in range(3):
            share(part, way, head).wait_send()
        for way in (1, 2):
            share_pass(part, way, others[way]).wait_send()

    summed = None
    query_f = proj[0, :, :dk].astype(F32) * scale
    for d in range(2):
        carry_c[...] = jnp.zeros_like(carry_c)
        carry_n[...] = jnp.zeros_like(carry_n)

        def merge(state, pack, peak_in):
            total = pack[1:2, :]
            stable = pack[2:3, :]
            new = jnp.maximum(peak_in + total, stable)
            old_w = jnp.exp(peak_in + total - new)
            new_w = jnp.exp(stable - new)
            carry_c[...] = old_w * carry_c[...] + new_w * state.astype(F32)
            carry_n[...] = old_w * carry_n[...] + new_w * pack[0:1, :]
            return new

        def join(i, peak_in):
            return merge(state_in[d], pack_in[d], peak_in)

        def join_mate(i, peak_in):
            return merge(mate_state[d], mate_pack[d], peak_in)

        peak_in = lax.fori_loop(0, jnp.minimum(z if d == 0 else ups, 1), join, jnp.full((1, dv), LOWEST, F32))
        peak_in = lax.fori_loop(0, y if d == 0 else 1 - y, join_mate, peak_in)
        cum_c, peak, den = local[d]
        carried = cum_c + peak_in[:, :1]
        top = jnp.maximum(carried, peak)
        carry_w = jnp.exp(carried - top)
        own_w = jnp.exp(peak - top)
        num = own_w * local_num[d] + carry_w * dot(query_f.astype(BF16), carry_c[...].astype(BF16), NN)
        den = own_w * den + carry_w * jnp.sum(query_f * carry_n[:, :dk], axis=-1, keepdims=True)
        result = num / jnp.maximum(jnp.abs(den), jnp.exp(-top))
        summed = result if d == 0 else summed + result
    inverse = lax.rsqrt(jnp.mean(summed * summed, axis=-1, keepdims=True) + EPS)
    joined[head, :, :dv] = (summed * inverse * head_gain[...]).astype(BF16)
    share_start(0)

    @pl.when(prior_exists)
    def _():
        edge(0).wait_recv()

    @pl.when(later_exists)
    def _():
        edge(1).wait_recv()

    mixed = (proj[2].astype(F32) * proj[3].astype(F32)).astype(BF16).astype(F32)
    pos = lax.broadcasted_iota(jnp.int32, mixed.shape, 0)
    prior = jnp.where(pos == 0, edge_in[0, 0:1, :], pltpu.roll(mixed, 1, 0))
    later = jnp.where(pos == rows - 1, edge_in[1, 0:1, :], pltpu.roll(mixed, rows - 1, 0))
    taps_f = taps[...].astype(F32)
    local_num[0] = taps_f[0:1] * prior + taps_f[1:2] * mixed + taps_f[2:3] * later
    for i, part in enumerate(parts_of(chunks - 1)):
        span = pl.ds(part[0], part[1])
        own_part(chunks - 1, part)
        outer = acc[span, :].astype(BF16).astype(F32)
        joined[head, span, dv:] = (outer * local_num[0, span, :]).astype(BF16)
        share(1, 1 + i, head).start()
    share(1, 0, head).start()
    share_relay(0)
    share_relay(1)

    for line in range(lines):
        for piece in range(WO_PIECES):
            wo_mate_take(line, piece).wait_recv()
    for part in range(2):
        share_wait(part)

    span_j = 2 * dv
    width = 256

    def emit(i, c):
        span = pl.ds(pl.multiple_of(i * width, width), width)
        total = dot(joined[0], wo_all[0:span_j, span], NN)
        for j in range(1, t):
            total += dot(joined[j], wo_all[j * span_j : (j + 1) * span_j, span], NN)
        out[:, span] = total.astype(BF16)
        return c

    lax.fori_loop(0, out.shape[1] // width, emit, 0)

    def token_end(k, c):
        _, line = pick(k, False)
        token_send(line).wait_send()
        for way in range(3):
            token_pass(line, way).wait_send()
        inner = jnp.clip(inner_count - k, 0, 1)
        up = inner * inner_up + (1 - inner) * (1 - inner_up)
        step = inner * k + (1 - inner) * (k - inner_count)
        line = up * (lines - 1 - step) + (1 - up) * step
        for chunk in range(chunks):
            for part in parts_of(chunk):
                hop(chunk, part, k, up, line).wait_send()
        return c

    lax.fori_loop(0, lines - 1, token_end, 0)
    for chunk in range(chunks):
        w_send(chunk).wait_send()
    for copy in swap_states():
        copy.wait_send()

    @pl.when(at_end)
    def _():
        for copy in chain(d_in, inner_way):
            copy.wait_send()

    @pl.when(jnp.logical_not(at_end))
    def _():
        for copy in chain(d_in, inner_way) + chain(d_out, -inner_way):
            copy.wait_send()


    @pl.when(later_exists)
    def _():
        edge(0).wait_send()

    @pl.when(prior_exists)
    def _():
        edge(1).wait_send()

    for part in range(2):
        share_end(part)
    for piece in range(WO_PIECES):

        @pl.when(has_up)
        def _():
            wo_line(z, piece, 1, lines + 1).wait_send()

        @pl.when(has_down)
        def _():
            wo_line(z, piece, -1, lines).wait_send()

        for line in range(lines):

            @pl.when(jnp.logical_and(z > line, has_up))
            def _():
                wo_line(line, piece, 1, line).wait_send()

            @pl.when(jnp.logical_and(z < line, has_down))
            def _():
                wo_line(line, piece, -1, line).wait_send()

            wo_mate(line, piece).wait_send()


def body(
    n,
    t,
    tokens,
    norm_gain,
    w_query,
    w_key,
    w_value,
    w_gates,
    input_bias,
    forget_bias,
    decay_shift,
    head_gain,
    w_conv_b,
    w_conv_c,
    w_conv_in,
    conv_taps,
    w_out,
):
    rows, model = tokens.shape
    depth, dk = w_query.shape
    dv = w_value.shape[1]
    lines = n // PAIR
    chunks = 5
    part_k = PAIR * depth // t
    cols = w_out.shape[1]
    gates = jnp.transpose(w_gates[..., 0], (1, 2, 0))
    hbm = pl.BlockSpec(memory_space=pl.ANY)
    vmem = pl.BlockSpec(memory_space=pltpu.VMEM)
    smem = pl.BlockSpec(memory_space=pltpu.SMEM)
    dma = pltpu.SemaphoreType.DMA
    return pl.pallas_call(
        functools.partial(kernel, n, t, dk, dv),
        out_shape=jax.ShapeDtypeStruct((rows, cols), BF16),
        in_specs=[hbm, vmem] + [hbm] * 7 + [vmem] + [smem] * 2 + [vmem] * 3,
        out_specs=vmem,
        scratch_shapes=[
            pltpu.VMEM((rows, model), BF16),
            pltpu.VMEM((lines, t, rows, part_k), BF16),
            pltpu.VMEM((lines, t, rows, part_k), BF16),
            pltpu.VMEM((chunks, PAIR * depth, dv), BF16),
            pltpu.VMEM((n * w_out.shape[0], cols), BF16),
            pltpu.VMEM((rows, dv), F32),
            pltpu.VMEM((chunks, lines - 1, rows, dv), BF16),
            pltpu.VMEM((chunks, lines + 1, rows, dv), BF16),
            pltpu.VMEM((chunks, rows, dv), BF16),
            pltpu.VMEM((8, model), BF16),
            pltpu.VMEM((8, rows), F32),
            pltpu.VMEM((2, dk, dv), BF16),
            pltpu.VMEM((2, 8, dv), F32),
            pltpu.VMEM((2, dk, dv), BF16),
            pltpu.VMEM((2, 8, dv), F32),
            pltpu.VMEM((2, dk, dv), BF16),
            pltpu.VMEM((2, 8, dv), F32),
            pltpu.VMEM((2, dk, dv), BF16),
            pltpu.VMEM((2, 8, dv), F32),
            pltpu.VMEM((2, 8, dv), F32),
            pltpu.VMEM((2, 8, dv), F32),
            pltpu.VMEM((dk, dv), F32),
            pltpu.VMEM((1, dv), F32),
            pltpu.VMEM((2, rows, dv), F32),
            pltpu.VMEM((t, rows, 2 * dv), BF16),
            dma((8,)),
            dma((rows // 32,)),
            dma((lines,)),
            dma((lines,)),
            dma((3, lines)),
            dma((3, lines)),
            dma((chunks,)),
            dma((chunks,)),
            dma((chunks + 1, lines - 1)),
            dma((chunks + 1, lines + 1)),
            dma((3,)),
            dma((3,)),
            dma((3,)),
            dma((3,)),
            dma((2,)),
            dma((2,)),
            dma((2, 3)),
            dma((2, 3)),
            dma((2, 2)),
            dma((2, 2)),
            dma((lines + 2, WO_PIECES)),
            dma((lines, WO_PIECES)),
            dma((lines, WO_PIECES)),
            dma((lines, WO_PIECES)),
        ],
        compiler_params=pltpu.CompilerParams(
            collective_id=0, has_side_effects=True, vmem_limit_bytes=60 * 1024 * 1024
        ),
    )(
        tokens,
        norm_gain.reshape(1, model),
        w_query,
        w_key,
        w_value,
        w_conv_b,
        w_conv_c,
        w_conv_in,
        w_out,
        gates,
        input_bias.T,
        forget_bias.T,
        jnp.swapaxes(decay_shift, 1, 2),
        head_gain.reshape(1, dv),
        conv_taps,
    )


def solution(mesh):
    placed = (
        P("sp", None),
        P(),
        P("sp", "tp"),
        P("sp", "tp"),
        P("sp", "tp"),
        P(None, None, None, "tp"),
        P(None, "tp"),
        P(None, "tp"),
        P(None, "sp", "tp"),
        P("tp"),
        P("sp", "tp"),
        P("sp", "tp"),
        P("sp", "tp"),
        P(None, "tp"),
        P("sp", "tp"),
    )
    n, t = mesh.shape["sp"], mesh.shape["tp"]

    def step(*args):
        form = body if fits(n, t, *args) else gather_body
        return form(n, t, *args)

    return jax.shard_map(step, mesh=mesh, in_specs=placed, out_specs=P("sp", "tp"), check_vma=False)
```

```python
import functools

import jax
import jax.numpy as jnp
from jax import lax
from jax.experimental import pallas as pl
from jax.experimental.pallas import tpu as pltpu
from jax.sharding import PartitionSpec as P

EPS = 1e-06
HIGH = lax.Precision.HIGHEST
LOWEST = -1e30
PIECES = 4
F32 = jnp.float32
BF16 = jnp.bfloat16


def dot(a, b, dims, precision=None):
    return lax.dot_general(a, b, (dims, ((), ())), precision=precision, preferred_element_type=F32)


NN = ((1,), (0,))
NT = ((1,), (1,))
TN = ((0,), (0,))


def ring_place(index, n):
    odd = lax.rem(index, 2)
    half = lax.div(index, 2)
    return (1 - odd) * half + odd * (n - 1 - half)


def ring_index(place, n):
    late = lax.div(place, n // 2)
    return (1 - late) * (2 * place) + late * (2 * (n - 1 - place) + 1)


def pieces(depth):
    return max(1, min(PIECES, depth // 16))


def gather_kernel(
    n,
    t,
    dk,
    dv,
    tokens,
    norm_gain,
    w_query,
    w_key,
    w_value,
    w_conv_b,
    w_conv_c,
    w_conv_in,
    w_out,
    w_gates,
    input_bias,
    forget_bias,
    decay_shift,
    head_gain,
    taps,
    out,
    normed,
    w_all,
    wo_all,
    proj,
    state_out,
    pack_out,
    state_in,
    pack_in,
    carry_c,
    carry_n,
    joined,
    w_ss,
    w_rs,
    wo_ss,
    wo_rs,
    st_ss,
    st_rs,
    pk_ss,
    pk_rs,
    j_ss,
    j_rs,
    own_sem,
    gate_bias,
    decay,
):
    me = lax.axis_index("sp")
    head = lax.axis_index("tp")
    place = ring_place(me, n)
    right = ring_index(lax.rem(place + 1, n), n)
    left = ring_index(lax.rem(place + n - 1, n), n)
    rows = tokens.shape[0]

    parts = (w_query, w_key, w_value, w_conv_b, w_conv_c, w_conv_in)
    copies = []
    offset = 0
    for part in parts:
        depth, cols = part.shape
        spot = w_all.at[pl.ds(pl.multiple_of(me * depth, depth), depth), pl.ds(offset, cols)]
        copies.append(pltpu.make_async_copy(part, spot, own_sem.at[len(copies)]))
        offset += cols
    depth_o = w_out.shape[0]
    spot = wo_all.at[pl.ds(pl.multiple_of(me * depth_o, depth_o), depth_o), :]
    copies.append(pltpu.make_async_copy(w_out, spot, own_sem.at[len(copies)]))
    for copy in copies:
        copy.start()

    barrier = pltpu.get_barrier_semaphore()

    def greet_sp(o, c):
        pl.semaphore_signal(barrier, inc=1, device_id={"sp": lax.rem(me + o, n)})
        return c

    def greet_tp(o, c):
        pl.semaphore_signal(barrier, inc=1, device_id={"tp": lax.rem(head + o, t)})
        return c

    lax.fori_loop(1, n, greet_sp, 0)
    lax.fori_loop(1, t, greet_tp, 0)
    pl.semaphore_wait(barrier, n + t - 2)

    def hop(depth, whole, ss, rs, way, step, piece):
        width = whole.shape[1]
        half, tall = width // 2, depth // pieces(depth)
        holder = ring_index(lax.rem(place + (n + step if way else n - step), n), n)
        columns = pl.ds(way * half, half)
        there = whole.at[pl.ds(pl.multiple_of(holder * depth + piece * tall, tall), tall), columns]
        turn = step * pieces(depth) + piece
        return pltpu.make_async_remote_copy(
            src_ref=there,
            dst_ref=there,
            send_sem=ss.at[way, turn],
            recv_sem=rs.at[way, turn],
            device_id={"sp": left if way else right},
        )

    def ring_start(*ring):
        for piece in range(pieces(ring[0])):
            for way in range(2):
                hop(*ring, way, 0, piece).start()

    def ring_step(step, *ring):
        for piece in range(pieces(ring[0])):
            for way in range(2):
                hop(*ring, way, step - 1, piece).wait_recv()
                hop(*ring, way, step, piece).start()

    def ring_last(*ring):
        for piece in range(pieces(ring[0])):
            for way in range(2):
                hop(*ring, way, n - 2, piece).wait_recv()

    def ring_drain(*ring):
        def drain(step, c):
            for piece in range(pieces(ring[0])):
                for way in range(2):
                    hop(*ring, way, step, piece).wait_send()
            return c

        lax.fori_loop(0, n - 1, drain, 0)

    w_ring = (w_query.shape[0], w_all, w_ss, w_rs)
    wo_ring = (depth_o, wo_all, wo_ss, wo_rs)
    for copy in copies:
        copy.wait()
    ring_start(*w_ring)

    gate_bias[...] = jnp.zeros_like(gate_bias)
    gate_bias[0:2, :] = input_bias[...]
    gate_bias[2:4, :] = forget_bias[...]
    decay[...] = jnp.zeros_like(decay)
    decay[2:4, :] = decay_shift[...]

    chunk = 32

    def norm_rows(i, c):
        span = pl.ds(pl.multiple_of(i * chunk, chunk), chunk)
        values = tokens[span, :].astype(F32)
        inverse = lax.rsqrt(jnp.mean(values * values, axis=-1, keepdims=True) + EPS)
        normed[span, :] = (values * inverse * norm_gain[...]).astype(BF16)
        return c

    lax.fori_loop(0, rows // chunk, norm_rows, 0)

    gates = dot(w_gates[...], normed[...], NT) + gate_bias[...]
    forget = jnp.minimum(gates, 0.0) - jnp.log1p(jnp.exp(-jnp.abs(gates))) + decay[...]
    row_id = lax.broadcasted_iota(jnp.int32, (rows, rows), 0)
    col_id = lax.broadcasted_iota(jnp.int32, (rows, rows), 1)
    upto = (row_id <= col_id).astype(F32)
    after = (row_id >= col_id).astype(F32)
    sums = (dot(forget, upto, NN, HIGH), dot(forget, after, NN, HIGH))
    gates_t = gates.T
    sums_t = (sums[0].T, sums[1].T)

    lax.fori_loop(1, n - 1, lambda s, c: (ring_step(s, *w_ring), c)[1], 0)
    ring_start(*wo_ring)
    ring_last(*w_ring)
    done = [0]

    def advance():
        if done[0] + 1 < n - 1:
            done[0] += 1
            ring_step(done[0], *wo_ring)

    width = 256

    def project(i, c):
        span = pl.ds(pl.multiple_of(i * width, width), width)
        proj[:, span] = dot(normed[...], w_all[:, span], NN).astype(BF16)
        return c

    lax.fori_loop(0, proj.shape[1] // width, project, 0)

    query = proj[:, :dk]
    keys = proj[:, dk : 2 * dk]
    values = proj[:, 2 * dk : 2 * dk + dv]
    base = 2 * dk + dv
    bw = (proj.shape[1] - base) // 3
    mixed = (proj[:, base + bw : base + 2 * bw].astype(F32) * proj[:, base + 2 * bw :].astype(F32)).astype(BF16).astype(F32)

    keys_f = keys.astype(F32)
    totals = []
    for d in range(2):
        cum_c = sums_t[d][:, 2 + d : 3 + d]
        in_c = gates_t[:, d : d + 1]
        last = rows - 1 if d == 0 else 0
        total = cum_c[last : last + 1, :]
        update = total - cum_c + in_c
        stable = jnp.max(update, axis=0, keepdims=True)
        weighted = keys_f * jnp.exp(update - stable)
        state_out[d] = dot(weighted.astype(BF16), values, TN).astype(BF16)
        edge = mixed[rows - 1 :, :] if d == 0 else mixed[:1, :]
        wide = pack_out.shape[-1]
        pack_out[d, 0:1, :] = edge
        pack_out[d, 1:2, :dk] = jnp.sum(weighted, axis=0, keepdims=True)
        pack_out[d, 1:2, dk:] = jnp.zeros((1, wide - dk), F32)
        pack_out[d, 2:3, :] = jnp.broadcast_to(total, (1, wide))
        pack_out[d, 3:4, :] = jnp.broadcast_to(stable, (1, wide))
        pack_out[d, 4:, :] = jnp.zeros((4, wide), F32)

    def give(o):
        other = lax.rem(me + o, n)
        d = lax.div(me + o, n)
        ids = {"sp": other}
        return (
            pltpu.make_async_remote_copy(state_out.at[d], state_in.at[me], st_ss.at[o], st_rs.at[me], device_id=ids),
            pltpu.make_async_remote_copy(pack_out.at[d], pack_in.at[me], pk_ss.at[o], pk_rs.at[me], device_id=ids),
        )

    def take(o):
        source = lax.rem(me + o, n)
        ids = {"sp": source}
        return (
            pltpu.make_async_remote_copy(state_out.at[0], state_in.at[source], st_ss.at[o], st_rs.at[source], device_id=ids),
            pltpu.make_async_remote_copy(pack_out.at[0], pack_in.at[source], pk_ss.at[o], pk_rs.at[source], device_id=ids),
        )

    def give_all(o, c):
        for copy in give(o):
            copy.start()
        return c

    def take_all(o, c):
        for copy in take(o):
            copy.wait_recv()
        return c

    def give_end(o, c):
        for copy in give(o):
            copy.wait_send()
        return c

    lax.fori_loop(1, n, give_all, 0)
    advance()

    scale = dk ** (-0.5)
    scores = dot(query, keys, NT) * scale
    local = []
    for d in range(2):
        cum_c = sums_t[d][:, 2 + d : 3 + d]
        cum_r = sums[d][2 + d : 3 + d, :]
        in_r = gates[d : d + 1, :]
        allowed = row_id >= col_id if d == 0 else row_id <= col_id
        log_weight = jnp.where(allowed, cum_c - cum_r + in_r, -jnp.inf)
        peak = jnp.max(log_weight, axis=-1, keepdims=True)
        part = scores * jnp.exp(log_weight - peak)
        num = dot(part, values.astype(F32), NN, HIGH)
        local.append((cum_c, peak, num, jnp.sum(part, axis=-1, keepdims=True)))
        advance()

    lax.fori_loop(1, n, take_all, 0)

    before = pack_in[lax.rem(me + n - 1, n), 0:1, :] * jnp.minimum(me, 1).astype(F32)
    behind = pack_in[lax.rem(me + 1, n), 0:1, :] * jnp.minimum(n - 1 - me, 1).astype(F32)
    pos = lax.broadcasted_iota(jnp.int32, mixed.shape, 0)
    prior = jnp.where(pos == 0, before, pltpu.roll(mixed, 1, 0))
    later = jnp.where(pos == rows - 1, behind, pltpu.roll(mixed, rows - 1, 0))
    taps_f = taps[...].astype(F32)
    filtered = taps_f[0:1] * prior + taps_f[1:2] * mixed + taps_f[2:3] * later
    joined[head, :, dv:] = (proj[:, base : base + bw].astype(F32) * filtered).astype(BF16)

    def share(part, o, source):
        columns = pl.ds(part * dv, dv)
        slot = joined.at[source, :, columns]
        return pltpu.make_async_remote_copy(
            slot,
            slot,
            j_ss.at[part, o],
            j_rs.at[part, source],
            device_id={"tp": lax.rem(head + o, t)},
        )

    for o in range(1, t):
        share(1, o, head).start()
    advance()

    summed = None
    query_f = query.astype(F32) * scale
    for d in range(2):
        carry_c[...] = jnp.zeros_like(carry_c)
        carry_n[...] = jnp.zeros_like(carry_n)

        def join(i, peak_in):
            source = i if d == 0 else n - 1 - i
            total = pack_in[source, 2:3, :]
            stable = pack_in[source, 3:4, :]
            new = jnp.maximum(peak_in + total, stable)
            old_w = jnp.exp(peak_in + total - new)
            new_w = jnp.exp(stable - new)
            carry_c[...] = old_w * carry_c[...] + new_w * state_in[source].astype(F32)
            carry_n[...] = old_w * carry_n[...] + new_w * pack_in[source, 1:2, :]
            return new

        peak_in = lax.fori_loop(0, me if d == 0 else n - 1 - me, join, jnp.full((1, dv), LOWEST, F32))
        cum_c, peak, num, den = local[d]
        carried = cum_c + peak_in[:, :1]
        top = jnp.maximum(carried, peak)
        carry_w = jnp.exp(carried - top)
        own_w = jnp.exp(peak - top)
        num = own_w * num + carry_w * dot(query_f, carry_c[...], NN, HIGH)
        den = own_w * den + carry_w * jnp.sum(query_f * carry_n[:, :dk], axis=-1, keepdims=True)
        result = num / jnp.maximum(jnp.abs(den), jnp.exp(-top))
        summed = result if d == 0 else summed + result
        if d == 0:
            advance()
    inverse = lax.rsqrt(jnp.mean(summed * summed, axis=-1, keepdims=True) + EPS)
    joined[head, :, :dv] = (summed * inverse * head_gain[...]).astype(BF16)
    for o in range(1, t):
        share(0, o, head).start()

    lax.fori_loop(done[0] + 1, n - 1, lambda s, c: (ring_step(s, *wo_ring), c)[1], 0)
    ring_last(*wo_ring)
    for part in range(2):
        for o in range(1, t):
            share(part, o, lax.rem(head + o, t)).wait_recv()

    span_j = 2 * dv

    def emit(i, c):
        span = pl.ds(pl.multiple_of(i * width, width), width)
        total = dot(joined[0], wo_all[0:span_j, span], NN)
        for j in range(1, t):
            total += dot(joined[j], wo_all[j * span_j : (j + 1) * span_j, span], NN)
        out[:, span] = total.astype(BF16)
        return c

    lax.fori_loop(0, out.shape[1] // width, emit, 0)
    ring_drain(*w_ring)
    ring_drain(*wo_ring)
    lax.fori_loop(1, n, give_end, 0)
    for part in range(2):
        for o in range(1, t):
            share(part, o, head).wait_send()


def gather_body(
    n,
    t,
    tokens,
    norm_gain,
    w_query,
    w_key,
    w_value,
    w_gates,
    input_bias,
    forget_bias,
    decay_shift,
    head_gain,
    w_conv_b,
    w_conv_c,
    w_conv_in,
    conv_taps,
    w_out,
):
    rows, model = tokens.shape
    dk, dv = w_query.shape[1], w_value.shape[1]
    gates = jnp.transpose(w_gates[..., 0], (2, 1, 0)).reshape(4, model)
    gates = jnp.pad(gates, ((0, 4), (0, 0)))
    depth = w_query.shape[0]
    wide, cols = 2 * dk + dv + 3 * w_conv_b.shape[1], w_out.shape[1]
    hbm = pl.BlockSpec(memory_space=pl.ANY)
    vmem = pl.BlockSpec(memory_space=pltpu.VMEM)
    dma = pltpu.SemaphoreType.DMA
    return pl.pallas_call(
        functools.partial(gather_kernel, n, t, dk, dv),
        out_shape=jax.ShapeDtypeStruct((rows, cols), BF16),
        in_specs=[vmem] * 2 + [hbm] * 7 + [vmem] * 6,
        out_specs=vmem,
        scratch_shapes=[
            pltpu.VMEM((rows, model), BF16),
            pltpu.VMEM((n * depth, wide), BF16),
            pltpu.VMEM((n * w_out.shape[0], cols), BF16),
            pltpu.VMEM((rows, wide), BF16),
            pltpu.VMEM((2, dk, dv), BF16),
            pltpu.VMEM((2, 8, dv), F32),
            pltpu.VMEM((n, dk, dv), BF16),
            pltpu.VMEM((n, 8, dv), F32),
            pltpu.VMEM((dk, dv), F32),
            pltpu.VMEM((1, dv), F32),
            pltpu.VMEM((t, rows, 2 * dv), BF16),
            dma((2, (n - 1) * pieces(depth))),
            dma((2, (n - 1) * pieces(depth))),
            dma((2, (n - 1) * pieces(w_out.shape[0]))),
            dma((2, (n - 1) * pieces(w_out.shape[0]))),
            dma((n,)),
            dma((n,)),
            dma((n,)),
            dma((n,)),
            dma((2, t)),
            dma((2, t)),
            dma((7,)),
            pltpu.VMEM((8, 1), F32),
            pltpu.VMEM((8, rows), F32),
        ],
        compiler_params=pltpu.CompilerParams(
            collective_id=0, has_side_effects=True, vmem_limit_bytes=60 * 1024 * 1024
        ),
    )(
        tokens,
        norm_gain.reshape(1, model),
        w_query,
        w_key,
        w_value,
        w_conv_b,
        w_conv_c,
        w_conv_in,
        w_out,
        gates,
        input_bias,
        forget_bias,
        decay_shift[..., 0],
        head_gain.reshape(1, dv),
        conv_taps,
    )


PAIR = 2
WO_PIECES = 2


def fits(n, t, tokens, norm_gain, w_query, w_key, w_value, *rest):
    w_conv, w_out = rest[5], rest[9]
    depth, dk = w_query.shape
    dv = w_value.shape[1]
    rows = tokens.shape[0]
    even = n % PAIR == 0 and n > PAIR and t == 4
    wide = 2 * dk == dv and w_conv.shape[1] == dv and dv % 128 == 0 and dk % 128 == 0
    deep = (PAIR * depth) % (t * 128) == 0 and rows % 32 == 0 and w_out.shape[0] % (16 * WO_PIECES) == 0
    return even and wide and deep and rows <= depth


def kernel(
    n,
    t,
    dk,
    dv,
    tokens,
    norm_gain,
    w_query,
    w_key,
    w_value,
    w_conv_b,
    w_conv_c,
    w_conv_in,
    w_out,
    w_gates,
    input_bias,
    forget_bias,
    decay_shift,
    head_gain,
    taps,
    out,
    tok,
    nbuf,
    tall,
    wbuf,
    wo_all,
    acc,
    sbuf,
    rbuf,
    proj,
    wg,
    decay,
    state_out,
    pack_out,
    mate_state,
    mate_pack,
    pair_state,
    pair_pack,
    state_in,
    pack_in,
    edge_out,
    edge_in,
    carry_c,
    carry_n,
    local_num,
    joined,
    result,
    out_sem,
    own_sem,
    tok_sem,
    tk_ss,
    tk_rs,
    tf_ss,
    tf_rs,
    w_ss,
    w_rs,
    rs_ss,
    rs_rs,
    st_ss,
    st_rs,
    pk_ss,
    pk_rs,
    ed_ss,
    ed_rs,
    j_ss,
    j_rs,
    jp_ss,
    jp_rs,
    oz_ss,
    oz_rs,
    oy_ss,
    oy_rs,
    ox_ss,
    ox_rs,
):
    me = lax.axis_index("sp")
    head = lax.axis_index("tp")
    lines = n // PAIR
    z = lax.div(me, PAIR)
    y = lax.rem(me, PAIR)
    mate = me + 1 - 2 * y
    core = lax.rem(head, 2)
    core_mate = head + 1 - 2 * core
    x_mate = lax.rem(head + 2, t)
    far_mate = lax.rem(core_mate + 2, t)
    rows, model = tokens.shape
    depth = w_query.shape[0]
    part_k = nbuf.shape[-1]
    chunks = wbuf.shape[0]

    def at_line(line):
        return PAIR * line + y

    rows_at_once = 32

    def load_rows(i):
        span = pl.ds(pl.multiple_of(i * rows_at_once, rows_at_once), rows_at_once)
        return pltpu.make_async_copy(tokens.at[span, :], tok.at[span, :], tok_sem.at[i])

    def load_start(i, c):
        load_rows(i).start()
        return c

    lax.fori_loop(0, rows // rows_at_once, load_start, 0)
    mine = pl.ds(pl.multiple_of(y * depth, depth), depth)
    loads = []
    plan = ((w_query, 0, 0), (w_key, 0, dk), (w_value, 1, 0), (w_conv_c, 2, 0), (w_conv_in, 3, 0), (w_conv_b, 4, 0))
    for part, chunk, offset in plan:
        spot = wbuf.at[chunk, mine, pl.ds(offset, part.shape[1])]
        loads.append(pltpu.make_async_copy(part, spot, own_sem.at[1 + len(loads)]))
    depth_o = w_out.shape[0]
    spot = wo_all.at[pl.ds(pl.multiple_of(me * depth_o, depth_o), depth_o), :]
    loads.append(pltpu.make_async_copy(w_out, spot, own_sem.at[1 + len(loads)]))
    for load in loads:
        load.start()

    edge_in[...] = jnp.zeros_like(edge_in)

    barrier = pltpu.get_barrier_semaphore()

    def greet_sp(o, c):
        pl.semaphore_signal(barrier, inc=1, device_id={"sp": lax.rem(me + o, n)})
        return c

    def greet_tp(o, c):
        pl.semaphore_signal(barrier, inc=1, device_id={"tp": lax.rem(head + o, t)})
        return c

    lax.fori_loop(1, n, greet_sp, 0)
    lax.fori_loop(1, t, greet_tp, 0)

    def norm_rows(i, c):
        load_rows(i).wait()
        span = pl.ds(pl.multiple_of(i * rows_at_once, rows_at_once), rows_at_once)
        values = tok[span, :].astype(F32)
        inverse = lax.rsqrt(jnp.mean(values * values, axis=-1, keepdims=True) + EPS)
        normed = (values * inverse * norm_gain[...]).astype(BF16)
        for b in range(lines * t):
            nbuf[b // t, b % t, span, :] = normed[:, b * part_k : (b + 1) * part_k]
        return c

    lax.fori_loop(0, rows // rows_at_once, norm_rows, 0)
    pl.semaphore_wait(barrier, n + t - 2)

    ups = lines - 1 - z

    half_way = lines // 2
    end_here = 1 - jnp.minimum(z, 1) * jnp.minimum(ups, 1)
    inner_up = jnp.minimum(lax.div(ups, half_way), 1)
    inner_count = inner_up * ups + (1 - inner_up) * z

    def pick(k, near):
        up = jnp.clip(ups - k, 0, 1)
        down_k = k - ups
        if near:
            return up, up * (z + 1 + k) + (1 - up) * (z - 1 - down_k)
        return up, up * (lines - 1 - k) + (1 - up) * down_k

    def token_send(line):
        return pltpu.make_async_remote_copy(
            nbuf.at[line, head], tall.at[z, head], tk_ss.at[line], tk_rs.at[z], device_id={"sp": at_line(line)}
        )

    def token_take(line):
        return pltpu.make_async_remote_copy(
            nbuf.at[line, head], tall.at[line, head], tk_ss.at[line], tk_rs.at[line], device_id={"sp": at_line(line)}
        )

    def token_pass(line, way):
        quarter = (head, head, x_mate)[way]
        there = tall.at[line, quarter]
        return pltpu.make_async_remote_copy(
            there, there, tf_ss.at[way, line], tf_rs.at[way, line], device_id={"tp": (core_mate, x_mate, core_mate)[way]}
        )

    def token_get(line, way):
        quarter = (core_mate, x_mate, far_mate)[way]
        there = tall.at[line, quarter]
        return pltpu.make_async_remote_copy(
            there, there, tf_ss.at[way, line], tf_rs.at[way, line], device_id={"tp": (core_mate, x_mate, core_mate)[way]}
        )

    def send_tokens(k, c):
        _, line = pick(k, False)
        token_send(line).start()
        return c

    lax.fori_loop(0, lines - 1, send_tokens, 0)

    def w_send(chunk):
        there = wbuf.at[chunk, mine, :]
        return pltpu.make_async_remote_copy(there, there, w_ss.at[chunk], w_rs.at[chunk], device_id={"sp": mate})

    def w_take(chunk):
        there = wbuf.at[chunk, pl.ds(pl.multiple_of((1 - y) * depth, depth), depth), :]
        return pltpu.make_async_remote_copy(there, there, w_ss.at[chunk], w_rs.at[chunk], device_id={"sp": mate})

    for load in loads:
        load.wait()
    for chunk in range(chunks):
        w_send(chunk).start()

    tall_o = depth_o // WO_PIECES

    def wo_rows(index, piece):
        return wo_all.at[pl.ds(pl.multiple_of(index * depth_o + piece * tall_o, tall_o), tall_o), :]

    def wo_line(line, piece, way, sem):
        there = wo_rows(at_line(line), piece)
        return pltpu.make_async_remote_copy(
            there, there, oz_ss.at[sem, piece], oz_rs.at[line, piece], device_id={"sp": at_line(z + way)}
        )

    def wo_mate(line, piece):
        there = wo_rows(at_line(line), piece)
        return pltpu.make_async_remote_copy(
            there, there, oy_ss.at[line, piece], oy_rs.at[line, piece], device_id={"sp": mate}
        )

    def wo_mate_take(line, piece):
        there = wo_rows(PAIR * line + 1 - y, piece)
        return pltpu.make_async_remote_copy(
            there, there, oy_ss.at[line, piece], oy_rs.at[line, piece], device_id={"sp": mate}
        )

    def wo_own(way, wanted):
        @pl.when(wanted)
        def _():
            for piece in range(WO_PIECES):
                wo_line(z, piece, way, lines + (way + 1) // 2).start()

    has_up, has_down = z < lines - 1, z > 0
    at_end = jnp.logical_or(z == 0, z == lines - 1)
    upper = z >= half_way

    def wo_outward():
        wo_own(1, jnp.logical_and(upper, has_up))
        wo_own(-1, jnp.logical_and(jnp.logical_not(upper), has_down))

    def wo_inward(ends):
        here = at_end if ends else jnp.logical_not(at_end)
        wo_own(-1, jnp.logical_and(jnp.logical_and(upper, has_down), here))
        wo_own(1, jnp.logical_and(jnp.logical_and(jnp.logical_not(upper), has_up), here))

    def wo_relay(line, wanted, along, across, pieces_now=range(WO_PIECES)):
        @pl.when(jnp.logical_and(wanted, jnp.logical_and(line >= 0, line < lines)))
        def _():
            for piece in pieces_now:
                if along:
                    wo_line(line, piece, 0, line).wait_recv()

                    @pl.when(jnp.logical_and(line < z, has_up))
                    def _():
                        wo_line(line, piece, 1, line).start()

                    @pl.when(jnp.logical_and(line > z, has_down))
                    def _():
                        wo_line(line, piece, -1, line).start()

                if across:

                    @pl.when(from_mate(line, piece))
                    def _():
                        wo_mate(line, piece).start()

                    if spread and piece == tail_piece:

                        @pl.when(jnp.logical_and(at_end, line == near_line))
                        def _():
                            mate_cut(line, y).start()

    inner_way = 2 * inner_up - 1

    spread = lines == 4
    tail_piece = WO_PIECES - 1
    near_line, far_line = z + inner_way, z + 2 * inner_way
    at_mid = jnp.logical_not(at_end)

    def cut_rows(index, half, halves):
        count = tall_o // halves
        first = index * depth_o + tail_piece * tall_o + half * count
        return wo_all.at[pl.ds(pl.multiple_of(first, count), count), :]

    def mate_cut(line, row):
        there = cut_rows(PAIR * line + row, 1, 2)
        return pltpu.make_async_remote_copy(
            there, there, oy_ss.at[line, tail_piece], oy_rs.at[line, tail_piece], device_id={"sp": mate}
        )

    def along_row(line, way, kind):
        there = cut_rows(PAIR * line + 1 - y, 0, 1 + kind)
        return pltpu.make_async_remote_copy(
            there, there, ox_ss.at[kind], ox_rs.at[kind], device_id={"sp": at_line(z + way)}
        )

    def from_mate(line, piece):
        if not spread or piece != tail_piece:
            return line >= 0
        return jnp.logical_or(
            jnp.logical_and(at_mid, line != far_line), jnp.logical_and(at_end, line != near_line)
        )

    def spread_send():
        if spread:

            @pl.when(at_mid)
            def _():
                wo_mate_take(z, tail_piece).wait_recv()
                along_row(z, -inner_way, 1).start()
                wo_mate_take(z - inner_way, tail_piece).wait_recv()
                along_row(z - inner_way, inner_way, 0).start()

    def wo_first(pieces_now, along=True, across=True, wanted=True):
        wo_relay(z - inner_way * (1 - 2 * end_here), wanted, along, across, pieces_now)

    def wo_second(along, across, pieces_now=range(WO_PIECES)):
        wo_relay(z + inner_way, jnp.logical_not(at_end), along, across, pieces_now)

    def wo_rest(away, pieces_now, along=True, across=True, wanted=True):
        wo_relay(z - away, wanted, along, across, pieces_now)
        wo_relay(z + away, wanted, along, across, pieces_now)

    for piece in range(WO_PIECES):
        wo_mate(z, piece).start()
    wo_inward(True)

    wg[...] = jnp.zeros_like(wg)
    wg[0:2, :] = w_gates[0]
    wg[2:4, :] = w_gates[1]
    decay[...] = jnp.zeros_like(decay)
    decay[1:2, :] = decay_shift[0]
    decay[3:4, :] = decay_shift[1]
    gates = None
    for b in range(lines * t):
        piece = dot(wg[:, b * part_k : (b + 1) * part_k], nbuf[b // t, b % t], NT)
        gates = piece if b == 0 else gates + piece
    gate_id = lax.broadcasted_iota(jnp.int32, gates.shape, 0)
    offsets = (input_bias[0, 0], forget_bias[0, 0], input_bias[0, 1], forget_bias[0, 1])
    for i, offset in enumerate(offsets):
        gates = jnp.where(gate_id == i, gates + offset, gates)
    forget = jnp.minimum(gates, 0.0) - jnp.log1p(jnp.exp(-jnp.abs(gates))) + decay[...]
    row_id = lax.broadcasted_iota(jnp.int32, (rows, rows), 0)
    col_id = lax.broadcasted_iota(jnp.int32, (rows, rows), 1)
    upto = (row_id <= col_id).astype(F32)
    after = (row_id >= col_id).astype(F32)
    sums = (dot(forget, upto, NN, HIGH), dot(forget, after, NN, HIGH))
    gates_t = gates.T
    sums_t = (sums[0].T, sums[1].T)

    def relay_direct(k, c):
        _, line = pick(k, True)
        token_take(line).wait_recv()
        token_pass(line, 1).start()
        token_pass(line, 0).start()
        return c

    def relay_across(k, c):
        _, line = pick(k, True)
        token_get(line, 1).wait_recv()
        token_pass(line, 2).start()
        return c

    def tokens_ready(k, c):
        _, line = pick(k, True)
        token_get(line, 0).wait_recv()
        token_get(line, 2).wait_recv()
        return c

    lax.fori_loop(0, lines - 1, relay_direct, 0)
    wo_outward()
    wo_inward(False)
    lax.fori_loop(0, lines - 1, relay_across, 0)
    lax.fori_loop(0, lines - 1, tokens_ready, 0)
    def parts_of(chunk):
        if isinstance(chunk, int) and chunk == chunks - 1:
            return ((0, rows // 2, chunk), (rows // 2, rows // 2, chunks))
        return ((0, rows, chunk),)

    def hop(chunk, part, k, up, line):
        first, count, sem = part
        last = (1 - up) * (1 - jnp.minimum(jnp.abs(z - line) - 1, 1))
        slot = line + last * (lines - line)
        return pltpu.make_async_remote_copy(
            sbuf.at[chunk, k, pl.ds(first, count)],
            rbuf.at[chunk, slot, pl.ds(first, count)],
            rs_ss.at[sem, k],
            rs_rs.at[sem, slot],
            device_id={"sp": at_line(z + 2 * up - 1)},
        )

    def arrived(chunk, part, slot):
        first, count, sem = part
        return pltpu.make_async_remote_copy(
            sbuf.at[chunk, 0, pl.ds(first, count)],
            rbuf.at[chunk, slot, pl.ds(first, count)],
            rs_ss.at[sem, 0],
            rs_rs.at[sem, slot],
            device_id={"sp": me},
        )

    def product(source, line, chunk, part):
        span = pl.ds(part[0], part[1])
        total = dot(source[line, 0, span, :], wbuf[chunk, 0:part_k, :], NN)
        for q in range(1, t):
            total += dot(source[line, q, span, :], wbuf[chunk, q * part_k : (q + 1) * part_k, :], NN)
        return total

    def add_along(chunk, part, slot, up, line):
        span = pl.ds(part[0], part[1])
        acc[span, :] = product(tall, line, chunk, part)
        before = up * jnp.minimum(z, 1) + (1 - up) * jnp.minimum(ups, 1)

        @pl.when(before == 1)
        def _():
            arrived(chunk, part, line).wait_recv()
            sbuf[chunk, slot, span, :] = (acc[span, :] + rbuf[chunk, line, span, :].astype(F32)).astype(BF16)

        @pl.when(before == 0)
        def _():
            sbuf[chunk, slot, span, :] = acc[span, :].astype(BF16)

        hop(chunk, part, slot, up, line).start()

    def inward_span(first, last, chunk):
        def one(k, c):
            line = inner_up * (lines - 1 - k) + (1 - inner_up) * k
            for part in parts_of(chunk):
                add_along(chunk, part, k, inner_up, line)
            return c

        lax.fori_loop(first, last, one, 0)

    def inward_where(runs, chunk):
        @pl.when(runs == 1)
        def _():
            w_take(chunk).wait_recv()

        inward_span(0, runs * inner_count, chunk)

    def inward(end_chunk, mid_chunk):
        end_runs, mid_runs = end_chunk < chunks, mid_chunk >= 0
        if end_runs and mid_runs and max(end_chunk, mid_chunk) < chunks - 1:
            inward_where(1, end_here * end_chunk + (1 - end_here) * mid_chunk)
            return
        if end_runs:
            inward_where(end_here, end_chunk)
        if mid_runs:
            inward_where(1 - end_here, mid_chunk)

    def outward(chunk):
        for part in parts_of(chunk):

            def one(k, c):
                line = (1 - inner_up) * (lines - 1 - k) + inner_up * k
                add_along(chunk, part, inner_count + k, 1 - inner_up, line)
                return c

            lax.fori_loop(0, lines - 1 - inner_count, one, 0)

    def own_part(chunk, part):
        span = pl.ds(part[0], part[1])
        acc[span, :] = product(nbuf, z, chunk, part)

        @pl.when(has_down)
        def _():
            arrived(chunk, part, z).wait_recv()
            acc[span, :] += rbuf[chunk, z, span, :].astype(F32)

        @pl.when(has_up)
        def _():
            arrived(chunk, part, lines).wait_recv()
            acc[span, :] += rbuf[chunk, lines, span, :].astype(F32)

    def own_chunk(chunk):
        own_part(chunk, parts_of(chunk)[0])
        proj[chunk] = acc[...].astype(BF16)

    inward(0, -1)
    inward(1, -1)
    inward(2, 0)
    wo_first((0,))
    wo_second(True, False, (0,))
    inward(3, 1)
    wo_first(range(1, WO_PIECES), True, False)
    outward(0)
    wo_second(True, False, range(1, WO_PIECES))
    own_chunk(0)
    wo_rest(2, (0,), True, True, at_end)
    inward(chunks, 2)
    outward(1)
    own_chunk(1)

    keys_f = proj[0, :, dk:].astype(F32)
    wide = pack_out.shape[-1]
    for d in range(2):
        cum_c = sums_t[d][:, 2 * d + 1 : 2 * d + 2]
        in_c = gates_t[:, 2 * d : 2 * d + 1]
        last = rows - 1 if d == 0 else 0
        total = cum_c[last : last + 1, :]
        update = total - cum_c + in_c
        stable = jnp.max(update, axis=0, keepdims=True)
        weighted = keys_f * jnp.exp(update - stable)
        state_out[d] = dot(weighted.astype(BF16), proj[1], TN).astype(BF16)
        pack_out[d, 0:1, :dk] = jnp.sum(weighted, axis=0, keepdims=True)
        pack_out[d, 0:1, dk:] = jnp.zeros((1, wide - dk), F32)
        pack_out[d, 1:2, :] = jnp.broadcast_to(total, (1, wide))
        pack_out[d, 2:3, :] = jnp.broadcast_to(stable, (1, wide))
        pack_out[d, 3:, :] = jnp.zeros((5, wide), F32)

    def swap_states():
        return (
            pltpu.make_async_remote_copy(state_out, mate_state, st_ss.at[2], st_rs.at[2], device_id={"sp": mate}),
            pltpu.make_async_remote_copy(pack_out, mate_pack, pk_ss.at[2], pk_rs.at[2], device_id={"sp": mate}),
        )

    for copy in swap_states():
        copy.start()
    wo_first(range(1, WO_PIECES), False, True)
    wo_second(False, True, (0,))
    wo_rest(2, (0,), True, False, at_mid)
    wo_rest(2, range(1, WO_PIECES), True, False)
    wo_rest(2, range(1, WO_PIECES), False, True, at_end)

    d_in, d_out = 1 - inner_up, inner_up

    def chain(d, way):
        ids = {"sp": at_line(z + way)}
        return (
            pltpu.make_async_remote_copy(pair_state.at[d], state_in.at[d], st_ss.at[d], st_rs.at[d], device_id=ids),
            pltpu.make_async_remote_copy(pair_pack.at[d], pack_in.at[d], pk_ss.at[d], pk_rs.at[d], device_id=ids),
        )

    def chain_add(d):
        for copy in chain(d, 0):
            copy.wait_recv()
        total, stable, first_w, second_w = blend(pack_in[d], pair_pack[d])
        joint = first_w[:, :1] * state_in[d].astype(F32) + second_w[:, :1] * pair_state[d].astype(F32)
        pair_state[d] = joint.astype(BF16)
        pair_pack[d, 0:1, :] = first_w * pack_in[d, 0:1, :] + second_w * pair_pack[d, 0:1, :]
        pair_pack[d, 1:2, :] = total
        pair_pack[d, 2:3, :] = stable

    def chain_from_end():
        @pl.when(at_end)
        def _():
            for copy in chain(d_in, inner_way):
                copy.start()

    def chain_inward():
        @pl.when(jnp.logical_not(at_end))
        def _():
            chain_add(d_in)
            for copy in chain(d_in, inner_way):
                copy.start()

    def chain_outward():
        @pl.when(jnp.logical_not(at_end))
        def _():
            chain_add(d_out)
            for copy in chain(d_out, -inner_way):
                copy.start()

        @pl.when(at_end)
        def _():
            for copy in chain(d_out, 0):
                copy.wait_recv()

    def blend(first, second):
        total = first[1:2, :] + second[1:2, :]
        moved = first[2:3, :] + second[1:2, :]
        stable = jnp.maximum(moved, second[2:3, :])
        return total, stable, jnp.exp(moved - stable), jnp.exp(second[2:3, :] - stable)

    def pair_up():
        for copy in swap_states():
            copy.wait_recv()
        own_first = (1 - y).astype(F32)
        for d in range(2):
            lead = own_first if d == 0 else 1.0 - own_first
            mine_p, other_p = pack_out[d], mate_pack[d]
            first = lead * mine_p + (1.0 - lead) * other_p
            second = lead * other_p + (1.0 - lead) * mine_p
            total, stable, first_w, second_w = blend(first, second)
            mine_w = lead * first_w + (1.0 - lead) * second_w
            other_w = lead * second_w + (1.0 - lead) * first_w
            joint = mine_w * state_out[d].astype(F32) + other_w * mate_state[d].astype(F32)
            pair_state[d] = joint.astype(BF16)
            pair_pack[d, 0:1, :] = mine_w * mine_p[0:1, :] + other_w * other_p[0:1, :]
            pair_pack[d, 1:2, :] = total
            pair_pack[d, 2:3, :] = stable
            pair_pack[d, 3:, :] = jnp.zeros((5, wide), F32)

    inward(chunks, 3)
    pair_up()
    chain_from_end()
    inward(4, -1)
    outward(2)
    for away in range(3, lines):
        wo_rest(away, (0,))
    own_chunk(2)

    scale = dk ** (-0.5)
    scores = dot(proj[0, :, :dk], proj[0, :, dk:], NT) * scale
    local = []
    for d in range(2):
        cum_c = sums_t[d][:, 2 * d + 1 : 2 * d + 2]
        cum_r = sums[d][2 * d + 1 : 2 * d + 2, :]
        in_r = gates[2 * d : 2 * d + 1, :]
        allowed = row_id >= col_id if d == 0 else row_id <= col_id
        log_weight = jnp.where(allowed, cum_c - cum_r + in_r, -jnp.inf)
        peak = jnp.max(log_weight, axis=-1, keepdims=True)
        part = scores * jnp.exp(log_weight - peak)
        local_num[d] = dot(part.astype(BF16), proj[1], NN)
        local.append((cum_c, peak, jnp.sum(part, axis=-1, keepdims=True)))

    outward(3)
    own_chunk(3)

    mixed = (proj[2].astype(F32) * proj[3].astype(F32)).astype(BF16).astype(F32)
    edge_out[0, 0:1, :] = mixed[rows - 1 :, :]
    edge_out[1, 0:1, :] = mixed[:1, :]
    edge_out[0, 1:, :] = jnp.zeros((7, dv), F32)
    edge_out[1, 1:, :] = jnp.zeros((7, dv), F32)

    def edge(way):
        other = me + 1 if way == 0 else me - 1
        return pltpu.make_async_remote_copy(
            edge_out.at[way], edge_in.at[way], ed_ss.at[way], ed_rs.at[way], device_id={"sp": other}
        )

    later_exists, prior_exists = me < n - 1, me > 0

    @pl.when(later_exists)
    def _():
        edge(0).start()

    @pl.when(prior_exists)
    def _():
        edge(1).start()

    wo_second(False, True, range(1, WO_PIECES))
    wo_rest(2, range(WO_PIECES), False, True, jnp.logical_not(at_end))
    chain_inward()


    @pl.when(at_mid)
    def _():
        w_take(4).wait_recv()

    inward_span(0, 1 - end_here, 4)
    chain_outward()
    inward_span(1, (1 - end_here) * inner_count, 4)
    for away in range(3, lines):
        wo_rest(away, range(1, WO_PIECES))

    half_rows = rows // 2

    def joined_part(part, source, way):
        columns = pl.ds(part * dv, dv)
        if way == 0:
            return joined.at[source, :, columns]
        return joined.at[source, pl.ds((way - 1) * half_rows, half_rows), columns]

    others = (core_mate, x_mate, far_mate)

    def share(part, way, source):
        slot = joined_part(part, source, way)
        return pltpu.make_async_remote_copy(
            slot, slot, j_ss.at[part, way], j_rs.at[part, way], device_id={"tp": others[way]}
        )

    def share_pass(part, way, source):
        slot = joined_part(part, source, way)
        return pltpu.make_async_remote_copy(
            slot, slot, jp_ss.at[part, way - 1], jp_rs.at[part, way - 1], device_id={"tp": core_mate}
        )

    def share_start(part):
        for way in (1, 2, 0):
            share(part, way, head).start()

    def share_relay(part):
        for way in (1, 2):
            share(part, way, others[way]).wait_recv()
            share_pass(part, way, others[way]).start()

    def share_wait(part):
        share(part, 0, core_mate).wait_recv()
        for way in (1, 2):
            share_pass(part, way, others[3 - way]).wait_recv()

    def share_end(part):
        for way in range(3):
            share(part, way, head).wait_send()
        for way in (1, 2):
            share_pass(part, way, others[way]).wait_send()

    summed = None
    query_f = proj[0, :, :dk].astype(F32) * scale
    for d in range(2):
        carry_c[...] = jnp.zeros_like(carry_c)
        carry_n[...] = jnp.zeros_like(carry_n)

        def merge(state, pack, peak_in):
            total = pack[1:2, :]
            stable = pack[2:3, :]
            new = jnp.maximum(peak_in + total, stable)
            old_w = jnp.exp(peak_in + total - new)
            new_w = jnp.exp(stable - new)
            carry_c[...] = old_w * carry_c[...] + new_w * state.astype(F32)
            carry_n[...] = old_w * carry_n[...] + new_w * pack[0:1, :]
            return new

        def join(i, peak_in):
            return merge(state_in[d], pack_in[d], peak_in)

        def join_mate(i, peak_in):
            return merge(mate_state[d], mate_pack[d], peak_in)

        peak_in = lax.fori_loop(0, jnp.minimum(z if d == 0 else ups, 1), join, jnp.full((1, dv), LOWEST, F32))
        peak_in = lax.fori_loop(0, y if d == 0 else 1 - y, join_mate, peak_in)
        cum_c, peak, den = local[d]
        carried = cum_c + peak_in[:, :1]
        top = jnp.maximum(carried, peak)
        carry_w = jnp.exp(carried - top)
        own_w = jnp.exp(peak - top)
        num = own_w * local_num[d] + carry_w * dot(query_f.astype(BF16), carry_c[...].astype(BF16), NN)
        den = own_w * den + carry_w * jnp.sum(query_f * carry_n[:, :dk], axis=-1, keepdims=True)
        cell = num / jnp.maximum(jnp.abs(den), jnp.exp(-top))
        summed = cell if d == 0 else summed + cell
    inverse = lax.rsqrt(jnp.mean(summed * summed, axis=-1, keepdims=True) + EPS)
    joined[head, :, :dv] = (summed * inverse * head_gain[...]).astype(BF16)
    share_start(0)
    outward(4)
    spread_send()

    @pl.when(prior_exists)
    def _():
        edge(0).wait_recv()

    @pl.when(later_exists)
    def _():
        edge(1).wait_recv()

    mixed = (proj[2].astype(F32) * proj[3].astype(F32)).astype(BF16).astype(F32)
    pos = lax.broadcasted_iota(jnp.int32, mixed.shape, 0)
    prior = jnp.where(pos == 0, edge_in[0, 0:1, :], pltpu.roll(mixed, 1, 0))
    later = jnp.where(pos == rows - 1, edge_in[1, 0:1, :], pltpu.roll(mixed, rows - 1, 0))
    taps_f = taps[...].astype(F32)
    local_num[0] = taps_f[0:1] * prior + taps_f[1:2] * mixed + taps_f[2:3] * later
    for i, part in enumerate(parts_of(chunks - 1)):
        span = pl.ds(part[0], part[1])
        own_part(chunks - 1, part)
        outer = acc[span, :].astype(BF16).astype(F32)
        joined[head, span, dv:] = (outer * local_num[0, span, :]).astype(BF16)
        share(1, 1 + i, head).start()
    share(1, 0, head).start()
    share_relay(0)
    share_relay(1)

    for line in range(lines):
        for piece in range(WO_PIECES):
            if not spread or piece != tail_piece:
                wo_mate_take(line, piece).wait_recv()
                continue

            @pl.when(jnp.logical_or(jnp.logical_and(at_mid, line == near_line), jnp.logical_and(at_end, line != near_line)))
            def _():
                wo_mate_take(line, piece).wait_recv()

    if spread:

        @pl.when(at_mid)
        def _():
            along_row(far_line, 0, 0).wait_recv()

        @pl.when(at_end)
        def _():
            along_row(near_line, 0, 1).wait_recv()
            mate_cut(near_line, 1 - y).wait_recv()

    for part in range(2):
        share_wait(part)

    span_j = 2 * dv
    width = 256

    def emit(i, c):
        span = pl.ds(pl.multiple_of(i * width, width), width)
        total = dot(joined[0], wo_all[0:span_j, span], NN)
        for j in range(1, t):
            total += dot(joined[j], wo_all[j * span_j : (j + 1) * span_j, span], NN)
        result[:, span] = total.astype(BF16)
        put(i).start()
        return c

    def put(i):
        span = pl.ds(pl.multiple_of(i * width, width), width)
        return pltpu.make_async_copy(result.at[:, span], out.at[:, span], out_sem.at[i])

    def put_end(i, c):
        put(i).wait()
        return c

    lax.fori_loop(0, out.shape[1] // width, emit, 0)

    def token_end(k, c):
        _, line = pick(k, False)
        token_send(line).wait_send()
        for way in range(3):
            token_pass(line, way).wait_send()
        inner = jnp.clip(inner_count - k, 0, 1)
        up = inner * inner_up + (1 - inner) * (1 - inner_up)
        step = inner * k + (1 - inner) * (k - inner_count)
        line = up * (lines - 1 - step) + (1 - up) * step
        for chunk in range(chunks):
            for part in parts_of(chunk):
                hop(chunk, part, k, up, line).wait_send()
        return c

    lax.fori_loop(0, lines - 1, token_end, 0)
    for chunk in range(chunks):
        w_send(chunk).wait_send()
    for copy in swap_states():
        copy.wait_send()

    @pl.when(at_end)
    def _():
        for copy in chain(d_in, inner_way):
            copy.wait_send()

    @pl.when(jnp.logical_not(at_end))
    def _():
        for copy in chain(d_in, inner_way) + chain(d_out, -inner_way):
            copy.wait_send()


    @pl.when(later_exists)
    def _():
        edge(0).wait_send()

    @pl.when(prior_exists)
    def _():
        edge(1).wait_send()

    for part in range(2):
        share_end(part)
    for piece in range(WO_PIECES):

        @pl.when(has_up)
        def _():
            wo_line(z, piece, 1, lines + 1).wait_send()

        @pl.when(has_down)
        def _():
            wo_line(z, piece, -1, lines).wait_send()

        for line in range(lines):

            @pl.when(jnp.logical_and(z > line, has_up))
            def _():
                wo_line(line, piece, 1, line).wait_send()

            @pl.when(jnp.logical_and(z < line, has_down))
            def _():
                wo_line(line, piece, -1, line).wait_send()

            @pl.when(from_mate(line, piece))
            def _():
                wo_mate(line, piece).wait_send()

    if spread:

        @pl.when(at_mid)
        def _():
            along_row(z, -inner_way, 1).wait_send()
            along_row(z - inner_way, inner_way, 0).wait_send()

        @pl.when(at_end)
        def _():
            mate_cut(near_line, y).wait_send()

    lax.fori_loop(0, out.shape[1] // width, put_end, 0)

def body(
    n,
    t,
    tokens,
    norm_gain,
    w_query,
    w_key,
    w_value,
    w_gates,
    input_bias,
    forget_bias,
    decay_shift,
    head_gain,
    w_conv_b,
    w_conv_c,
    w_conv_in,
    conv_taps,
    w_out,
):
    rows, model = tokens.shape
    depth, dk = w_query.shape
    dv = w_value.shape[1]
    lines = n // PAIR
    chunks = 5
    part_k = PAIR * depth // t
    cols = w_out.shape[1]
    gates = jnp.transpose(w_gates[..., 0], (1, 2, 0))
    hbm = pl.BlockSpec(memory_space=pl.ANY)
    vmem = pl.BlockSpec(memory_space=pltpu.VMEM)
    smem = pl.BlockSpec(memory_space=pltpu.SMEM)
    dma = pltpu.SemaphoreType.DMA
    return pl.pallas_call(
        functools.partial(kernel, n, t, dk, dv),
        out_shape=jax.ShapeDtypeStruct((rows, cols), BF16),
        in_specs=[hbm, vmem] + [hbm] * 7 + [vmem] + [smem] * 2 + [vmem] * 3,
        out_specs=hbm,
        scratch_shapes=[
            pltpu.VMEM((rows, model), BF16),
            pltpu.VMEM((lines, t, rows, part_k), BF16),
            pltpu.VMEM((lines, t, rows, part_k), BF16),
            pltpu.VMEM((chunks, PAIR * depth, dv), BF16),
            pltpu.VMEM((n * w_out.shape[0], cols), BF16),
            pltpu.VMEM((rows, dv), F32),
            pltpu.VMEM((chunks, lines - 1, rows, dv), BF16),
            pltpu.VMEM((chunks, lines + 1, rows, dv), BF16),
            pltpu.VMEM((chunks, rows, dv), BF16),
            pltpu.VMEM((8, model), BF16),
            pltpu.VMEM((8, rows), F32),
            pltpu.VMEM((2, dk, dv), BF16),
            pltpu.VMEM((2, 8, dv), F32),
            pltpu.VMEM((2, dk, dv), BF16),
            pltpu.VMEM((2, 8, dv), F32),
            pltpu.VMEM((2, dk, dv), BF16),
            pltpu.VMEM((2, 8, dv), F32),
            pltpu.VMEM((2, dk, dv), BF16),
            pltpu.VMEM((2, 8, dv), F32),
            pltpu.VMEM((2, 8, dv), F32),
            pltpu.VMEM((2, 8, dv), F32),
            pltpu.VMEM((dk, dv), F32),
            pltpu.VMEM((1, dv), F32),
            pltpu.VMEM((2, rows, dv), F32),
            pltpu.VMEM((t, rows, 2 * dv), BF16),
            pltpu.VMEM((rows, cols), BF16),
            dma((cols // 256,)),
            dma((8,)),
            dma((rows // 32,)),
            dma((lines,)),
            dma((lines,)),
            dma((3, lines)),
            dma((3, lines)),
            dma((chunks,)),
            dma((chunks,)),
            dma((chunks + 1, lines - 1)),
            dma((chunks + 1, lines + 1)),
            dma((3,)),
            dma((3,)),
            dma((3,)),
            dma((3,)),
            dma((2,)),
            dma((2,)),
            dma((2, 3)),
            dma((2, 3)),
            dma((2, 2)),
            dma((2, 2)),
            dma((lines + 2, WO_PIECES)),
            dma((lines, WO_PIECES)),
            dma((lines, WO_PIECES)),
            dma((lines, WO_PIECES)),
            dma((2,)),
            dma((2,)),
        ],
        compiler_params=pltpu.CompilerParams(
            collective_id=0, has_side_effects=True, vmem_limit_bytes=60 * 1024 * 1024
        ),
    )(
        tokens,
        norm_gain.reshape(1, model),
        w_query,
        w_key,
        w_value,
        w_conv_b,
        w_conv_c,
        w_conv_in,
        w_out,
        gates,
        input_bias.T,
        forget_bias.T,
        jnp.swapaxes(decay_shift, 1, 2),
        head_gain.reshape(1, dv),
        conv_taps,
    )


def solution(mesh):
    placed = (
        P("sp", None),
        P(),
        P("sp", "tp"),
        P("sp", "tp"),
        P("sp", "tp"),
        P(None, None, None, "tp"),
        P(None, "tp"),
        P(None, "tp"),
        P(None, "sp", "tp"),
        P("tp"),
        P("sp", "tp"),
        P("sp", "tp"),
        P("sp", "tp"),
        P(None, "tp"),
        P("sp", "tp"),
    )
    n, t = mesh.shape["sp"], mesh.shape["tp"]

    def step(*args):
        form = body if fits(n, t, *args) else gather_body
        return form(n, t, *args)

    return jax.shard_map(step, mesh=mesh, in_specs=placed, out_specs=P("sp", "tp"), check_vma=False)
```

```python
import functools

import jax
import jax.numpy as jnp
from jax import lax
from jax.experimental import pallas as pl
from jax.experimental.pallas import tpu as pltpu
from jax.sharding import PartitionSpec as P

EPS = 1e-06
HIGH = lax.Precision.HIGHEST
LOWEST = -1e30
PIECES = 4
F32 = jnp.float32
BF16 = jnp.bfloat16


def dot(a, b, dims, precision=None):
    return lax.dot_general(a, b, (dims, ((), ())), precision=precision, preferred_element_type=F32)


NN = ((1,), (0,))
NT = ((1,), (1,))
TN = ((0,), (0,))


def ring_place(index, n):
    odd = lax.rem(index, 2)
    half = lax.div(index, 2)
    return (1 - odd) * half + odd * (n - 1 - half)


def ring_index(place, n):
    late = lax.div(place, n // 2)
    return (1 - late) * (2 * place) + late * (2 * (n - 1 - place) + 1)


def pieces(depth):
    return max(1, min(PIECES, depth // 16))


def gather_kernel(
    n,
    t,
    dk,
    dv,
    tokens,
    norm_gain,
    w_query,
    w_key,
    w_value,
    w_conv_b,
    w_conv_c,
    w_conv_in,
    w_out,
    w_gates,
    input_bias,
    forget_bias,
    decay_shift,
    head_gain,
    taps,
    out,
    normed,
    w_all,
    wo_all,
    proj,
    state_out,
    pack_out,
    state_in,
    pack_in,
    carry_c,
    carry_n,
    joined,
    w_ss,
    w_rs,
    wo_ss,
    wo_rs,
    st_ss,
    st_rs,
    pk_ss,
    pk_rs,
    j_ss,
    j_rs,
    own_sem,
    gate_bias,
    decay,
):
    me = lax.axis_index("sp")
    head = lax.axis_index("tp")
    place = ring_place(me, n)
    right = ring_index(lax.rem(place + 1, n), n)
    left = ring_index(lax.rem(place + n - 1, n), n)
    rows = tokens.shape[0]

    parts = (w_query, w_key, w_value, w_conv_b, w_conv_c, w_conv_in)
    copies = []
    offset = 0
    for part in parts:
        depth, cols = part.shape
        spot = w_all.at[pl.ds(pl.multiple_of(me * depth, depth), depth), pl.ds(offset, cols)]
        copies.append(pltpu.make_async_copy(part, spot, own_sem.at[len(copies)]))
        offset += cols
    depth_o = w_out.shape[0]
    spot = wo_all.at[pl.ds(pl.multiple_of(me * depth_o, depth_o), depth_o), :]
    copies.append(pltpu.make_async_copy(w_out, spot, own_sem.at[len(copies)]))
    for copy in copies:
        copy.start()

    barrier = pltpu.get_barrier_semaphore()

    def greet_sp(o, c):
        pl.semaphore_signal(barrier, inc=1, device_id={"sp": lax.rem(me + o, n)})
        return c

    def greet_tp(o, c):
        pl.semaphore_signal(barrier, inc=1, device_id={"tp": lax.rem(head + o, t)})
        return c

    lax.fori_loop(1, n, greet_sp, 0)
    lax.fori_loop(1, t, greet_tp, 0)
    pl.semaphore_wait(barrier, n + t - 2)

    def hop(depth, whole, ss, rs, way, step, piece):
        width = whole.shape[1]
        half, tall = width // 2, depth // pieces(depth)
        holder = ring_index(lax.rem(place + (n + step if way else n - step), n), n)
        columns = pl.ds(way * half, half)
        there = whole.at[pl.ds(pl.multiple_of(holder * depth + piece * tall, tall), tall), columns]
        turn = step * pieces(depth) + piece
        return pltpu.make_async_remote_copy(
            src_ref=there,
            dst_ref=there,
            send_sem=ss.at[way, turn],
            recv_sem=rs.at[way, turn],
            device_id={"sp": left if way else right},
        )

    def ring_start(*ring):
        for piece in range(pieces(ring[0])):
            for way in range(2):
                hop(*ring, way, 0, piece).start()

    def ring_step(step, *ring):
        for piece in range(pieces(ring[0])):
            for way in range(2):
                hop(*ring, way, step - 1, piece).wait_recv()
                hop(*ring, way, step, piece).start()

    def ring_last(*ring):
        for piece in range(pieces(ring[0])):
            for way in range(2):
                hop(*ring, way, n - 2, piece).wait_recv()

    def ring_drain(*ring):
        def drain(step, c):
            for piece in range(pieces(ring[0])):
                for way in range(2):
                    hop(*ring, way, step, piece).wait_send()
            return c

        lax.fori_loop(0, n - 1, drain, 0)

    w_ring = (w_query.shape[0], w_all, w_ss, w_rs)
    wo_ring = (depth_o, wo_all, wo_ss, wo_rs)
    for copy in copies:
        copy.wait()
    ring_start(*w_ring)

    gate_bias[...] = jnp.zeros_like(gate_bias)
    gate_bias[0:2, :] = input_bias[...]
    gate_bias[2:4, :] = forget_bias[...]
    decay[...] = jnp.zeros_like(decay)
    decay[2:4, :] = decay_shift[...]

    chunk = 32

    def norm_rows(i, c):
        span = pl.ds(pl.multiple_of(i * chunk, chunk), chunk)
        values = tokens[span, :].astype(F32)
        inverse = lax.rsqrt(jnp.mean(values * values, axis=-1, keepdims=True) + EPS)
        normed[span, :] = (values * inverse * norm_gain[...]).astype(BF16)
        return c

    lax.fori_loop(0, rows // chunk, norm_rows, 0)

    gates = dot(w_gates[...], normed[...], NT) + gate_bias[...]
    forget = jnp.minimum(gates, 0.0) - jnp.log1p(jnp.exp(-jnp.abs(gates))) + decay[...]
    row_id = lax.broadcasted_iota(jnp.int32, (rows, rows), 0)
    col_id = lax.broadcasted_iota(jnp.int32, (rows, rows), 1)
    upto = (row_id <= col_id).astype(F32)
    after = (row_id >= col_id).astype(F32)
    sums = (dot(forget, upto, NN, HIGH), dot(forget, after, NN, HIGH))
    gates_t = gates.T
    sums_t = (sums[0].T, sums[1].T)

    lax.fori_loop(1, n - 1, lambda s, c: (ring_step(s, *w_ring), c)[1], 0)
    ring_start(*wo_ring)
    ring_last(*w_ring)
    done = [0]

    def advance():
        if done[0] + 1 < n - 1:
            done[0] += 1
            ring_step(done[0], *wo_ring)

    width = 256

    def project(i, c):
        span = pl.ds(pl.multiple_of(i * width, width), width)
        proj[:, span] = dot(normed[...], w_all[:, span], NN).astype(BF16)
        return c

    lax.fori_loop(0, proj.shape[1] // width, project, 0)

    query = proj[:, :dk]
    keys = proj[:, dk : 2 * dk]
    values = proj[:, 2 * dk : 2 * dk + dv]
    base = 2 * dk + dv
    bw = (proj.shape[1] - base) // 3
    mixed = (proj[:, base + bw : base + 2 * bw].astype(F32) * proj[:, base + 2 * bw :].astype(F32)).astype(BF16).astype(F32)

    keys_f = keys.astype(F32)
    totals = []
    for d in range(2):
        cum_c = sums_t[d][:, 2 + d : 3 + d]
        in_c = gates_t[:, d : d + 1]
        last = rows - 1 if d == 0 else 0
        total = cum_c[last : last + 1, :]
        update = total - cum_c + in_c
        stable = jnp.max(update, axis=0, keepdims=True)
        weighted = keys_f * jnp.exp(update - stable)
        state_out[d] = dot(weighted.astype(BF16), values, TN).astype(BF16)
        edge = mixed[rows - 1 :, :] if d == 0 else mixed[:1, :]
        wide = pack_out.shape[-1]
        pack_out[d, 0:1, :] = edge
        pack_out[d, 1:2, :dk] = jnp.sum(weighted, axis=0, keepdims=True)
        pack_out[d, 1:2, dk:] = jnp.zeros((1, wide - dk), F32)
        pack_out[d, 2:3, :] = jnp.broadcast_to(total, (1, wide))
        pack_out[d, 3:4, :] = jnp.broadcast_to(stable, (1, wide))
        pack_out[d, 4:, :] = jnp.zeros((4, wide), F32)

    def give(o):
        other = lax.rem(me + o, n)
        d = lax.div(me + o, n)
        ids = {"sp": other}
        return (
            pltpu.make_async_remote_copy(state_out.at[d], state_in.at[me], st_ss.at[o], st_rs.at[me], device_id=ids),
            pltpu.make_async_remote_copy(pack_out.at[d], pack_in.at[me], pk_ss.at[o], pk_rs.at[me], device_id=ids),
        )

    def take(o):
        source = lax.rem(me + o, n)
        ids = {"sp": source}
        return (
            pltpu.make_async_remote_copy(state_out.at[0], state_in.at[source], st_ss.at[o], st_rs.at[source], device_id=ids),
            pltpu.make_async_remote_copy(pack_out.at[0], pack_in.at[source], pk_ss.at[o], pk_rs.at[source], device_id=ids),
        )

    def give_all(o, c):
        for copy in give(o):
            copy.start()
        return c

    def take_all(o, c):
        for copy in take(o):
            copy.wait_recv()
        return c

    def give_end(o, c):
        for copy in give(o):
            copy.wait_send()
        return c

    lax.fori_loop(1, n, give_all, 0)
    advance()

    scale = dk ** (-0.5)
    scores = dot(query, keys, NT) * scale
    local = []
    for d in range(2):
        cum_c = sums_t[d][:, 2 + d : 3 + d]
        cum_r = sums[d][2 + d : 3 + d, :]
        in_r = gates[d : d + 1, :]
        allowed = row_id >= col_id if d == 0 else row_id <= col_id
        log_weight = jnp.where(allowed, cum_c - cum_r + in_r, -jnp.inf)
        peak = jnp.max(log_weight, axis=-1, keepdims=True)
        part = scores * jnp.exp(log_weight - peak)
        num = dot(part, values.astype(F32), NN, HIGH)
        local.append((cum_c, peak, num, jnp.sum(part, axis=-1, keepdims=True)))
        advance()

    lax.fori_loop(1, n, take_all, 0)

    before = pack_in[lax.rem(me + n - 1, n), 0:1, :] * jnp.minimum(me, 1).astype(F32)
    behind = pack_in[lax.rem(me + 1, n), 0:1, :] * jnp.minimum(n - 1 - me, 1).astype(F32)
    pos = lax.broadcasted_iota(jnp.int32, mixed.shape, 0)
    prior = jnp.where(pos == 0, before, pltpu.roll(mixed, 1, 0))
    later = jnp.where(pos == rows - 1, behind, pltpu.roll(mixed, rows - 1, 0))
    taps_f = taps[...].astype(F32)
    filtered = taps_f[0:1] * prior + taps_f[1:2] * mixed + taps_f[2:3] * later
    joined[head, :, dv:] = (proj[:, base : base + bw].astype(F32) * filtered).astype(BF16)

    def share(part, o, source):
        columns = pl.ds(part * dv, dv)
        slot = joined.at[source, :, columns]
        return pltpu.make_async_remote_copy(
            slot,
            slot,
            j_ss.at[part, o],
            j_rs.at[part, source],
            device_id={"tp": lax.rem(head + o, t)},
        )

    for o in range(1, t):
        share(1, o, head).start()
    advance()

    summed = None
    query_f = query.astype(F32) * scale
    for d in range(2):
        carry_c[...] = jnp.zeros_like(carry_c)
        carry_n[...] = jnp.zeros_like(carry_n)

        def join(i, peak_in):
            source = i if d == 0 else n - 1 - i
            total = pack_in[source, 2:3, :]
            stable = pack_in[source, 3:4, :]
            new = jnp.maximum(peak_in + total, stable)
            old_w = jnp.exp(peak_in + total - new)
            new_w = jnp.exp(stable - new)
            carry_c[...] = old_w * carry_c[...] + new_w * state_in[source].astype(F32)
            carry_n[...] = old_w * carry_n[...] + new_w * pack_in[source, 1:2, :]
            return new

        peak_in = lax.fori_loop(0, me if d == 0 else n - 1 - me, join, jnp.full((1, dv), LOWEST, F32))
        cum_c, peak, num, den = local[d]
        carried = cum_c + peak_in[:, :1]
        top = jnp.maximum(carried, peak)
        carry_w = jnp.exp(carried - top)
        own_w = jnp.exp(peak - top)
        num = own_w * num + carry_w * dot(query_f, carry_c[...], NN, HIGH)
        den = own_w * den + carry_w * jnp.sum(query_f * carry_n[:, :dk], axis=-1, keepdims=True)
        result = num / jnp.maximum(jnp.abs(den), jnp.exp(-top))
        summed = result if d == 0 else summed + result
        if d == 0:
            advance()
    inverse = lax.rsqrt(jnp.mean(summed * summed, axis=-1, keepdims=True) + EPS)
    joined[head, :, :dv] = (summed * inverse * head_gain[...]).astype(BF16)
    for o in range(1, t):
        share(0, o, head).start()

    lax.fori_loop(done[0] + 1, n - 1, lambda s, c: (ring_step(s, *wo_ring), c)[1], 0)
    ring_last(*wo_ring)
    for part in range(2):
        for o in range(1, t):
            share(part, o, lax.rem(head + o, t)).wait_recv()

    span_j = 2 * dv

    def emit(i, c):
        span = pl.ds(pl.multiple_of(i * width, width), width)
        total = dot(joined[0], wo_all[0:span_j, span], NN)
        for j in range(1, t):
            total += dot(joined[j], wo_all[j * span_j : (j + 1) * span_j, span], NN)
        out[:, span] = total.astype(BF16)
        return c

    lax.fori_loop(0, out.shape[1] // width, emit, 0)
    ring_drain(*w_ring)
    ring_drain(*wo_ring)
    lax.fori_loop(1, n, give_end, 0)
    for part in range(2):
        for o in range(1, t):
            share(part, o, head).wait_send()


def gather_body(
    n,
    t,
    tokens,
    norm_gain,
    w_query,
    w_key,
    w_value,
    w_gates,
    input_bias,
    forget_bias,
    decay_shift,
    head_gain,
    w_conv_b,
    w_conv_c,
    w_conv_in,
    conv_taps,
    w_out,
):
    rows, model = tokens.shape
    dk, dv = w_query.shape[1], w_value.shape[1]
    gates = jnp.transpose(w_gates[..., 0], (2, 1, 0)).reshape(4, model)
    gates = jnp.pad(gates, ((0, 4), (0, 0)))
    depth = w_query.shape[0]
    wide, cols = 2 * dk + dv + 3 * w_conv_b.shape[1], w_out.shape[1]
    hbm = pl.BlockSpec(memory_space=pl.ANY)
    vmem = pl.BlockSpec(memory_space=pltpu.VMEM)
    dma = pltpu.SemaphoreType.DMA
    return pl.pallas_call(
        functools.partial(gather_kernel, n, t, dk, dv),
        out_shape=jax.ShapeDtypeStruct((rows, cols), BF16),
        in_specs=[vmem] * 2 + [hbm] * 7 + [vmem] * 6,
        out_specs=vmem,
        scratch_shapes=[
            pltpu.VMEM((rows, model), BF16),
            pltpu.VMEM((n * depth, wide), BF16),
            pltpu.VMEM((n * w_out.shape[0], cols), BF16),
            pltpu.VMEM((rows, wide), BF16),
            pltpu.VMEM((2, dk, dv), BF16),
            pltpu.VMEM((2, 8, dv), F32),
            pltpu.VMEM((n, dk, dv), BF16),
            pltpu.VMEM((n, 8, dv), F32),
            pltpu.VMEM((dk, dv), F32),
            pltpu.VMEM((1, dv), F32),
            pltpu.VMEM((t, rows, 2 * dv), BF16),
            dma((2, (n - 1) * pieces(depth))),
            dma((2, (n - 1) * pieces(depth))),
            dma((2, (n - 1) * pieces(w_out.shape[0]))),
            dma((2, (n - 1) * pieces(w_out.shape[0]))),
            dma((n,)),
            dma((n,)),
            dma((n,)),
            dma((n,)),
            dma((2, t)),
            dma((2, t)),
            dma((7,)),
            pltpu.VMEM((8, 1), F32),
            pltpu.VMEM((8, rows), F32),
        ],
        compiler_params=pltpu.CompilerParams(
            collective_id=0, has_side_effects=True, vmem_limit_bytes=60 * 1024 * 1024
        ),
    )(
        tokens,
        norm_gain.reshape(1, model),
        w_query,
        w_key,
        w_value,
        w_conv_b,
        w_conv_c,
        w_conv_in,
        w_out,
        gates,
        input_bias,
        forget_bias,
        decay_shift[..., 0],
        head_gain.reshape(1, dv),
        conv_taps,
    )


PAIR = 2
WO_PIECES = 2


def fits(n, t, tokens, norm_gain, w_query, w_key, w_value, *rest):
    w_conv, w_out = rest[5], rest[9]
    depth, dk = w_query.shape
    dv = w_value.shape[1]
    rows = tokens.shape[0]
    even = n % PAIR == 0 and n > PAIR and t == 4
    wide = 2 * dk == dv and w_conv.shape[1] == dv and dv % 128 == 0 and dk % 128 == 0
    deep = (PAIR * depth) % (t * 128) == 0 and rows % 32 == 0 and w_out.shape[0] % (16 * WO_PIECES) == 0
    return even and wide and deep and rows <= depth


def kernel(
    n,
    t,
    dk,
    dv,
    tokens,
    norm_gain,
    w_query,
    w_key,
    w_value,
    w_conv_b,
    w_conv_c,
    w_conv_in,
    w_out,
    w_gates,
    input_bias,
    forget_bias,
    decay_shift,
    head_gain,
    taps,
    out,
    tok,
    nbuf,
    tall,
    wbuf,
    wo_all,
    acc,
    sbuf,
    rbuf,
    proj,
    wg,
    decay,
    state_out,
    pack_out,
    mate_state,
    mate_pack,
    pair_state,
    pair_pack,
    state_in,
    pack_in,
    edge_out,
    edge_in,
    carry_c,
    carry_n,
    local_num,
    joined,
    result,
    out_acc,
    out_sem,
    own_sem,
    tok_sem,
    tk_ss,
    tk_rs,
    tf_ss,
    tf_rs,
    w_ss,
    w_rs,
    rs_ss,
    rs_rs,
    st_ss,
    st_rs,
    pk_ss,
    pk_rs,
    ed_ss,
    ed_rs,
    j_ss,
    j_rs,
    jp_rs,
    oz_ss,
    oz_rs,
    oy_ss,
    oy_rs,
    ox_ss,
    ox_rs,
):
    me = lax.axis_index("sp")
    head = lax.axis_index("tp")
    lines = n // PAIR
    z = lax.div(me, PAIR)
    y = lax.rem(me, PAIR)
    mate = me + 1 - 2 * y
    core = lax.rem(head, 2)
    core_mate = head + 1 - 2 * core
    x_mate = lax.rem(head + 2, t)
    far_mate = lax.rem(core_mate + 2, t)
    rows, model = tokens.shape
    depth = w_query.shape[0]
    part_k = nbuf.shape[-1]
    chunks = wbuf.shape[0]

    def at_line(line):
        return PAIR * line + y

    rows_at_once = 32

    def load_rows(i):
        span = pl.ds(pl.multiple_of(i * rows_at_once, rows_at_once), rows_at_once)
        return pltpu.make_async_copy(tokens.at[span, :], tok.at[span, :], tok_sem.at[i])

    def load_start(i, c):
        load_rows(i).start()
        return c

    lax.fori_loop(0, rows // rows_at_once, load_start, 0)
    mine = pl.ds(pl.multiple_of(y * depth, depth), depth)
    loads = []
    plan = ((w_query, 0, 0), (w_key, 0, dk), (w_value, 1, 0), (w_conv_c, 2, 0), (w_conv_in, 3, 0), (w_conv_b, 4, 0))
    for part, chunk, offset in plan:
        spot = wbuf.at[chunk, mine, pl.ds(offset, part.shape[1])]
        loads.append(pltpu.make_async_copy(part, spot, own_sem.at[1 + len(loads)]))
    depth_o = w_out.shape[0]
    spot = wo_all.at[pl.ds(pl.multiple_of(me * depth_o, depth_o), depth_o), :]
    loads.append(pltpu.make_async_copy(w_out, spot, own_sem.at[1 + len(loads)]))
    for load in loads:
        load.start()

    edge_in[...] = jnp.zeros_like(edge_in)

    barrier = pltpu.get_barrier_semaphore()

    def greet_sp(o, c):
        pl.semaphore_signal(barrier, inc=1, device_id={"sp": lax.rem(me + o, n)})
        return c

    def greet_tp(o, c):
        pl.semaphore_signal(barrier, inc=1, device_id={"tp": lax.rem(head + o, t)})
        return c

    lax.fori_loop(1, n, greet_sp, 0)
    lax.fori_loop(1, t, greet_tp, 0)

    def norm_rows(i, c):
        load_rows(i).wait()
        span = pl.ds(pl.multiple_of(i * rows_at_once, rows_at_once), rows_at_once)
        values = tok[span, :].astype(F32)
        inverse = lax.rsqrt(jnp.mean(values * values, axis=-1, keepdims=True) + EPS)
        normed = (values * inverse * norm_gain[...]).astype(BF16)
        for b in range(lines * t):
            nbuf[b // t, b % t, span, :] = normed[:, b * part_k : (b + 1) * part_k]
        return c

    lax.fori_loop(0, rows // rows_at_once, norm_rows, 0)
    pl.semaphore_wait(barrier, n + t - 2)

    ups = lines - 1 - z

    half_way = lines // 2
    end_here = 1 - jnp.minimum(z, 1) * jnp.minimum(ups, 1)
    inner_up = jnp.minimum(lax.div(ups, half_way), 1)
    inner_count = inner_up * ups + (1 - inner_up) * z

    def pick(k, near):
        up = jnp.clip(ups - k, 0, 1)
        down_k = k - ups
        if near:
            return up, up * (z + 1 + k) + (1 - up) * (z - 1 - down_k)
        return up, up * (lines - 1 - k) + (1 - up) * down_k

    def token_send(line):
        return pltpu.make_async_remote_copy(
            nbuf.at[line, head], tall.at[z, head], tk_ss.at[0], tk_rs.at[z], device_id={"sp": at_line(line)}
        )

    def token_take(line):
        return pltpu.make_async_remote_copy(
            nbuf.at[line, head], tall.at[line, head], tk_ss.at[0], tk_rs.at[line], device_id={"sp": at_line(line)}
        )

    def token_pass(line, way):
        quarter = (head, head, x_mate)[way]
        there = tall.at[line, quarter]
        sem = lines if way != 1 else line
        return pltpu.make_async_remote_copy(
            there, there, tf_ss.at[0], tf_rs.at[sem], device_id={"tp": (core_mate, x_mate, core_mate)[way]}
        )

    def token_get(line):
        there = tall.at[line, x_mate]
        return pltpu.make_async_remote_copy(there, there, tf_ss.at[0], tf_rs.at[line], device_id={"tp": x_mate})

    def send_tokens(k, c):
        _, line = pick(k, False)
        token_send(line).start()
        return c

    lax.fori_loop(0, lines - 1, send_tokens, 0)

    def w_send(chunk):
        there = wbuf.at[chunk, mine, :]
        return pltpu.make_async_remote_copy(there, there, w_ss.at[0], w_rs.at[chunk], device_id={"sp": mate})

    def w_take(chunk):
        there = wbuf.at[chunk, pl.ds(pl.multiple_of((1 - y) * depth, depth), depth), :]
        return pltpu.make_async_remote_copy(there, there, w_ss.at[0], w_rs.at[chunk], device_id={"sp": mate})

    for load in loads:
        load.wait()
    for chunk in range(chunks):
        w_send(chunk).start()

    tall_o = depth_o // WO_PIECES

    def wo_rows(index, piece):
        return wo_all.at[pl.ds(pl.multiple_of(index * depth_o + piece * tall_o, tall_o), tall_o), :]

    def wo_line(line, piece, way, sem):
        there = wo_rows(at_line(line), piece)
        return pltpu.make_async_remote_copy(
            there, there, oz_ss.at[0], oz_rs.at[line, piece], device_id={"sp": at_line(z + way)}
        )

    def wo_mate(line, piece):
        there = wo_rows(at_line(line), piece)
        return pltpu.make_async_remote_copy(
            there, there, oy_ss.at[0], oy_rs.at[line, piece], device_id={"sp": mate}
        )

    def wo_mate_take(line, piece):
        there = wo_rows(PAIR * line + 1 - y, piece)
        return pltpu.make_async_remote_copy(
            there, there, oy_ss.at[0], oy_rs.at[line, piece], device_id={"sp": mate}
        )

    def wo_own(way, wanted):
        @pl.when(wanted)
        def _():
            for piece in range(WO_PIECES):
                wo_line(z, piece, way, lines + (way + 1) // 2).start()

    has_up, has_down = z < lines - 1, z > 0
    at_end = jnp.logical_or(z == 0, z == lines - 1)
    upper = z >= half_way

    def wo_outward():
        wo_own(1, jnp.logical_and(upper, has_up))
        wo_own(-1, jnp.logical_and(jnp.logical_not(upper), has_down))

    def wo_inward(ends):
        here = at_end if ends else jnp.logical_not(at_end)
        wo_own(-1, jnp.logical_and(jnp.logical_and(upper, has_down), here))
        wo_own(1, jnp.logical_and(jnp.logical_and(jnp.logical_not(upper), has_up), here))

    def wo_relay(line, wanted, along, across, pieces_now=range(WO_PIECES)):
        @pl.when(jnp.logical_and(wanted, jnp.logical_and(line >= 0, line < lines)))
        def _():
            for piece in pieces_now:
                if along:
                    wo_line(line, piece, 0, line).wait_recv()

                    @pl.when(jnp.logical_and(line < z, has_up))
                    def _():
                        wo_line(line, piece, 1, line).start()

                    @pl.when(jnp.logical_and(line > z, has_down))
                    def _():
                        wo_line(line, piece, -1, line).start()

                if across:

                    @pl.when(from_mate(line, piece))
                    def _():
                        wo_mate(line, piece).start()

                    if spread and piece == tail_piece:

                        @pl.when(jnp.logical_and(at_end, line == near_line))
                        def _():
                            mate_cut(line, y).start()

    inner_way = 2 * inner_up - 1

    spread = lines == 4
    tail_piece = WO_PIECES - 1
    near_line, far_line = z + inner_way, z + 2 * inner_way
    at_mid = jnp.logical_not(at_end)

    def cut_rows(index, half, halves):
        count = tall_o // halves
        first = index * depth_o + tail_piece * tall_o + half * count
        return wo_all.at[pl.ds(pl.multiple_of(first, count), count), :]

    def mate_cut(line, row):
        there = cut_rows(PAIR * line + row, 1, 2)
        return pltpu.make_async_remote_copy(
            there, there, oy_ss.at[0], oy_rs.at[line, tail_piece], device_id={"sp": mate}
        )

    def along_row(line, way, kind):
        there = cut_rows(PAIR * line + 1 - y, 0, 1 + kind)
        return pltpu.make_async_remote_copy(
            there, there, ox_ss.at[kind], ox_rs.at[kind], device_id={"sp": at_line(z + way)}
        )

    def from_mate(line, piece):
        if not spread or piece != tail_piece:
            return line >= 0
        return jnp.logical_or(
            jnp.logical_and(at_mid, line != far_line), jnp.logical_and(at_end, line != near_line)
        )

    def spread_send():
        if spread:

            @pl.when(at_mid)
            def _():
                wo_mate_take(z, tail_piece).wait_recv()
                along_row(z, -inner_way, 1).start()
                wo_mate_take(z - inner_way, tail_piece).wait_recv()
                along_row(z - inner_way, inner_way, 0).start()

    def wo_first(pieces_now, along=True, across=True, wanted=True):
        wo_relay(z - inner_way * (1 - 2 * end_here), wanted, along, across, pieces_now)

    def wo_second(along, across, pieces_now=range(WO_PIECES)):
        wo_relay(z + inner_way, jnp.logical_not(at_end), along, across, pieces_now)

    def wo_rest(away, pieces_now, along=True, across=True, wanted=True):
        wo_relay(z - away, wanted, along, across, pieces_now)
        wo_relay(z + away, wanted, along, across, pieces_now)

    for piece in range(WO_PIECES):
        wo_mate(z, piece).start()
    wo_inward(True)

    wg[...] = jnp.zeros_like(wg)
    wg[0:2, :] = w_gates[0]
    wg[2:4, :] = w_gates[1]
    decay[...] = jnp.zeros_like(decay)
    decay[1:2, :] = decay_shift[0]
    decay[3:4, :] = decay_shift[1]
    gates = None
    for b in range(lines * t):
        piece = dot(wg[:, b * part_k : (b + 1) * part_k], nbuf[b // t, b % t], NT)
        gates = piece if b == 0 else gates + piece
    gate_id = lax.broadcasted_iota(jnp.int32, gates.shape, 0)
    offsets = (input_bias[0, 0], forget_bias[0, 0], input_bias[0, 1], forget_bias[0, 1])
    for i, offset in enumerate(offsets):
        gates = jnp.where(gate_id == i, gates + offset, gates)
    forget = jnp.minimum(gates, 0.0) - jnp.log1p(jnp.exp(-jnp.abs(gates))) + decay[...]
    row_id = lax.broadcasted_iota(jnp.int32, (rows, rows), 0)
    col_id = lax.broadcasted_iota(jnp.int32, (rows, rows), 1)
    upto = (row_id <= col_id).astype(F32)
    after = (row_id >= col_id).astype(F32)
    sums = (dot(forget, upto, NN, HIGH), dot(forget, after, NN, HIGH))
    gates_t = gates.T
    sums_t = (sums[0].T, sums[1].T)

    def relay_direct(k, c):
        _, line = pick(k, True)
        token_take(line).wait_recv()
        token_pass(line, 1).start()
        token_pass(line, 0).start()
        return c

    def relay_across(k, c):
        _, line = pick(k, True)
        token_get(line).wait_recv()
        token_pass(line, 2).start()
        return c

    lax.fori_loop(0, lines - 1, relay_direct, 0)
    wo_outward()
    wo_inward(False)
    lax.fori_loop(0, lines - 1, relay_across, 0)
    both = tall.at[pl.ds(0, lines - 1), pl.ds(0, 2)]
    pltpu.make_async_remote_copy(both, both, tf_ss.at[0], tf_rs.at[lines], device_id={"tp": core_mate}).wait_recv()
    def parts_of(chunk):
        if isinstance(chunk, int) and chunk == chunks - 1:
            return ((0, rows // 2, chunk), (rows // 2, rows // 2, chunks))
        return ((0, rows, chunk),)

    def hop(chunk, part, k, up, line):
        first, count, sem = part
        last = (1 - up) * (1 - jnp.minimum(jnp.abs(z - line) - 1, 1))
        slot = line + last * (lines - line)
        return pltpu.make_async_remote_copy(
            sbuf.at[chunk, k, pl.ds(first, count)],
            rbuf.at[chunk, slot, pl.ds(first, count)],
            rs_ss.at[0],
            rs_rs.at[sem, slot],
            device_id={"sp": at_line(z + 2 * up - 1)},
        )

    def arrived(chunk, part, slot):
        first, count, sem = part
        return pltpu.make_async_remote_copy(
            sbuf.at[chunk, 0, pl.ds(first, count)],
            rbuf.at[chunk, slot, pl.ds(first, count)],
            rs_ss.at[0],
            rs_rs.at[sem, slot],
            device_id={"sp": me},
        )

    def product(source, line, chunk, part):
        span = pl.ds(part[0], part[1])
        total = dot(source[line, 0, span, :], wbuf[chunk, 0:part_k, :], NN)
        for q in range(1, t):
            total += dot(source[line, q, span, :], wbuf[chunk, q * part_k : (q + 1) * part_k, :], NN)
        return total

    def add_along(chunk, part, slot, up, line):
        span = pl.ds(part[0], part[1])
        acc[span, :] = product(tall, line, chunk, part)
        before = up * jnp.minimum(z, 1) + (1 - up) * jnp.minimum(ups, 1)

        @pl.when(before == 1)
        def _():
            arrived(chunk, part, line).wait_recv()
            sbuf[chunk, slot, span, :] = (acc[span, :] + rbuf[chunk, line, span, :].astype(F32)).astype(BF16)

        @pl.when(before == 0)
        def _():
            sbuf[chunk, slot, span, :] = acc[span, :].astype(BF16)

        hop(chunk, part, slot, up, line).start()

    def inward_span(first, last, chunk):
        def one(k, c):
            line = inner_up * (lines - 1 - k) + (1 - inner_up) * k
            for part in parts_of(chunk):
                add_along(chunk, part, k, inner_up, line)
            return c

        lax.fori_loop(first, last, one, 0)

    def inward_where(runs, chunk):
        @pl.when(runs == 1)
        def _():
            w_take(chunk).wait_recv()

        inward_span(0, runs * inner_count, chunk)

    def inward(end_chunk, mid_chunk):
        end_runs, mid_runs = end_chunk < chunks, mid_chunk >= 0
        if end_runs and mid_runs and max(end_chunk, mid_chunk) < chunks - 1:
            inward_where(1, end_here * end_chunk + (1 - end_here) * mid_chunk)
            return
        if end_runs:
            inward_where(end_here, end_chunk)
        if mid_runs:
            inward_where(1 - end_here, mid_chunk)

    def outward(chunk):
        for part in parts_of(chunk):

            def one(k, c):
                line = (1 - inner_up) * (lines - 1 - k) + inner_up * k
                add_along(chunk, part, inner_count + k, 1 - inner_up, line)
                return c

            lax.fori_loop(0, lines - 1 - inner_count, one, 0)

    def own_part(chunk, part):
        span = pl.ds(part[0], part[1])
        acc[span, :] = product(nbuf, z, chunk, part)

        @pl.when(has_down)
        def _():
            arrived(chunk, part, z).wait_recv()
            acc[span, :] += rbuf[chunk, z, span, :].astype(F32)

        @pl.when(has_up)
        def _():
            arrived(chunk, part, lines).wait_recv()
            acc[span, :] += rbuf[chunk, lines, span, :].astype(F32)

    def own_chunk(chunk):
        own_part(chunk, parts_of(chunk)[0])
        proj[chunk] = acc[...].astype(BF16)

    inward(0, -1)
    inward(1, -1)
    inward(2, 0)
    wo_first((0,))
    wo_second(True, False, (0,))
    inward(3, 1)
    wo_first(range(1, WO_PIECES), True, False)
    outward(0)
    wo_second(True, False, range(1, WO_PIECES))
    own_chunk(0)
    wo_rest(2, (0,), True, True, at_end)
    inward(chunks, 2)
    outward(1)
    own_chunk(1)

    keys_f = proj[0, :, dk:].astype(F32)
    wide = pack_out.shape[-1]
    for d in range(2):
        cum_c = sums_t[d][:, 2 * d + 1 : 2 * d + 2]
        in_c = gates_t[:, 2 * d : 2 * d + 1]
        last = rows - 1 if d == 0 else 0
        total = cum_c[last : last + 1, :]
        update = total - cum_c + in_c
        stable = jnp.max(update, axis=0, keepdims=True)
        weighted = keys_f * jnp.exp(update - stable)
        state_out[d] = dot(weighted.astype(BF16), proj[1], TN).astype(BF16)
        pack_out[d, 0:1, :dk] = jnp.sum(weighted, axis=0, keepdims=True)
        pack_out[d, 0:1, dk:] = jnp.zeros((1, wide - dk), F32)
        pack_out[d, 1:2, :] = jnp.broadcast_to(total, (1, wide))
        pack_out[d, 2:3, :] = jnp.broadcast_to(stable, (1, wide))
        pack_out[d, 3:, :] = jnp.zeros((5, wide), F32)

    def swap_states():
        return (
            pltpu.make_async_remote_copy(state_out, mate_state, st_ss.at[2], st_rs.at[2], device_id={"sp": mate}),
            pltpu.make_async_remote_copy(pack_out, mate_pack, pk_ss.at[2], pk_rs.at[2], device_id={"sp": mate}),
        )

    for copy in swap_states():
        copy.start()
    wo_first(range(1, WO_PIECES), False, True)
    wo_second(False, True, (0,))
    wo_rest(2, (0,), True, False, at_mid)
    wo_rest(2, range(1, WO_PIECES), True, False)
    wo_rest(2, range(1, WO_PIECES), False, True, at_end)

    d_in, d_out = 1 - inner_up, inner_up

    def chain(d, way):
        ids = {"sp": at_line(z + way)}
        return (
            pltpu.make_async_remote_copy(pair_state.at[d], state_in.at[d], st_ss.at[d], st_rs.at[d], device_id=ids),
            pltpu.make_async_remote_copy(pair_pack.at[d], pack_in.at[d], pk_ss.at[d], pk_rs.at[d], device_id=ids),
        )

    def chain_add(d):
        for copy in chain(d, 0):
            copy.wait_recv()
        total, stable, first_w, second_w = blend(pack_in[d], pair_pack[d])
        joint = first_w[:, :1] * state_in[d].astype(F32) + second_w[:, :1] * pair_state[d].astype(F32)
        pair_state[d] = joint.astype(BF16)
        pair_pack[d, 0:1, :] = first_w * pack_in[d, 0:1, :] + second_w * pair_pack[d, 0:1, :]
        pair_pack[d, 1:2, :] = total
        pair_pack[d, 2:3, :] = stable

    def chain_from_end():
        @pl.when(at_end)
        def _():
            for copy in chain(d_in, inner_way):
                copy.start()

    def chain_inward():
        @pl.when(jnp.logical_not(at_end))
        def _():
            chain_add(d_in)
            for copy in chain(d_in, inner_way):
                copy.start()

    def chain_outward():
        @pl.when(jnp.logical_not(at_end))
        def _():
            chain_add(d_out)
            for copy in chain(d_out, -inner_way):
                copy.start()

        @pl.when(at_end)
        def _():
            for copy in chain(d_out, 0):
                copy.wait_recv()

    def blend(first, second):
        total = first[1:2, :] + second[1:2, :]
        moved = first[2:3, :] + second[1:2, :]
        stable = jnp.maximum(moved, second[2:3, :])
        return total, stable, jnp.exp(moved - stable), jnp.exp(second[2:3, :] - stable)

    def pair_up():
        for copy in swap_states():
            copy.wait_recv()
        own_first = (1 - y).astype(F32)
        for d in range(2):
            lead = own_first if d == 0 else 1.0 - own_first
            mine_p, other_p = pack_out[d], mate_pack[d]
            first = lead * mine_p + (1.0 - lead) * other_p
            second = lead * other_p + (1.0 - lead) * mine_p
            total, stable, first_w, second_w = blend(first, second)
            mine_w = lead * first_w + (1.0 - lead) * second_w
            other_w = lead * second_w + (1.0 - lead) * first_w
            joint = mine_w * state_out[d].astype(F32) + other_w * mate_state[d].astype(F32)
            pair_state[d] = joint.astype(BF16)
            pair_pack[d, 0:1, :] = mine_w * mine_p[0:1, :] + other_w * other_p[0:1, :]
            pair_pack[d, 1:2, :] = total
            pair_pack[d, 2:3, :] = stable
            pair_pack[d, 3:, :] = jnp.zeros((5, wide), F32)

    inward(chunks, 3)
    pair_up()
    chain_from_end()
    inward(4, -1)
    outward(2)
    for away in range(3, lines):
        wo_rest(away, (0,))
    own_chunk(2)

    scale = dk ** (-0.5)
    scores = dot(proj[0, :, :dk], proj[0, :, dk:], NT) * scale
    local = []
    for d in range(2):
        cum_c = sums_t[d][:, 2 * d + 1 : 2 * d + 2]
        cum_r = sums[d][2 * d + 1 : 2 * d + 2, :]
        in_r = gates[2 * d : 2 * d + 1, :]
        allowed = row_id >= col_id if d == 0 else row_id <= col_id
        log_weight = jnp.where(allowed, cum_c - cum_r + in_r, -jnp.inf)
        peak = jnp.max(log_weight, axis=-1, keepdims=True)
        part = scores * jnp.exp(log_weight - peak)
        local_num[d] = dot(part.astype(BF16), proj[1], NN)
        local.append((cum_c, peak, jnp.sum(part, axis=-1, keepdims=True)))

    outward(3)
    own_chunk(3)

    mixed = (proj[2].astype(F32) * proj[3].astype(F32)).astype(BF16).astype(F32)
    edge_out[0, 0:1, :] = mixed[rows - 1 :, :]
    edge_out[1, 0:1, :] = mixed[:1, :]
    edge_out[0, 1:, :] = jnp.zeros((7, dv), F32)
    edge_out[1, 1:, :] = jnp.zeros((7, dv), F32)

    def edge(way):
        other = me + 1 if way == 0 else me - 1
        return pltpu.make_async_remote_copy(
            edge_out.at[way], edge_in.at[way], ed_ss.at[way], ed_rs.at[way], device_id={"sp": other}
        )

    later_exists, prior_exists = me < n - 1, me > 0

    @pl.when(later_exists)
    def _():
        edge(0).start()

    @pl.when(prior_exists)
    def _():
        edge(1).start()

    wo_second(False, True, range(1, WO_PIECES))
    wo_rest(2, range(WO_PIECES), False, True, jnp.logical_not(at_end))
    chain_inward()


    @pl.when(at_mid)
    def _():
        w_take(4).wait_recv()

    inward_span(0, 1 - end_here, 4)
    chain_outward()
    inward_span(1, (1 - end_here) * inner_count, 4)
    for away in range(3, lines):
        wo_rest(away, range(1, WO_PIECES))

    half_rows = rows // 2

    def joined_part(part, source, way):
        columns = pl.ds(part * dv, dv)
        if way == 0:
            return joined.at[source, :, columns]
        return joined.at[source, pl.ds((way - 1) * half_rows, half_rows), columns]

    others = (core_mate, x_mate, far_mate)

    def share(part, way, source):
        slot = joined_part(part, source, way)
        return pltpu.make_async_remote_copy(
            slot, slot, j_ss.at[0], j_rs.at[part, way], device_id={"tp": others[way]}
        )

    def share_pass(part, way, source):
        slot = joined_part(part, source, way)
        return pltpu.make_async_remote_copy(
            slot, slot, j_ss.at[0], jp_rs.at[part, way - 1], device_id={"tp": core_mate}
        )

    def share_start(part):
        for way in (1, 2, 0):
            share(part, way, head).start()

    def share_relay(part):
        for way in (1, 2):
            share(part, way, others[way]).wait_recv()
            share_pass(part, way, others[way]).start()

    def share_wait(part):
        share(part, 0, core_mate).wait_recv()
        for way in (1, 2):
            share_pass(part, way, others[3 - way]).wait_recv()

    summed = None
    query_f = proj[0, :, :dk].astype(F32) * scale
    for d in range(2):
        carry_c[...] = jnp.zeros_like(carry_c)
        carry_n[...] = jnp.zeros_like(carry_n)

        def merge(state, pack, peak_in):
            total = pack[1:2, :]
            stable = pack[2:3, :]
            new = jnp.maximum(peak_in + total, stable)
            old_w = jnp.exp(peak_in + total - new)
            new_w = jnp.exp(stable - new)
            carry_c[...] = old_w * carry_c[...] + new_w * state.astype(F32)
            carry_n[...] = old_w * carry_n[...] + new_w * pack[0:1, :]
            return new

        def join(i, peak_in):
            return merge(state_in[d], pack_in[d], peak_in)

        def join_mate(i, peak_in):
            return merge(mate_state[d], mate_pack[d], peak_in)

        peak_in = lax.fori_loop(0, jnp.minimum(z if d == 0 else ups, 1), join, jnp.full((1, dv), LOWEST, F32))
        peak_in = lax.fori_loop(0, y if d == 0 else 1 - y, join_mate, peak_in)
        cum_c, peak, den = local[d]
        carried = cum_c + peak_in[:, :1]
        top = jnp.maximum(carried, peak)
        carry_w = jnp.exp(carried - top)
        own_w = jnp.exp(peak - top)
        num = own_w * local_num[d] + carry_w * dot(query_f.astype(BF16), carry_c[...].astype(BF16), NN)
        den = own_w * den + carry_w * jnp.sum(query_f * carry_n[:, :dk], axis=-1, keepdims=True)
        cell = num / jnp.maximum(jnp.abs(den), jnp.exp(-top))
        summed = cell if d == 0 else summed + cell
    inverse = lax.rsqrt(jnp.mean(summed * summed, axis=-1, keepdims=True) + EPS)
    joined[head, :, :dv] = (summed * inverse * head_gain[...]).astype(BF16)
    share_start(0)
    outward(4)
    spread_send()

    @pl.when(prior_exists)
    def _():
        edge(0).wait_recv()

    @pl.when(later_exists)
    def _():
        edge(1).wait_recv()

    mixed = (proj[2].astype(F32) * proj[3].astype(F32)).astype(BF16).astype(F32)
    pos = lax.broadcasted_iota(jnp.int32, mixed.shape, 0)
    prior = jnp.where(pos == 0, edge_in[0, 0:1, :], pltpu.roll(mixed, 1, 0))
    later = jnp.where(pos == rows - 1, edge_in[1, 0:1, :], pltpu.roll(mixed, rows - 1, 0))
    taps_f = taps[...].astype(F32)
    local_num[0] = taps_f[0:1] * prior + taps_f[1:2] * mixed + taps_f[2:3] * later
    for i, part in enumerate(parts_of(chunks - 1)):
        span = pl.ds(part[0], part[1])
        own_part(chunks - 1, part)
        outer = acc[span, :].astype(BF16).astype(F32)
        joined[head, span, dv:] = (outer * local_num[0, span, :]).astype(BF16)
        share(1, 1 + i, head).start()
    share(1, 0, head).start()
    share_relay(0)
    share_relay(1)

    for line in range(lines):
        for piece in range(WO_PIECES):
            if not spread or piece != tail_piece:
                wo_mate_take(line, piece).wait_recv()
                continue

            @pl.when(jnp.logical_or(jnp.logical_and(at_mid, line == near_line), jnp.logical_and(at_end, line != near_line)))
            def _():
                wo_mate_take(line, piece).wait_recv()

    if spread:

        @pl.when(at_mid)
        def _():
            along_row(far_line, 0, 0).wait_recv()

        @pl.when(at_end)
        def _():
            along_row(near_line, 0, 1).wait_recv()
            mate_cut(near_line, 1 - y).wait_recv()

    share_wait(0)
    width = 512

    def columns_of(part, i):
        span = pl.ds(pl.multiple_of(i * width, width), width)
        total = None
        for j in range(t):
            first = (2 * j + part) * dv
            term = dot(joined[j, :, part * dv : (part + 1) * dv], wo_all[first : first + dv, span], NN)
            total = term if j == 0 else total + term
        return span, total

    def emit_cell(i, c):
        span, total = columns_of(0, i)
        out_acc[:, span] = total
        return c

    def emit(i, c):
        span, total = columns_of(1, i)
        result[:, span] = (out_acc[:, span] + total).astype(BF16)
        put(i).start()
        return c

    def put(i):
        span = pl.ds(pl.multiple_of(i * width, width), width)
        return pltpu.make_async_copy(result.at[:, span], out.at[:, span], out_sem.at[i])

    def put_end(i, c):
        put(i).wait()
        return c

    lax.fori_loop(0, out.shape[1] // width, emit_cell, 0)
    share_wait(1)
    lax.fori_loop(0, out.shape[1] // width, emit, 0)

    def sent(ref, sem):
        pltpu.make_async_remote_copy(ref, ref, sem.at[0], w_rs.at[0], device_id={"sp": mate}).wait_send()

    sent(nbuf.at[pl.ds(0, lines - 1), 0], tk_ss)
    sent(tall.at[pl.ds(0, lines - 1), pl.ds(0, 3)], tf_ss)
    sent(wbuf.at[:, mine, :], w_ss)
    sent(sbuf, rs_ss)
    sent(joined.at[pl.ds(0, 3)], j_ss)

    @pl.when(at_end)
    def _():
        sent(wo_all.at[pl.ds(0, depth_o)], oz_ss)

    @pl.when(at_mid)
    def _():
        sent(wo_all.at[pl.ds(0, (lines + 1) * depth_o)], oz_ss)

    if spread:

        @pl.when(at_end)
        def _():
            sent(wo_all.at[pl.ds(0, lines * depth_o - tall_o + tall_o // 2)], oy_ss)

        @pl.when(at_mid)
        def _():
            sent(wo_all.at[pl.ds(0, lines * depth_o - tall_o)], oy_ss)
            along_row(z, -inner_way, 1).wait_send()
            along_row(z - inner_way, inner_way, 0).wait_send()

    else:
        sent(wo_all.at[pl.ds(0, lines * depth_o)], oy_ss)

    for copy in swap_states():
        copy.wait_send()

    @pl.when(at_end)
    def _():
        for copy in chain(d_in, inner_way):
            copy.wait_send()

    @pl.when(jnp.logical_not(at_end))
    def _():
        for copy in chain(d_in, inner_way) + chain(d_out, -inner_way):
            copy.wait_send()


    @pl.when(later_exists)
    def _():
        edge(0).wait_send()

    @pl.when(prior_exists)
    def _():
        edge(1).wait_send()


    lax.fori_loop(0, out.shape[1] // width, put_end, 0)

def body(
    n,
    t,
    tokens,
    norm_gain,
    w_query,
    w_key,
    w_value,
    w_gates,
    input_bias,
    forget_bias,
    decay_shift,
    head_gain,
    w_conv_b,
    w_conv_c,
    w_conv_in,
    conv_taps,
    w_out,
):
    rows, model = tokens.shape
    depth, dk = w_query.shape
    dv = w_value.shape[1]
    lines = n // PAIR
    chunks = 5
    part_k = PAIR * depth // t
    cols = w_out.shape[1]
    gates = jnp.transpose(w_gates[..., 0], (1, 2, 0))
    hbm = pl.BlockSpec(memory_space=pl.ANY)
    vmem = pl.BlockSpec(memory_space=pltpu.VMEM)
    smem = pl.BlockSpec(memory_space=pltpu.SMEM)
    dma = pltpu.SemaphoreType.DMA
    return pl.pallas_call(
        functools.partial(kernel, n, t, dk, dv),
        out_shape=jax.ShapeDtypeStruct((rows, cols), BF16),
        in_specs=[hbm, vmem] + [hbm] * 7 + [vmem] + [smem] * 2 + [vmem] * 3,
        out_specs=hbm,
        scratch_shapes=[
            pltpu.VMEM((rows, model), BF16),
            pltpu.VMEM((lines, t, rows, part_k), BF16),
            pltpu.VMEM((lines, t, rows, part_k), BF16),
            pltpu.VMEM((chunks, PAIR * depth, dv), BF16),
            pltpu.VMEM((n * w_out.shape[0], cols), BF16),
            pltpu.VMEM((rows, dv), F32),
            pltpu.VMEM((chunks, lines - 1, rows, dv), BF16),
            pltpu.VMEM((chunks, lines + 1, rows, dv), BF16),
            pltpu.VMEM((chunks, rows, dv), BF16),
            pltpu.VMEM((8, model), BF16),
            pltpu.VMEM((8, rows), F32),
            pltpu.VMEM((2, dk, dv), BF16),
            pltpu.VMEM((2, 8, dv), F32),
            pltpu.VMEM((2, dk, dv), BF16),
            pltpu.VMEM((2, 8, dv), F32),
            pltpu.VMEM((2, dk, dv), BF16),
            pltpu.VMEM((2, 8, dv), F32),
            pltpu.VMEM((2, dk, dv), BF16),
            pltpu.VMEM((2, 8, dv), F32),
            pltpu.VMEM((2, 8, dv), F32),
            pltpu.VMEM((2, 8, dv), F32),
            pltpu.VMEM((dk, dv), F32),
            pltpu.VMEM((1, dv), F32),
            pltpu.VMEM((2, rows, dv), F32),
            pltpu.VMEM((t, rows, 2 * dv), BF16),
            pltpu.VMEM((rows, cols), BF16),
            pltpu.VMEM((rows, cols), F32),
            dma((cols // 256,)),
            dma((8,)),
            dma((rows // 32,)),
            dma((1,)),
            dma((lines,)),
            dma((1,)),
            dma((lines + 1,)),
            dma((1,)),
            dma((chunks,)),
            dma((1,)),
            dma((chunks + 1, lines + 1)),
            dma((3,)),
            dma((3,)),
            dma((3,)),
            dma((3,)),
            dma((2,)),
            dma((2,)),
            dma((1,)),
            dma((2, 3)),
            dma((2, 2)),
            dma((1,)),
            dma((lines, WO_PIECES)),
            dma((1,)),
            dma((lines, WO_PIECES)),
            dma((2,)),
            dma((2,)),
        ],
        compiler_params=pltpu.CompilerParams(
            collective_id=0, has_side_effects=True, vmem_limit_bytes=60 * 1024 * 1024
        ),
    )(
        tokens,
        norm_gain.reshape(1, model),
        w_query,
        w_key,
        w_value,
        w_conv_b,
        w_conv_c,
        w_conv_in,
        w_out,
        gates,
        input_bias.T,
        forget_bias.T,
        jnp.swapaxes(decay_shift, 1, 2),
        head_gain.reshape(1, dv),
        conv_taps,
    )


def solution(mesh):
    placed = (
        P("sp", None),
        P(),
        P("sp", "tp"),
        P("sp", "tp"),
        P("sp", "tp"),
        P(None, None, None, "tp"),
        P(None, "tp"),
        P(None, "tp"),
        P(None, "sp", "tp"),
        P("tp"),
        P("sp", "tp"),
        P("sp", "tp"),
        P("sp", "tp"),
        P(None, "tp"),
        P("sp", "tp"),
    )
    n, t = mesh.shape["sp"], mesh.shape["tp"]

    def step(*args):
        form = body if fits(n, t, *args) else gather_body
        return form(n, t, *args)

    return jax.shard_map(step, mesh=mesh, in_specs=placed, out_specs=P("sp", "tp"), check_vma=False)
```

```python
import functools

import jax
import jax.numpy as jnp
from jax import lax
from jax.experimental import pallas as pl
from jax.experimental.pallas import tpu as pltpu
from jax.sharding import PartitionSpec as P

EPS = 1e-06
HIGH = lax.Precision.HIGHEST
LOWEST = -1e30
PIECES = 4
F32 = jnp.float32
BF16 = jnp.bfloat16


def dot(a, b, dims, precision=None):
    return lax.dot_general(a, b, (dims, ((), ())), precision=precision, preferred_element_type=F32)


NN = ((1,), (0,))
NT = ((1,), (1,))
TN = ((0,), (0,))


def ring_place(index, n):
    odd = lax.rem(index, 2)
    half = lax.div(index, 2)
    return (1 - odd) * half + odd * (n - 1 - half)


def ring_index(place, n):
    late = lax.div(place, n // 2)
    return (1 - late) * (2 * place) + late * (2 * (n - 1 - place) + 1)


def pieces(depth):
    return max(1, min(PIECES, depth // 16))


def gather_kernel(
    n,
    t,
    dk,
    dv,
    tokens,
    norm_gain,
    w_query,
    w_key,
    w_value,
    w_conv_b,
    w_conv_c,
    w_conv_in,
    w_out,
    w_gates,
    input_bias,
    forget_bias,
    decay_shift,
    head_gain,
    taps,
    out,
    normed,
    w_all,
    wo_all,
    proj,
    state_out,
    pack_out,
    state_in,
    pack_in,
    carry_c,
    carry_n,
    joined,
    w_ss,
    w_rs,
    wo_ss,
    wo_rs,
    st_ss,
    st_rs,
    pk_ss,
    pk_rs,
    j_ss,
    j_rs,
    own_sem,
    gate_bias,
    decay,
):
    me = lax.axis_index("sp")
    head = lax.axis_index("tp")
    place = ring_place(me, n)
    right = ring_index(lax.rem(place + 1, n), n)
    left = ring_index(lax.rem(place + n - 1, n), n)
    rows = tokens.shape[0]

    parts = (w_query, w_key, w_value, w_conv_b, w_conv_c, w_conv_in)
    copies = []
    offset = 0
    for part in parts:
        depth, cols = part.shape
        spot = w_all.at[pl.ds(pl.multiple_of(me * depth, depth), depth), pl.ds(offset, cols)]
        copies.append(pltpu.make_async_copy(part, spot, own_sem.at[len(copies)]))
        offset += cols
    depth_o = w_out.shape[0]
    spot = wo_all.at[pl.ds(pl.multiple_of(me * depth_o, depth_o), depth_o), :]
    copies.append(pltpu.make_async_copy(w_out, spot, own_sem.at[len(copies)]))
    for copy in copies:
        copy.start()

    barrier = pltpu.get_barrier_semaphore()

    def greet_sp(o, c):
        pl.semaphore_signal(barrier, inc=1, device_id={"sp": lax.rem(me + o, n)})
        return c

    def greet_tp(o, c):
        pl.semaphore_signal(barrier, inc=1, device_id={"tp": lax.rem(head + o, t)})
        return c

    lax.fori_loop(1, n, greet_sp, 0)
    lax.fori_loop(1, t, greet_tp, 0)
    pl.semaphore_wait(barrier, n + t - 2)

    def hop(depth, whole, ss, rs, way, step, piece):
        width = whole.shape[1]
        half, tall = width // 2, depth // pieces(depth)
        holder = ring_index(lax.rem(place + (n + step if way else n - step), n), n)
        columns = pl.ds(way * half, half)
        there = whole.at[pl.ds(pl.multiple_of(holder * depth + piece * tall, tall), tall), columns]
        turn = step * pieces(depth) + piece
        return pltpu.make_async_remote_copy(
            src_ref=there,
            dst_ref=there,
            send_sem=ss.at[way, turn],
            recv_sem=rs.at[way, turn],
            device_id={"sp": left if way else right},
        )

    def ring_start(*ring):
        for piece in range(pieces(ring[0])):
            for way in range(2):
                hop(*ring, way, 0, piece).start()

    def ring_step(step, *ring):
        for piece in range(pieces(ring[0])):
            for way in range(2):
                hop(*ring, way, step - 1, piece).wait_recv()
                hop(*ring, way, step, piece).start()

    def ring_last(*ring):
        for piece in range(pieces(ring[0])):
            for way in range(2):
                hop(*ring, way, n - 2, piece).wait_recv()

    def ring_drain(*ring):
        def drain(step, c):
            for piece in range(pieces(ring[0])):
                for way in range(2):
                    hop(*ring, way, step, piece).wait_send()
            return c

        lax.fori_loop(0, n - 1, drain, 0)

    w_ring = (w_query.shape[0], w_all, w_ss, w_rs)
    wo_ring = (depth_o, wo_all, wo_ss, wo_rs)
    for copy in copies:
        copy.wait()
    ring_start(*w_ring)

    gate_bias[...] = jnp.zeros_like(gate_bias)
    gate_bias[0:2, :] = input_bias[...]
    gate_bias[2:4, :] = forget_bias[...]
    decay[...] = jnp.zeros_like(decay)
    decay[2:4, :] = decay_shift[...]

    chunk = 32

    def norm_rows(i, c):
        span = pl.ds(pl.multiple_of(i * chunk, chunk), chunk)
        values = tokens[span, :].astype(F32)
        inverse = lax.rsqrt(jnp.mean(values * values, axis=-1, keepdims=True) + EPS)
        normed[span, :] = (values * inverse * norm_gain[...]).astype(BF16)
        return c

    lax.fori_loop(0, rows // chunk, norm_rows, 0)

    gates = dot(w_gates[...], normed[...], NT) + gate_bias[...]
    forget = jnp.minimum(gates, 0.0) - jnp.log1p(jnp.exp(-jnp.abs(gates))) + decay[...]
    row_id = lax.broadcasted_iota(jnp.int32, (rows, rows), 0)
    col_id = lax.broadcasted_iota(jnp.int32, (rows, rows), 1)
    upto = (row_id <= col_id).astype(F32)
    after = (row_id >= col_id).astype(F32)
    sums = (dot(forget, upto, NN, HIGH), dot(forget, after, NN, HIGH))
    gates_t = gates.T
    sums_t = (sums[0].T, sums[1].T)

    lax.fori_loop(1, n - 1, lambda s, c: (ring_step(s, *w_ring), c)[1], 0)
    ring_start(*wo_ring)
    ring_last(*w_ring)
    done = [0]

    def advance():
        if done[0] + 1 < n - 1:
            done[0] += 1
            ring_step(done[0], *wo_ring)

    width = 256

    def project(i, c):
        span = pl.ds(pl.multiple_of(i * width, width), width)
        proj[:, span] = dot(normed[...], w_all[:, span], NN).astype(BF16)
        return c

    lax.fori_loop(0, proj.shape[1] // width, project, 0)

    query = proj[:, :dk]
    keys = proj[:, dk : 2 * dk]
    values = proj[:, 2 * dk : 2 * dk + dv]
    base = 2 * dk + dv
    bw = (proj.shape[1] - base) // 3
    mixed = (proj[:, base + bw : base + 2 * bw].astype(F32) * proj[:, base + 2 * bw :].astype(F32)).astype(BF16).astype(F32)

    keys_f = keys.astype(F32)
    totals = []
    for d in range(2):
        cum_c = sums_t[d][:, 2 + d : 3 + d]
        in_c = gates_t[:, d : d + 1]
        last = rows - 1 if d == 0 else 0
        total = cum_c[last : last + 1, :]
        update = total - cum_c + in_c
        stable = jnp.max(update, axis=0, keepdims=True)
        weighted = keys_f * jnp.exp(update - stable)
        state_out[d] = dot(weighted.astype(BF16), values, TN).astype(BF16)
        edge = mixed[rows - 1 :, :] if d == 0 else mixed[:1, :]
        wide = pack_out.shape[-1]
        pack_out[d, 0:1, :] = edge
        pack_out[d, 1:2, :dk] = jnp.sum(weighted, axis=0, keepdims=True)
        pack_out[d, 1:2, dk:] = jnp.zeros((1, wide - dk), F32)
        pack_out[d, 2:3, :] = jnp.broadcast_to(total, (1, wide))
        pack_out[d, 3:4, :] = jnp.broadcast_to(stable, (1, wide))
        pack_out[d, 4:, :] = jnp.zeros((4, wide), F32)

    def give(o):
        other = lax.rem(me + o, n)
        d = lax.div(me + o, n)
        ids = {"sp": other}
        return (
            pltpu.make_async_remote_copy(state_out.at[d], state_in.at[me], st_ss.at[o], st_rs.at[me], device_id=ids),
            pltpu.make_async_remote_copy(pack_out.at[d], pack_in.at[me], pk_ss.at[o], pk_rs.at[me], device_id=ids),
        )

    def take(o):
        source = lax.rem(me + o, n)
        ids = {"sp": source}
        return (
            pltpu.make_async_remote_copy(state_out.at[0], state_in.at[source], st_ss.at[o], st_rs.at[source], device_id=ids),
            pltpu.make_async_remote_copy(pack_out.at[0], pack_in.at[source], pk_ss.at[o], pk_rs.at[source], device_id=ids),
        )

    def give_all(o, c):
        for copy in give(o):
            copy.start()
        return c

    def take_all(o, c):
        for copy in take(o):
            copy.wait_recv()
        return c

    def give_end(o, c):
        for copy in give(o):
            copy.wait_send()
        return c

    lax.fori_loop(1, n, give_all, 0)
    advance()

    scale = dk ** (-0.5)
    scores = dot(query, keys, NT) * scale
    local = []
    for d in range(2):
        cum_c = sums_t[d][:, 2 + d : 3 + d]
        cum_r = sums[d][2 + d : 3 + d, :]
        in_r = gates[d : d + 1, :]
        allowed = row_id >= col_id if d == 0 else row_id <= col_id
        log_weight = jnp.where(allowed, cum_c - cum_r + in_r, -jnp.inf)
        peak = jnp.max(log_weight, axis=-1, keepdims=True)
        part = scores * jnp.exp(log_weight - peak)
        num = dot(part, values.astype(F32), NN, HIGH)
        local.append((cum_c, peak, num, jnp.sum(part, axis=-1, keepdims=True)))
        advance()

    lax.fori_loop(1, n, take_all, 0)

    before = pack_in[lax.rem(me + n - 1, n), 0:1, :] * jnp.minimum(me, 1).astype(F32)
    behind = pack_in[lax.rem(me + 1, n), 0:1, :] * jnp.minimum(n - 1 - me, 1).astype(F32)
    pos = lax.broadcasted_iota(jnp.int32, mixed.shape, 0)
    prior = jnp.where(pos == 0, before, pltpu.roll(mixed, 1, 0))
    later = jnp.where(pos == rows - 1, behind, pltpu.roll(mixed, rows - 1, 0))
    taps_f = taps[...].astype(F32)
    filtered = taps_f[0:1] * prior + taps_f[1:2] * mixed + taps_f[2:3] * later
    joined[head, :, dv:] = (proj[:, base : base + bw].astype(F32) * filtered).astype(BF16)

    def share(part, o, source):
        columns = pl.ds(part * dv, dv)
        slot = joined.at[source, :, columns]
        return pltpu.make_async_remote_copy(
            slot,
            slot,
            j_ss.at[part, o],
            j_rs.at[part, source],
            device_id={"tp": lax.rem(head + o, t)},
        )

    for o in range(1, t):
        share(1, o, head).start()
    advance()

    summed = None
    query_f = query.astype(F32) * scale
    for d in range(2):
        carry_c[...] = jnp.zeros_like(carry_c)
        carry_n[...] = jnp.zeros_like(carry_n)

        def join(i, peak_in):
            source = i if d == 0 else n - 1 - i
            total = pack_in[source, 2:3, :]
            stable = pack_in[source, 3:4, :]
            new = jnp.maximum(peak_in + total, stable)
            old_w = jnp.exp(peak_in + total - new)
            new_w = jnp.exp(stable - new)
            carry_c[...] = old_w * carry_c[...] + new_w * state_in[source].astype(F32)
            carry_n[...] = old_w * carry_n[...] + new_w * pack_in[source, 1:2, :]
            return new

        peak_in = lax.fori_loop(0, me if d == 0 else n - 1 - me, join, jnp.full((1, dv), LOWEST, F32))
        cum_c, peak, num, den = local[d]
        carried = cum_c + peak_in[:, :1]
        top = jnp.maximum(carried, peak)
        carry_w = jnp.exp(carried - top)
        own_w = jnp.exp(peak - top)
        num = own_w * num + carry_w * dot(query_f, carry_c[...], NN, HIGH)
        den = own_w * den + carry_w * jnp.sum(query_f * carry_n[:, :dk], axis=-1, keepdims=True)
        result = num / jnp.maximum(jnp.abs(den), jnp.exp(-top))
        summed = result if d == 0 else summed + result
        if d == 0:
            advance()
    inverse = lax.rsqrt(jnp.mean(summed * summed, axis=-1, keepdims=True) + EPS)
    joined[head, :, :dv] = (summed * inverse * head_gain[...]).astype(BF16)
    for o in range(1, t):
        share(0, o, head).start()

    lax.fori_loop(done[0] + 1, n - 1, lambda s, c: (ring_step(s, *wo_ring), c)[1], 0)
    ring_last(*wo_ring)
    for part in range(2):
        for o in range(1, t):
            share(part, o, lax.rem(head + o, t)).wait_recv()

    span_j = 2 * dv

    def emit(i, c):
        span = pl.ds(pl.multiple_of(i * width, width), width)
        total = dot(joined[0], wo_all[0:span_j, span], NN)
        for j in range(1, t):
            total += dot(joined[j], wo_all[j * span_j : (j + 1) * span_j, span], NN)
        out[:, span] = total.astype(BF16)
        return c

    lax.fori_loop(0, out.shape[1] // width, emit, 0)
    ring_drain(*w_ring)
    ring_drain(*wo_ring)
    lax.fori_loop(1, n, give_end, 0)
    for part in range(2):
        for o in range(1, t):
            share(part, o, head).wait_send()


def gather_body(
    n,
    t,
    tokens,
    norm_gain,
    w_query,
    w_key,
    w_value,
    w_gates,
    input_bias,
    forget_bias,
    decay_shift,
    head_gain,
    w_conv_b,
    w_conv_c,
    w_conv_in,
    conv_taps,
    w_out,
):
    rows, model = tokens.shape
    dk, dv = w_query.shape[1], w_value.shape[1]
    gates = jnp.transpose(w_gates[..., 0], (2, 1, 0)).reshape(4, model)
    gates = jnp.pad(gates, ((0, 4), (0, 0)))
    depth = w_query.shape[0]
    wide, cols = 2 * dk + dv + 3 * w_conv_b.shape[1], w_out.shape[1]
    hbm = pl.BlockSpec(memory_space=pl.ANY)
    vmem = pl.BlockSpec(memory_space=pltpu.VMEM)
    dma = pltpu.SemaphoreType.DMA
    return pl.pallas_call(
        functools.partial(gather_kernel, n, t, dk, dv),
        out_shape=jax.ShapeDtypeStruct((rows, cols), BF16),
        in_specs=[vmem] * 2 + [hbm] * 7 + [vmem] * 6,
        out_specs=vmem,
        scratch_shapes=[
            pltpu.VMEM((rows, model), BF16),
            pltpu.VMEM((n * depth, wide), BF16),
            pltpu.VMEM((n * w_out.shape[0], cols), BF16),
            pltpu.VMEM((rows, wide), BF16),
            pltpu.VMEM((2, dk, dv), BF16),
            pltpu.VMEM((2, 8, dv), F32),
            pltpu.VMEM((n, dk, dv), BF16),
            pltpu.VMEM((n, 8, dv), F32),
            pltpu.VMEM((dk, dv), F32),
            pltpu.VMEM((1, dv), F32),
            pltpu.VMEM((t, rows, 2 * dv), BF16),
            dma((2, (n - 1) * pieces(depth))),
            dma((2, (n - 1) * pieces(depth))),
            dma((2, (n - 1) * pieces(w_out.shape[0]))),
            dma((2, (n - 1) * pieces(w_out.shape[0]))),
            dma((n,)),
            dma((n,)),
            dma((n,)),
            dma((n,)),
            dma((2, t)),
            dma((2, t)),
            dma((7,)),
            pltpu.VMEM((8, 1), F32),
            pltpu.VMEM((8, rows), F32),
        ],
        compiler_params=pltpu.CompilerParams(
            collective_id=0, has_side_effects=True, vmem_limit_bytes=60 * 1024 * 1024
        ),
    )(
        tokens,
        norm_gain.reshape(1, model),
        w_query,
        w_key,
        w_value,
        w_conv_b,
        w_conv_c,
        w_conv_in,
        w_out,
        gates,
        input_bias,
        forget_bias,
        decay_shift[..., 0],
        head_gain.reshape(1, dv),
        conv_taps,
    )


PAIR = 2
WO_PIECES = 2


def fits(n, t, tokens, norm_gain, w_query, w_key, w_value, *rest):
    w_conv, w_out = rest[5], rest[9]
    depth, dk = w_query.shape
    dv = w_value.shape[1]
    rows = tokens.shape[0]
    even = n % PAIR == 0 and n > PAIR and t == 4
    wide = 2 * dk == dv and w_conv.shape[1] == dv and dv % 128 == 0 and dk % 128 == 0
    deep = (PAIR * depth) % (t * 128) == 0 and rows % 32 == 0 and w_out.shape[0] % (16 * WO_PIECES) == 0
    return even and wide and deep and rows <= depth


def kernel(
    n,
    t,
    dk,
    dv,
    tokens,
    norm_gain,
    w_query,
    w_key,
    w_value,
    w_conv_b,
    w_conv_c,
    w_conv_in,
    w_out,
    w_gates,
    input_bias,
    forget_bias,
    decay_shift,
    head_gain,
    taps,
    out,
    tok,
    nbuf,
    tall,
    wbuf,
    wo_all,
    acc,
    sbuf,
    rbuf,
    proj,
    wg,
    decay,
    state_out,
    pack_out,
    mate_state,
    mate_pack,
    pair_state,
    pair_pack,
    state_in,
    pack_in,
    edge_out,
    edge_in,
    carry_c,
    carry_n,
    local_num,
    joined,
    result,
    out_acc,
    out_sem,
    own_sem,
    tok_sem,
    tk_ss,
    tk_rs,
    tf_ss,
    tf_rs,
    w_ss,
    w_rs,
    rs_ss,
    rs_rs,
    st_ss,
    st_rs,
    pk_ss,
    pk_rs,
    ed_ss,
    ed_rs,
    j_ss,
    j_rs,
    jp_rs,
    oz_ss,
    oz_rs,
    oy_ss,
    oy_rs,
    ox_ss,
    ox_rs,
):
    me = lax.axis_index("sp")
    head = lax.axis_index("tp")
    lines = n // PAIR
    z = lax.div(me, PAIR)
    y = lax.rem(me, PAIR)
    mate = me + 1 - 2 * y
    core = lax.rem(head, 2)
    core_mate = head + 1 - 2 * core
    x_mate = lax.rem(head + 2, t)
    far_mate = lax.rem(core_mate + 2, t)
    rows, model = tokens.shape
    depth = w_query.shape[0]
    part_k = nbuf.shape[-1]
    chunks = wbuf.shape[0]

    def at_line(line):
        return PAIR * line + y

    edge_in[...] = jnp.zeros_like(edge_in)

    barrier = pltpu.get_barrier_semaphore()

    def greet_sp(o, c):
        pl.semaphore_signal(barrier, inc=1, device_id={"sp": lax.rem(me + o, n)})
        return c

    def greet_tp(o, c):
        pl.semaphore_signal(barrier, inc=1, device_id={"tp": lax.rem(head + o, t)})
        return c

    lax.fori_loop(1, n, greet_sp, 0)
    lax.fori_loop(1, t, greet_tp, 0)

    rows_at_once = 32

    def load_rows(i):
        span = pl.ds(pl.multiple_of(i * rows_at_once, rows_at_once), rows_at_once)
        return pltpu.make_async_copy(tokens.at[span, :], tok.at[span, :], tok_sem.at[i])

    def load_start(i, c):
        load_rows(i).start()
        return c

    lax.fori_loop(0, rows // rows_at_once, load_start, 0)
    mine = pl.ds(pl.multiple_of(y * depth, depth), depth)
    loads = []
    plan = ((w_query, 0, 0), (w_key, 0, dk), (w_value, 1, 0), (w_conv_c, 2, 0), (w_conv_in, 3, 0), (w_conv_b, 4, 0))
    for part, chunk, offset in plan:
        spot = wbuf.at[chunk, mine, pl.ds(offset, part.shape[1])]
        loads.append(pltpu.make_async_copy(part, spot, own_sem.at[1 + len(loads)]))
    depth_o = w_out.shape[0]
    spot = wo_all.at[pl.ds(pl.multiple_of(me * depth_o, depth_o), depth_o), :]
    loads.append(pltpu.make_async_copy(w_out, spot, own_sem.at[1 + len(loads)]))
    for load in loads:
        load.start()

    def norm_rows(i, c):
        load_rows(i).wait()
        span = pl.ds(pl.multiple_of(i * rows_at_once, rows_at_once), rows_at_once)
        values = tok[span, :].astype(F32)
        inverse = lax.rsqrt(jnp.mean(values * values, axis=-1, keepdims=True) + EPS)
        normed = (values * inverse * norm_gain[...]).astype(BF16)
        for b in range(lines * t):
            nbuf[b // t, b % t, span, :] = normed[:, b * part_k : (b + 1) * part_k]
        return c

    lax.fori_loop(0, rows // rows_at_once, norm_rows, 0)
    pl.semaphore_wait(barrier, n + t - 2)

    ups = lines - 1 - z

    half_way = lines // 2
    end_here = 1 - jnp.minimum(z, 1) * jnp.minimum(ups, 1)
    inner_up = jnp.minimum(lax.div(ups, half_way), 1)
    inner_count = inner_up * ups + (1 - inner_up) * z

    def pick(k, near):
        up = jnp.clip(ups - k, 0, 1)
        down_k = k - ups
        if near:
            return up, up * (z + 1 + k) + (1 - up) * (z - 1 - down_k)
        return up, up * (lines - 1 - k) + (1 - up) * down_k

    def token_send(line):
        return pltpu.make_async_remote_copy(
            nbuf.at[line, head], tall.at[z, head], tk_ss.at[0], tk_rs.at[z], device_id={"sp": at_line(line)}
        )

    def token_take(line):
        return pltpu.make_async_remote_copy(
            nbuf.at[line, head], tall.at[line, head], tk_ss.at[0], tk_rs.at[line], device_id={"sp": at_line(line)}
        )

    def token_pass(line, way):
        quarter = (head, head, x_mate)[way]
        there = tall.at[line, quarter]
        sem = lines if way != 1 else line
        return pltpu.make_async_remote_copy(
            there, there, tf_ss.at[0], tf_rs.at[sem], device_id={"tp": (core_mate, x_mate, core_mate)[way]}
        )

    def token_get(line):
        there = tall.at[line, x_mate]
        return pltpu.make_async_remote_copy(there, there, tf_ss.at[0], tf_rs.at[line], device_id={"tp": x_mate})

    def send_tokens(k, c):
        _, line = pick(k, False)
        token_send(line).start()
        return c

    lax.fori_loop(0, lines - 1, send_tokens, 0)

    def w_send(chunk):
        there = wbuf.at[chunk, mine, :]
        return pltpu.make_async_remote_copy(there, there, w_ss.at[0], w_rs.at[chunk], device_id={"sp": mate})

    def w_take(chunk):
        there = wbuf.at[chunk, pl.ds(pl.multiple_of((1 - y) * depth, depth), depth), :]
        return pltpu.make_async_remote_copy(there, there, w_ss.at[0], w_rs.at[chunk], device_id={"sp": mate})

    for load in loads:
        load.wait()
    for chunk in range(chunks):
        w_send(chunk).start()

    tall_o = depth_o // WO_PIECES

    def wo_rows(index, piece):
        return wo_all.at[pl.ds(pl.multiple_of(index * depth_o + piece * tall_o, tall_o), tall_o), :]

    def wo_line(line, piece, way, sem):
        there = wo_rows(at_line(line), piece)
        return pltpu.make_async_remote_copy(
            there, there, oz_ss.at[0], oz_rs.at[line, piece], device_id={"sp": at_line(z + way)}
        )

    def wo_mate(line, piece):
        there = wo_rows(at_line(line), piece)
        return pltpu.make_async_remote_copy(
            there, there, oy_ss.at[0], oy_rs.at[line, piece], device_id={"sp": mate}
        )

    def wo_mate_take(line, piece):
        there = wo_rows(PAIR * line + 1 - y, piece)
        return pltpu.make_async_remote_copy(
            there, there, oy_ss.at[0], oy_rs.at[line, piece], device_id={"sp": mate}
        )

    def wo_own(way, wanted):
        @pl.when(wanted)
        def _():
            for piece in range(WO_PIECES):
                wo_line(z, piece, way, lines + (way + 1) // 2).start()

    has_up, has_down = z < lines - 1, z > 0
    at_end = jnp.logical_or(z == 0, z == lines - 1)
    upper = z >= half_way

    def wo_outward():
        wo_own(1, jnp.logical_and(upper, has_up))
        wo_own(-1, jnp.logical_and(jnp.logical_not(upper), has_down))

    def wo_inward(ends):
        here = at_end if ends else jnp.logical_not(at_end)
        wo_own(-1, jnp.logical_and(jnp.logical_and(upper, has_down), here))
        wo_own(1, jnp.logical_and(jnp.logical_and(jnp.logical_not(upper), has_up), here))

    def wo_relay(line, wanted, along, across, pieces_now=range(WO_PIECES)):
        @pl.when(jnp.logical_and(wanted, jnp.logical_and(line >= 0, line < lines)))
        def _():
            for piece in pieces_now:
                if along:
                    wo_line(line, piece, 0, line).wait_recv()

                    @pl.when(jnp.logical_and(line < z, has_up))
                    def _():
                        wo_line(line, piece, 1, line).start()

                    @pl.when(jnp.logical_and(line > z, has_down))
                    def _():
                        wo_line(line, piece, -1, line).start()

                if across:

                    @pl.when(from_mate(line, piece))
                    def _():
                        wo_mate(line, piece).start()

                    if spread and piece == tail_piece:

                        @pl.when(jnp.logical_and(at_end, line == near_line))
                        def _():
                            mate_cut(line, y).start()

    inner_way = 2 * inner_up - 1

    spread = lines == 4
    tail_piece = WO_PIECES - 1
    near_line, far_line = z + inner_way, z + 2 * inner_way
    at_mid = jnp.logical_not(at_end)

    def cut_rows(index, half, halves):
        count = tall_o // halves
        first = index * depth_o + tail_piece * tall_o + half * count
        return wo_all.at[pl.ds(pl.multiple_of(first, count), count), :]

    def mate_cut(line, row):
        there = cut_rows(PAIR * line + row, 1, 2)
        return pltpu.make_async_remote_copy(
            there, there, oy_ss.at[0], oy_rs.at[line, tail_piece], device_id={"sp": mate}
        )

    def along_row(line, way, kind):
        there = cut_rows(PAIR * line + 1 - y, 0, 1 + kind)
        return pltpu.make_async_remote_copy(
            there, there, ox_ss.at[kind], ox_rs.at[kind], device_id={"sp": at_line(z + way)}
        )

    def from_mate(line, piece):
        if not spread or piece != tail_piece:
            return line >= 0
        return jnp.logical_or(
            jnp.logical_and(at_mid, line != far_line), jnp.logical_and(at_end, line != near_line)
        )

    def spread_send():
        if spread:

            @pl.when(at_mid)
            def _():
                wo_mate_take(z, tail_piece).wait_recv()
                along_row(z, -inner_way, 1).start()
                wo_mate_take(z - inner_way, tail_piece).wait_recv()
                along_row(z - inner_way, inner_way, 0).start()

    def wo_first(pieces_now, along=True, across=True, wanted=True):
        wo_relay(z - inner_way * (1 - 2 * end_here), wanted, along, across, pieces_now)

    def wo_second(along, across, pieces_now=range(WO_PIECES)):
        wo_relay(z + inner_way, jnp.logical_not(at_end), along, across, pieces_now)

    def wo_rest(away, pieces_now, along=True, across=True, wanted=True):
        wo_relay(z - away, wanted, along, across, pieces_now)
        wo_relay(z + away, wanted, along, across, pieces_now)

    for piece in range(WO_PIECES):
        wo_mate(z, piece).start()
    wo_inward(True)

    wg[...] = jnp.zeros_like(wg)
    wg[0:2, :] = w_gates[0]
    wg[2:4, :] = w_gates[1]
    decay[...] = jnp.zeros_like(decay)
    decay[1:2, :] = decay_shift[0]
    decay[3:4, :] = decay_shift[1]
    gates = None
    for b in range(lines * t):
        piece = dot(wg[:, b * part_k : (b + 1) * part_k], nbuf[b // t, b % t], NT)
        gates = piece if b == 0 else gates + piece
    gate_id = lax.broadcasted_iota(jnp.int32, gates.shape, 0)
    offsets = (input_bias[0, 0], forget_bias[0, 0], input_bias[0, 1], forget_bias[0, 1])
    for i, offset in enumerate(offsets):
        gates = jnp.where(gate_id == i, gates + offset, gates)
    forget = jnp.minimum(gates, 0.0) - jnp.log1p(jnp.exp(-jnp.abs(gates))) + decay[...]
    row_id = lax.broadcasted_iota(jnp.int32, (rows, rows), 0)
    col_id = lax.broadcasted_iota(jnp.int32, (rows, rows), 1)
    upto = (row_id <= col_id).astype(F32)
    after = (row_id >= col_id).astype(F32)
    sums = (dot(forget, upto, NN, HIGH), dot(forget, after, NN, HIGH))
    gates_t = gates.T
    sums_t = (sums[0].T, sums[1].T)

    def relay_direct(k, c):
        _, line = pick(k, True)
        token_take(line).wait_recv()
        token_pass(line, 1).start()
        token_pass(line, 0).start()
        return c

    def relay_across(k, c):
        _, line = pick(k, True)
        token_get(line).wait_recv()
        token_pass(line, 2).start()
        return c

    wo_inward(False)
    lax.fori_loop(0, lines - 1, relay_direct, 0)
    wo_outward()
    lax.fori_loop(0, lines - 1, relay_across, 0)
    both = tall.at[pl.ds(0, lines - 1), pl.ds(0, 2)]
    pltpu.make_async_remote_copy(both, both, tf_ss.at[0], tf_rs.at[lines], device_id={"tp": core_mate}).wait_recv()
    def parts_of(chunk):
        if isinstance(chunk, int) and chunk == chunks - 1:
            return ((0, rows // 2, chunk), (rows // 2, rows // 2, chunks))
        return ((0, rows, chunk),)

    def hop(chunk, part, k, up, line):
        first, count, sem = part
        last = (1 - up) * (1 - jnp.minimum(jnp.abs(z - line) - 1, 1))
        slot = line + last * (lines - line)
        return pltpu.make_async_remote_copy(
            sbuf.at[chunk, k, pl.ds(first, count)],
            rbuf.at[chunk, slot, pl.ds(first, count)],
            rs_ss.at[0],
            rs_rs.at[sem, slot],
            device_id={"sp": at_line(z + 2 * up - 1)},
        )

    def arrived(chunk, part, slot):
        first, count, sem = part
        return pltpu.make_async_remote_copy(
            sbuf.at[chunk, 0, pl.ds(first, count)],
            rbuf.at[chunk, slot, pl.ds(first, count)],
            rs_ss.at[0],
            rs_rs.at[sem, slot],
            device_id={"sp": me},
        )

    def product(source, line, chunk, part):
        span = pl.ds(part[0], part[1])
        total = dot(source[line, 0, span, :], wbuf[chunk, 0:part_k, :], NN)
        for q in range(1, t):
            total += dot(source[line, q, span, :], wbuf[chunk, q * part_k : (q + 1) * part_k, :], NN)
        return total

    def add_along(chunk, part, slot, up, line):
        span = pl.ds(part[0], part[1])
        acc[span, :] = product(tall, line, chunk, part)
        before = up * jnp.minimum(z, 1) + (1 - up) * jnp.minimum(ups, 1)

        @pl.when(before == 1)
        def _():
            arrived(chunk, part, line).wait_recv()
            sbuf[chunk, slot, span, :] = (acc[span, :] + rbuf[chunk, line, span, :].astype(F32)).astype(BF16)

        @pl.when(before == 0)
        def _():
            sbuf[chunk, slot, span, :] = acc[span, :].astype(BF16)

        hop(chunk, part, slot, up, line).start()

    def inward_span(first, last, chunk):
        def one(k, c):
            line = inner_up * (lines - 1 - k) + (1 - inner_up) * k
            for part in parts_of(chunk):
                add_along(chunk, part, k, inner_up, line)
            return c

        lax.fori_loop(first, last, one, 0)

    def inward_where(runs, chunk):
        @pl.when(runs == 1)
        def _():
            w_take(chunk).wait_recv()

        inward_span(0, runs * inner_count, chunk)

    def inward(end_chunk, mid_chunk):
        end_runs, mid_runs = end_chunk < chunks, mid_chunk >= 0
        if end_runs and mid_runs and max(end_chunk, mid_chunk) < chunks - 1:
            inward_where(1, end_here * end_chunk + (1 - end_here) * mid_chunk)
            return
        if end_runs:
            inward_where(end_here, end_chunk)
        if mid_runs:
            inward_where(1 - end_here, mid_chunk)

    def outward(chunk):
        for part in parts_of(chunk):

            def one(k, c):
                line = (1 - inner_up) * (lines - 1 - k) + inner_up * k
                add_along(chunk, part, inner_count + k, 1 - inner_up, line)
                return c

            lax.fori_loop(0, lines - 1 - inner_count, one, 0)

    def own_part(chunk, part):
        span = pl.ds(part[0], part[1])
        acc[span, :] = product(nbuf, z, chunk, part)

        @pl.when(has_down)
        def _():
            arrived(chunk, part, z).wait_recv()
            acc[span, :] += rbuf[chunk, z, span, :].astype(F32)

        @pl.when(has_up)
        def _():
            arrived(chunk, part, lines).wait_recv()
            acc[span, :] += rbuf[chunk, lines, span, :].astype(F32)

    def own_chunk(chunk):
        own_part(chunk, parts_of(chunk)[0])
        proj[chunk] = acc[...].astype(BF16)

    inward(0, -1)
    inward(1, -1)
    inward(2, 0)
    wo_first((0,))
    wo_second(True, False, (0,))
    inward(3, 1)
    wo_first(range(1, WO_PIECES), True, False)
    outward(0)
    wo_second(True, False, range(1, WO_PIECES))
    own_chunk(0)
    wo_rest(2, (0,), True, True, at_end)
    inward(chunks, 2)
    outward(1)
    own_chunk(1)

    keys_f = proj[0, :, dk:].astype(F32)
    wide = pack_out.shape[-1]
    for d in range(2):
        cum_c = sums_t[d][:, 2 * d + 1 : 2 * d + 2]
        in_c = gates_t[:, 2 * d : 2 * d + 1]
        last = rows - 1 if d == 0 else 0
        total = cum_c[last : last + 1, :]
        update = total - cum_c + in_c
        stable = jnp.max(update, axis=0, keepdims=True)
        weighted = keys_f * jnp.exp(update - stable)
        state_out[d] = dot(weighted.astype(BF16), proj[1], TN).astype(BF16)
        pack_out[d, 0:1, :dk] = jnp.sum(weighted, axis=0, keepdims=True)
        pack_out[d, 0:1, dk:] = jnp.zeros((1, wide - dk), F32)
        pack_out[d, 1:2, :] = jnp.broadcast_to(total, (1, wide))
        pack_out[d, 2:3, :] = jnp.broadcast_to(stable, (1, wide))
        pack_out[d, 3:, :] = jnp.zeros((5, wide), F32)

    def swap_states():
        return (
            pltpu.make_async_remote_copy(state_out, mate_state, st_ss.at[2], st_rs.at[2], device_id={"sp": mate}),
            pltpu.make_async_remote_copy(pack_out, mate_pack, pk_ss.at[2], pk_rs.at[2], device_id={"sp": mate}),
        )

    for copy in swap_states():
        copy.start()
    wo_first(range(1, WO_PIECES), False, True)
    wo_second(False, True, (0,))
    wo_rest(2, (0,), True, False, at_mid)
    wo_rest(2, range(1, WO_PIECES), True, False)
    wo_rest(2, range(1, WO_PIECES), False, True, at_end)

    d_in, d_out = 1 - inner_up, inner_up

    def chain(d, way):
        ids = {"sp": at_line(z + way)}
        return (
            pltpu.make_async_remote_copy(pair_state.at[d], state_in.at[d], st_ss.at[d], st_rs.at[d], device_id=ids),
            pltpu.make_async_remote_copy(pair_pack.at[d], pack_in.at[d], pk_ss.at[d], pk_rs.at[d], device_id=ids),
        )

    def chain_add(d):
        for copy in chain(d, 0):
            copy.wait_recv()
        total, stable, first_w, second_w = blend(pack_in[d], pair_pack[d])
        joint = first_w[:, :1] * state_in[d].astype(F32) + second_w[:, :1] * pair_state[d].astype(F32)
        pair_state[d] = joint.astype(BF16)
        pair_pack[d, 0:1, :] = first_w * pack_in[d, 0:1, :] + second_w * pair_pack[d, 0:1, :]
        pair_pack[d, 1:2, :] = total
        pair_pack[d, 2:3, :] = stable

    def chain_from_end():
        @pl.when(at_end)
        def _():
            for copy in chain(d_in, inner_way):
                copy.start()

    def chain_inward():
        @pl.when(jnp.logical_not(at_end))
        def _():
            chain_add(d_in)
            for copy in chain(d_in, inner_way):
                copy.start()

    def chain_outward():
        @pl.when(jnp.logical_not(at_end))
        def _():
            chain_add(d_out)
            for copy in chain(d_out, -inner_way):
                copy.start()

        @pl.when(at_end)
        def _():
            for copy in chain(d_out, 0):
                copy.wait_recv()

    def blend(first, second):
        total = first[1:2, :] + second[1:2, :]
        moved = first[2:3, :] + second[1:2, :]
        stable = jnp.maximum(moved, second[2:3, :])
        return total, stable, jnp.exp(moved - stable), jnp.exp(second[2:3, :] - stable)

    def pair_up():
        for copy in swap_states():
            copy.wait_recv()
        own_first = (1 - y).astype(F32)
        for d in range(2):
            lead = own_first if d == 0 else 1.0 - own_first
            mine_p, other_p = pack_out[d], mate_pack[d]
            first = lead * mine_p + (1.0 - lead) * other_p
            second = lead * other_p + (1.0 - lead) * mine_p
            total, stable, first_w, second_w = blend(first, second)
            mine_w = lead * first_w + (1.0 - lead) * second_w
            other_w = lead * second_w + (1.0 - lead) * first_w
            joint = mine_w * state_out[d].astype(F32) + other_w * mate_state[d].astype(F32)
            pair_state[d] = joint.astype(BF16)
            pair_pack[d, 0:1, :] = mine_w * mine_p[0:1, :] + other_w * other_p[0:1, :]
            pair_pack[d, 1:2, :] = total
            pair_pack[d, 2:3, :] = stable
            pair_pack[d, 3:, :] = jnp.zeros((5, wide), F32)

    inward(chunks, 3)
    pair_up()
    chain_from_end()
    inward(4, -1)
    outward(2)
    for away in range(3, lines):
        wo_rest(away, (0,))
    own_chunk(2)

    scale = dk ** (-0.5)
    scores = dot(proj[0, :, :dk], proj[0, :, dk:], NT) * scale
    local = []
    for d in range(2):
        cum_c = sums_t[d][:, 2 * d + 1 : 2 * d + 2]
        cum_r = sums[d][2 * d + 1 : 2 * d + 2, :]
        in_r = gates[2 * d : 2 * d + 1, :]
        allowed = row_id >= col_id if d == 0 else row_id <= col_id
        log_weight = jnp.where(allowed, cum_c - cum_r + in_r, -jnp.inf)
        peak = jnp.max(log_weight, axis=-1, keepdims=True)
        part = scores * jnp.exp(log_weight - peak)
        local_num[d] = dot(part.astype(BF16), proj[1], NN)
        local.append((cum_c, peak, jnp.sum(part, axis=-1, keepdims=True)))

    outward(3)
    own_chunk(3)

    mixed = (proj[2].astype(F32) * proj[3].astype(F32)).astype(BF16).astype(F32)
    edge_out[0, 0:1, :] = mixed[rows - 1 :, :]
    edge_out[1, 0:1, :] = mixed[:1, :]
    edge_out[0, 1:, :] = jnp.zeros((7, dv), F32)
    edge_out[1, 1:, :] = jnp.zeros((7, dv), F32)

    def edge(way):
        other = me + 1 if way == 0 else me - 1
        return pltpu.make_async_remote_copy(
            edge_out.at[way], edge_in.at[way], ed_ss.at[way], ed_rs.at[way], device_id={"sp": other}
        )

    later_exists, prior_exists = me < n - 1, me > 0

    @pl.when(later_exists)
    def _():
        edge(0).start()

    @pl.when(prior_exists)
    def _():
        edge(1).start()

    wo_second(False, True, range(1, WO_PIECES))
    wo_rest(2, range(WO_PIECES), False, True, jnp.logical_not(at_end))
    chain_inward()


    @pl.when(at_mid)
    def _():
        w_take(4).wait_recv()

    inward_span(0, 1 - end_here, 4)
    chain_outward()
    inward_span(1, (1 - end_here) * inner_count, 4)
    for away in range(3, lines):
        wo_rest(away, range(1, WO_PIECES))

    half_rows = rows // 2

    def joined_part(part, source, way):
        columns = pl.ds(part * dv, dv)
        if way == 0:
            return joined.at[source, :, columns]
        return joined.at[source, pl.ds((way - 1) * half_rows, half_rows), columns]

    others = (core_mate, x_mate, far_mate)

    def share(part, way, source):
        slot = joined_part(part, source, way)
        return pltpu.make_async_remote_copy(
            slot, slot, j_ss.at[0], j_rs.at[part, way], device_id={"tp": others[way]}
        )

    def share_pass(part, way, source):
        slot = joined_part(part, source, way)
        return pltpu.make_async_remote_copy(
            slot, slot, j_ss.at[0], jp_rs.at[part, way - 1], device_id={"tp": core_mate}
        )

    def share_start(part):
        for way in (1, 2, 0):
            share(part, way, head).start()

    def share_relay(part):
        for way in (1, 2):
            share(part, way, others[way]).wait_recv()
            share_pass(part, way, others[way]).start()

    def share_wait(part):
        share(part, 0, core_mate).wait_recv()
        for way in (1, 2):
            share_pass(part, way, others[3 - way]).wait_recv()

    summed = None
    query_f = proj[0, :, :dk].astype(F32) * scale
    for d in range(2):
        carry_c[...] = jnp.zeros_like(carry_c)
        carry_n[...] = jnp.zeros_like(carry_n)

        def merge(state, pack, peak_in):
            total = pack[1:2, :]
            stable = pack[2:3, :]
            new = jnp.maximum(peak_in + total, stable)
            old_w = jnp.exp(peak_in + total - new)
            new_w = jnp.exp(stable - new)
            carry_c[...] = old_w * carry_c[...] + new_w * state.astype(F32)
            carry_n[...] = old_w * carry_n[...] + new_w * pack[0:1, :]
            return new

        def join(i, peak_in):
            return merge(state_in[d], pack_in[d], peak_in)

        def join_mate(i, peak_in):
            return merge(mate_state[d], mate_pack[d], peak_in)

        peak_in = lax.fori_loop(0, jnp.minimum(z if d == 0 else ups, 1), join, jnp.full((1, dv), LOWEST, F32))
        peak_in = lax.fori_loop(0, y if d == 0 else 1 - y, join_mate, peak_in)
        cum_c, peak, den = local[d]
        carried = cum_c + peak_in[:, :1]
        top = jnp.maximum(carried, peak)
        carry_w = jnp.exp(carried - top)
        own_w = jnp.exp(peak - top)
        num = own_w * local_num[d] + carry_w * dot(query_f.astype(BF16), carry_c[...].astype(BF16), NN)
        den = own_w * den + carry_w * jnp.sum(query_f * carry_n[:, :dk], axis=-1, keepdims=True)
        cell = num / jnp.maximum(jnp.abs(den), jnp.exp(-top))
        summed = cell if d == 0 else summed + cell
    inverse = lax.rsqrt(jnp.mean(summed * summed, axis=-1, keepdims=True) + EPS)
    joined[head, :, :dv] = (summed * inverse * head_gain[...]).astype(BF16)
    share_start(0)
    outward(4)
    spread_send()

    @pl.when(prior_exists)
    def _():
        edge(0).wait_recv()

    @pl.when(later_exists)
    def _():
        edge(1).wait_recv()

    mixed = (proj[2].astype(F32) * proj[3].astype(F32)).astype(BF16).astype(F32)
    pos = lax.broadcasted_iota(jnp.int32, mixed.shape, 0)
    prior = jnp.where(pos == 0, edge_in[0, 0:1, :], pltpu.roll(mixed, 1, 0))
    later = jnp.where(pos == rows - 1, edge_in[1, 0:1, :], pltpu.roll(mixed, rows - 1, 0))
    taps_f = taps[...].astype(F32)
    local_num[0] = taps_f[0:1] * prior + taps_f[1:2] * mixed + taps_f[2:3] * later
    for i, part in enumerate(parts_of(chunks - 1)):
        span = pl.ds(part[0], part[1])
        own_part(chunks - 1, part)
        outer = acc[span, :].astype(BF16).astype(F32)
        joined[head, span, dv:] = (outer * local_num[0, span, :]).astype(BF16)
        share(1, 1 + i, head).start()
    share(1, 0, head).start()
    share_relay(0)
    share_relay(1)

    for line in range(lines):
        for piece in range(WO_PIECES):
            if not spread or piece != tail_piece:
                wo_mate_take(line, piece).wait_recv()
                continue

            @pl.when(jnp.logical_or(jnp.logical_and(at_mid, line == near_line), jnp.logical_and(at_end, line != near_line)))
            def _():
                wo_mate_take(line, piece).wait_recv()

    if spread:

        @pl.when(at_mid)
        def _():
            along_row(far_line, 0, 0).wait_recv()

        @pl.when(at_end)
        def _():
            along_row(near_line, 0, 1).wait_recv()
            mate_cut(near_line, 1 - y).wait_recv()

    share_wait(0)
    width = 512

    def columns_of(part, i):
        span = pl.ds(pl.multiple_of(i * width, width), width)
        total = None
        for j in range(t):
            first = (2 * j + part) * dv
            term = dot(joined[j, :, part * dv : (part + 1) * dv], wo_all[first : first + dv, span], NN)
            total = term if j == 0 else total + term
        return span, total

    def emit_cell(i, c):
        span, total = columns_of(0, i)
        out_acc[:, span] = total
        return c

    def emit(i, c):
        span, total = columns_of(1, i)
        result[:, span] = (out_acc[:, span] + total).astype(BF16)
        put(i).start()
        return c

    def put(i):
        span = pl.ds(pl.multiple_of(i * width, width), width)
        return pltpu.make_async_copy(result.at[:, span], out.at[:, span], out_sem.at[i])

    def put_end(i, c):
        put(i).wait()
        return c

    lax.fori_loop(0, out.shape[1] // width, emit_cell, 0)
    share_wait(1)
    lax.fori_loop(0, out.shape[1] // width, emit, 0)

    def sent(ref, sem):
        pltpu.make_async_remote_copy(ref, ref, sem.at[0], w_rs.at[0], device_id={"sp": mate}).wait_send()

    sent(nbuf.at[pl.ds(0, lines - 1), 0], tk_ss)
    sent(tall.at[pl.ds(0, lines - 1), pl.ds(0, 3)], tf_ss)
    sent(wbuf.at[:, mine, :], w_ss)
    sent(sbuf, rs_ss)
    sent(joined.at[pl.ds(0, 3)], j_ss)

    @pl.when(at_end)
    def _():
        sent(wo_all.at[pl.ds(0, depth_o)], oz_ss)

    @pl.when(at_mid)
    def _():
        sent(wo_all.at[pl.ds(0, (lines + 1) * depth_o)], oz_ss)

    if spread:

        @pl.when(at_end)
        def _():
            sent(wo_all.at[pl.ds(0, lines * depth_o - tall_o + tall_o // 2)], oy_ss)

        @pl.when(at_mid)
        def _():
            sent(wo_all.at[pl.ds(0, lines * depth_o - tall_o)], oy_ss)
            along_row(z, -inner_way, 1).wait_send()
            along_row(z - inner_way, inner_way, 0).wait_send()

    else:
        sent(wo_all.at[pl.ds(0, lines * depth_o)], oy_ss)

    for copy in swap_states():
        copy.wait_send()

    @pl.when(at_end)
    def _():
        for copy in chain(d_in, inner_way):
            copy.wait_send()

    @pl.when(jnp.logical_not(at_end))
    def _():
        for copy in chain(d_in, inner_way) + chain(d_out, -inner_way):
            copy.wait_send()


    @pl.when(later_exists)
    def _():
        edge(0).wait_send()

    @pl.when(prior_exists)
    def _():
        edge(1).wait_send()


    lax.fori_loop(0, out.shape[1] // width, put_end, 0)

def body(
    n,
    t,
    tokens,
    norm_gain,
    w_query,
    w_key,
    w_value,
    w_gates,
    input_bias,
    forget_bias,
    decay_shift,
    head_gain,
    w_conv_b,
    w_conv_c,
    w_conv_in,
    conv_taps,
    w_out,
):
    rows, model = tokens.shape
    depth, dk = w_query.shape
    dv = w_value.shape[1]
    lines = n // PAIR
    chunks = 5
    part_k = PAIR * depth // t
    cols = w_out.shape[1]
    gates = jnp.transpose(w_gates[..., 0], (1, 2, 0))
    hbm = pl.BlockSpec(memory_space=pl.ANY)
    vmem = pl.BlockSpec(memory_space=pltpu.VMEM)
    smem = pl.BlockSpec(memory_space=pltpu.SMEM)
    dma = pltpu.SemaphoreType.DMA
    return pl.pallas_call(
        functools.partial(kernel, n, t, dk, dv),
        out_shape=jax.ShapeDtypeStruct((rows, cols), BF16),
        in_specs=[hbm, vmem] + [hbm] * 7 + [vmem] + [smem] * 2 + [vmem] * 3,
        out_specs=hbm,
        scratch_shapes=[
            pltpu.VMEM((rows, model), BF16),
            pltpu.VMEM((lines, t, rows, part_k), BF16),
            pltpu.VMEM((lines, t, rows, part_k), BF16),
            pltpu.VMEM((chunks, PAIR * depth, dv), BF16),
            pltpu.VMEM((n * w_out.shape[0], cols), BF16),
            pltpu.VMEM((rows, dv), F32),
            pltpu.VMEM((chunks, lines - 1, rows, dv), BF16),
            pltpu.VMEM((chunks, lines + 1, rows, dv), BF16),
            pltpu.VMEM((chunks, rows, dv), BF16),
            pltpu.VMEM((8, model), BF16),
            pltpu.VMEM((8, rows), F32),
            pltpu.VMEM((2, dk, dv), BF16),
            pltpu.VMEM((2, 8, dv), F32),
            pltpu.VMEM((2, dk, dv), BF16),
            pltpu.VMEM((2, 8, dv), F32),
            pltpu.VMEM((2, dk, dv), BF16),
            pltpu.VMEM((2, 8, dv), F32),
            pltpu.VMEM((2, dk, dv), BF16),
            pltpu.VMEM((2, 8, dv), F32),
            pltpu.VMEM((2, 8, dv), F32),
            pltpu.VMEM((2, 8, dv), F32),
            pltpu.VMEM((dk, dv), F32),
            pltpu.VMEM((1, dv), F32),
            pltpu.VMEM((2, rows, dv), F32),
            pltpu.VMEM((t, rows, 2 * dv), BF16),
            pltpu.VMEM((rows, cols), BF16),
            pltpu.VMEM((rows, cols), F32),
            dma((cols // 256,)),
            dma((8,)),
            dma((rows // 32,)),
            dma((1,)),
            dma((lines,)),
            dma((1,)),
            dma((lines + 1,)),
            dma((1,)),
            dma((chunks,)),
            dma((1,)),
            dma((chunks + 1, lines + 1)),
            dma((3,)),
            dma((3,)),
            dma((3,)),
            dma((3,)),
            dma((2,)),
            dma((2,)),
            dma((1,)),
            dma((2, 3)),
            dma((2, 2)),
            dma((1,)),
            dma((lines, WO_PIECES)),
            dma((1,)),
            dma((lines, WO_PIECES)),
            dma((2,)),
            dma((2,)),
        ],
        compiler_params=pltpu.CompilerParams(
            collective_id=0, has_side_effects=True, vmem_limit_bytes=60 * 1024 * 1024
        ),
    )(
        tokens,
        norm_gain.reshape(1, model),
        w_query,
        w_key,
        w_value,
        w_conv_b,
        w_conv_c,
        w_conv_in,
        w_out,
        gates,
        input_bias.T,
        forget_bias.T,
        jnp.swapaxes(decay_shift, 1, 2),
        head_gain.reshape(1, dv),
        conv_taps,
    )


def solution(mesh):
    placed = (
        P("sp", None),
        P(),
        P("sp", "tp"),
        P("sp", "tp"),
        P("sp", "tp"),
        P(None, None, None, "tp"),
        P(None, "tp"),
        P(None, "tp"),
        P(None, "sp", "tp"),
        P("tp"),
        P("sp", "tp"),
        P("sp", "tp"),
        P("sp", "tp"),
        P(None, "tp"),
        P("sp", "tp"),
    )
    n, t = mesh.shape["sp"], mesh.shape["tp"]

    def step(*args):
        form = body if fits(n, t, *args) else gather_body
        return form(n, t, *args)

    return jax.shard_map(step, mesh=mesh, in_specs=placed, out_specs=P("sp", "tp"), check_vma=False)
```
